128 devices in a mesh: sp: 16 (over z, x), tp: 8 (over y, core).
Axes of the slice: x: 4, y: 4, z: 4, core: 2. Of those that a mesh axis runs over, the one named last changes fastest.
Arguments:
- hidden_states: bfloat16 [12288, 4096], P('sp'), may hold values from -60 to 60
- w_conv_b: bfloat16 [4096, 2048], P(None, 'tp'), may hold values from -0.09375 to 0.09375
- w_conv_c: bfloat16 [4096, 2048], P(None, 'tp'), may hold values from -0.09375 to 0.09375
- w_conv_h: bfloat16 [4096, 2048], P(None, 'tp'), may hold values from -0.09375 to 0.09375
- conv_taps: bfloat16 [3, 2048], P(None, 'tp'), may hold values from -3.5 to 3.5
- w_query: bfloat16 [4096, 2048], P(None, 'tp'), may hold values from -0.15625 to 0.15625
- w_key: bfloat16 [4096, 2048], P(None, 'tp'), may hold values from -0.09375 to 0.09375
- w_value: bfloat16 [4096, 2048], P(None, 'tp'), may hold values from -0.09375 to 0.09375
- lambdas: float32 [16], P('tp'), may hold values from 0.3 to 0.8
- head_gain: bfloat16 [128], replicated, may hold values from 0.099609375 to 1.8984375
- w_out_conv: bfloat16 [2048, 4096], P('tp'), may hold values from -1 to 1
- w_out_attn: bfloat16 [2048, 4096], P('tp'), may hold values from -1 to 1
- out_gain: bfloat16 [4096], replicated, may hold values from 0.099609375 to 1.8984375
Outputs:
- mixed: bfloat16 [12288, 4096], P('sp', 'tp')
The draws below stay inside these ranges and needn't reach their ends.
All inputs are finite; a program needn't handle non-finite values.
Results may differ from the reference program's by a relative error of at most 0.023.
Values may be sent and summed in bfloat16 or wider, within the bound.
No kernel may reach another device: no remote copies, remote signals or barrier semaphores. Data moves between devices by JAX's collectives and lax.ppermute only.
A program may use at most 192 MiB of HBM per device.

```python
import jax
import jax.numpy as jnp
from jax import lax

D = 4096
HEADS = 16
QK = 64
CONV = 2048
TAPS = 3
TOK_DEV = 768
VD = 128
TOKENS = 12288
N_TP = 8


def draw_hidden_states(key, part):
    values = jnp.clip(jax.random.normal(key, (TOKENS, D), jnp.float32), -6.0, 6.0)
    return jnp.clip(values, -60.0, 60.0).astype(jnp.bfloat16)


def rising_columns(key, row_count):
    columns = jnp.arange(D, dtype=jnp.float32) / D
    base = jnp.clip(jax.random.normal(key, (row_count, D), jnp.float32), -6.0, 6.0)
    ramp = 3.0 ** columns
    values = base * ramp[None, :] * (CONV + HEADS * VD) ** (-0.5)
    return jnp.clip(values, -1.0, 1.0).astype(jnp.bfloat16)


def draw_w_out_conv(key, part):
    return rising_columns(jax.random.fold_in(key, 11), CONV)


def draw_w_out_attn(key, part):
    return rising_columns(jax.random.fold_in(key, 13), HEADS * VD)


def block_scale(own_key, shape, cuts, smallest, high):
    gain = 1.0
    for position, shards_of in cuts:
        draws = jax.random.uniform(jax.random.fold_in(jax.random.fold_in(own_key, 6), position), (shards_of,), jnp.float32, smallest / len(cuts), high / len(cuts))
        gain = gain * jnp.repeat(jnp.exp(draws), shape[position] // shards_of).reshape((-1,) + (1,) * (len(shape) - 1 - position))
    return gain


def normal_values(key, shape, width, most, cuts=(), kind=jnp.bfloat16):
    values = width * jax.random.normal(key, shape, jnp.float32)
    if cuts:
        values = values * block_scale(key, shape, cuts, -0.22, 0.18)
    return jnp.clip(values, -most, most).astype(kind)


def setup_inputs(seed: int = 0) -> dict:
    splits = jax.random.split(jax.random.key(seed), 14)
    return {
        "hidden_states": draw_hidden_states(jax.random.fold_in(splits[13], 71), 0),
        "w_conv_b": normal_values(splits[1], (D, CONV), D ** -0.5, 0.09375, ((1, 8),)),
        "w_conv_c": normal_values(splits[2], (D, CONV), D ** -0.5, 0.09375, ((1, 8),)),
        "w_conv_h": normal_values(splits[3], (D, CONV), D ** -0.5, 0.09375, ((1, 8),)),
        "conv_taps": normal_values(splits[4], (TAPS, CONV), TAPS ** -0.5, 3.5, ((1, 8),)),
        "w_query": normal_values(splits[5], (D, HEADS * 2 * QK), (D // 3) ** -0.5, 0.15625, ((1, 8),)),
        "w_key": normal_values(splits[6], (D, HEADS * 2 * QK), D ** -0.5, 0.09375, ((1, 8),)),
        "w_value": normal_values(splits[7], (D, HEADS * VD), D ** -0.5, 0.09375, ((1, 8),)),
        "lambdas": jnp.clip(0.3 + 0.5 * jax.random.uniform(splits[8], (HEADS,), jnp.float32) ** block_scale(splits[8], (HEADS,), ((0, 8),), -0.2, 0.2), 0.3, 0.8),
        "head_gain": jnp.clip(1.0 + 0.18 * jax.random.normal(splits[9], (VD,), jnp.float32), 0.099609375, 1.8984375).astype(jnp.bfloat16),
        "w_out_conv": draw_w_out_conv(jax.random.fold_in(splits[13], 71), 0),
        "w_out_attn": draw_w_out_attn(jax.random.fold_in(splits[13], 71), 0),
        "out_gain": jnp.clip(1.0 + 0.18 * jax.random.normal(splits[12], (D,), jnp.float32), 0.099609375, 1.8984375).astype(jnp.bfloat16),
    }


def rotate(values, positions):
    inverse = 1.0 / 10000.0 ** (jnp.arange(0, QK, 2, dtype=jnp.float32) / QK)
    angles = positions[:, None] * inverse[None, :]
    angles = jnp.concatenate([angles, angles], axis=-1)
    cosine = jnp.cos(angles)[:, None, None, :]
    sine = jnp.sin(angles)[:, None, None, :]
    first_half, second_half = jnp.split(values, 2, axis=-1)
    return values * cosine + jnp.concatenate([-second_half, first_half], axis=-1) * sine

def reference(hidden_states, w_conv_b, w_conv_c, w_conv_h, conv_taps, w_query, w_key, w_value, lambdas, head_gain, w_out_conv, w_out_attn, out_gain):

    def project(weight):
        return jnp.dot(hidden_states, weight, preferred_element_type=jnp.float32).astype(jnp.bfloat16)
    u_b = project(w_conv_b)
    u_c = project(w_conv_c)
    u_h = project(w_conv_h)
    gated = u_c.astype(jnp.float32) * u_h.astype(jnp.float32)
    padded = jnp.concatenate([jnp.zeros((TAPS - 1, CONV), jnp.float32), gated], axis=0)
    taps_f = conv_taps.astype(jnp.float32)
    convolved = jnp.zeros((TOKENS, CONV), jnp.float32)
    for tap in range(TAPS):
        convolved = convolved + taps_f[tap][None, :] * padded[tap:tap + TOKENS]
    conv_out = (u_b.astype(jnp.float32) * convolved).astype(jnp.bfloat16)
    positions = jnp.arange(TOKENS, dtype=jnp.float32)
    query = rotate(project(w_query).reshape(TOKENS, HEADS, 2, QK).astype(jnp.float32), positions).astype(jnp.bfloat16)
    keys = rotate(project(w_key).reshape(TOKENS, HEADS, 2, QK).astype(jnp.float32), positions).astype(jnp.bfloat16)
    values = project(w_value).reshape(TOKENS, HEADS, VD)
    gain_f = head_gain.astype(jnp.float32)
    key_pos = jnp.arange(TOKENS, dtype=jnp.int32)

    def one_head(args):
        head_query, head_keys, head_values, weight_two = args
        keys_f = head_keys.astype(jnp.float32)
        values_f = head_values.astype(jnp.float32)

        def one_block(block_index):
            first = (block_index * TOK_DEV).astype(jnp.int32)
            block_query = lax.dynamic_slice_in_dim(head_query, first, TOK_DEV, 0).astype(jnp.float32)
            scores = jnp.einsum('qcd,kcd->cqk', block_query, keys_f) * QK ** (-0.5)
            query_pos = first + jnp.arange(TOK_DEV, dtype=jnp.int32)
            visible = key_pos[None, :] <= query_pos[:, None]
            scores = jnp.where(visible[None], scores, -jnp.inf)
            top = lax.optimization_barrier(jnp.max(scores, axis=-1, keepdims=True))
            weights = jnp.exp(scores - top)
            denom = lax.optimization_barrier(jnp.sum(weights, axis=-1))
            rounded = lax.optimization_barrier(weights.astype(jnp.bfloat16)).astype(jnp.float32)
            numer = jnp.einsum('cqk,ke->cqe', rounded, values_f)
            diff = numer[0] / denom[0][:, None] - weight_two * numer[1] / denom[1][:, None]
            normed = diff * lax.rsqrt(lax.optimization_barrier(jnp.mean(diff * diff, axis=-1, keepdims=True)) + 1e-05) * gain_f[None, :]
            return normed.astype(jnp.bfloat16)
        blocks = lax.map(one_block, jnp.arange(TOKENS // TOK_DEV, dtype=jnp.int32))
        return blocks.reshape(TOKENS, VD)
    per_head = lax.map(one_head, (query.transpose(1, 0, 2, 3), keys.transpose(1, 0, 2, 3), values.transpose(1, 0, 2), lambdas))
    attn_out = per_head.transpose(1, 0, 2).reshape(TOKENS, HEADS * VD)
    conv_width = CONV // N_TP
    attn_width = HEADS * VD // N_TP
    total = jnp.zeros((TOKENS, D), jnp.float32)
    for block in range(N_TP):
        term = jnp.dot(conv_out[:, block * conv_width:(block + 1) * conv_width], w_out_conv[block * conv_width:(block + 1) * conv_width], preferred_element_type=jnp.float32)
        term = term + jnp.dot(attn_out[:, block * attn_width:(block + 1) * attn_width], w_out_attn[block * attn_width:(block + 1) * attn_width], preferred_element_type=jnp.float32)
        total = total + lax.optimization_barrier(term.astype(jnp.bfloat16)).astype(jnp.float32)
    mix = total.astype(jnp.bfloat16).astype(jnp.float32)
    mean_value = lax.optimization_barrier(jnp.mean(mix, axis=-1, keepdims=True))
    variance = lax.optimization_barrier(jnp.mean(mix * mix, axis=-1, keepdims=True)) - mean_value * mean_value
    normed = (mix - mean_value) * lax.rsqrt(variance + 1e-05) * out_gain.astype(jnp.float32)[None, :]
    return normed.astype(jnp.bfloat16)
```

```python
import jax
import jax.numpy as jnp
import numpy as np
from jax import lax
from jax.experimental import pallas as pl
from jax.experimental.pallas import tpu as pltpu
from jax.sharding import Mesh
from jax.sharding import PartitionSpec as P

D = 4096
QK = 64
VD = 128
ROWS = 768
HALO = 16
LOG2E = 1.4426950408889634

CORE_OF_Z = (0, 1, 1, 0)


def forward_route(round_index):
    route = []
    for z in range(4):
        for c in range(2):
            local = round_index if z < 2 else 1 - round_index
            route.append((z * 2 + c, (2 * c + local) * 2 + CORE_OF_Z[z]))
    return route


def reverse(route):
    return [(b, a) for a, b in route]


def rotary_tables():
    inverse = 10000.0 ** (-np.arange(0, QK, 2, dtype=np.float64) / QK)
    inverse = np.tile(inverse, 128 // inverse.size)
    rows = np.arange(ROWS, dtype=np.float64)[:, None] * inverse
    starts = np.arange(16, dtype=np.float64)[:, None] * ROWS * inverse
    tables = (np.cos(rows), np.sin(rows), np.cos(starts), np.sin(starts))
    return tuple(t.astype(np.float32) for t in tables)


def qkv_kernel(first, h_ref, wq_ref, wk_ref, wv_ref, cr, sr, cs, ss, q_ref, kv_ref, acc):
    step = pl.program_id(0)
    h = h_ref[...]
    for i, w_ref in enumerate((wk_ref, wv_ref, wq_ref)):
        part = jnp.dot(h, w_ref[...], preferred_element_type=jnp.float32)

        @pl.when(step == 0)
        def _():
            acc[i] = part

        @pl.when(step > 0)
        def _():
            acc[i] += part

    @pl.when(step == pl.num_programs(0) - 1)
    def _():
        cosine = cs[...] * cr[...] - ss[...] * sr[...]
        sine = ss[...] * cr[...] + cs[...] * sr[...]
        lane = lax.broadcasted_iota(jnp.int32, (ROWS, 128), 1)
        upper = (lane % QK) < QK // 2

        def rotated(x):
            x = x.astype(jnp.bfloat16).astype(jnp.float32)
            swapped = jnp.where(upper, -pltpu.roll(x, 128 - QK // 2, 1), pltpu.roll(x, QK // 2, 1))
            return (x * cosine + swapped * sine).astype(jnp.bfloat16)

        for local in range(2):
            cols = slice(local * 128, local * 128 + 128)
            at = first[0] if local == 0 else 1 - first[0]
            kv_ref[at, :, 0:128] = rotated(acc[0, :, cols])
            kv_ref[at, :, 128:256] = acc[1, :, cols].astype(jnp.bfloat16)
            q_ref[at] = rotated(acc[2, :, cols])


def project_qkv(first, hidden, w_query, w_key, w_value, start_cos, start_sin):
    chunk = 512
    row_cos, row_sin, _, _ = rotary_tables()
    weight = pl.BlockSpec((chunk, 256), lambda k, *_: (k, 0))
    table = pl.BlockSpec((ROWS, 128), lambda k, *_: (0, 0))
    one = pl.BlockSpec((1, 128), lambda k, *_: (0, 0))
    return pl.pallas_call(
        qkv_kernel,
        out_shape=(
            jax.ShapeDtypeStruct((2, ROWS, 128), jnp.bfloat16),
            jax.ShapeDtypeStruct((2, ROWS, 256), jnp.bfloat16),
        ),
        grid_spec=pltpu.PrefetchScalarGridSpec(
            num_scalar_prefetch=1,
            grid=(D // chunk,),
            in_specs=[
                pl.BlockSpec((ROWS, chunk), lambda k, *_: (0, k)),
                weight,
                weight,
                weight,
                table,
                table,
                one,
                one,
            ],
            out_specs=(
                pl.BlockSpec((2, ROWS, 128), lambda k, *_: (0, 0, 0)),
                pl.BlockSpec((2, ROWS, 256), lambda k, *_: (0, 0, 0)),
            ),
            scratch_shapes=[pltpu.VMEM((3, ROWS, 256), jnp.float32)],
        ),
        compiler_params=pltpu.CompilerParams(vmem_limit_bytes=40 * 2**20),
        name="qkv",
    )(first, hidden, w_query, w_key, w_value, row_cos, row_sin, start_cos, start_sin)


def conv_kernel(h_ref, rim_ref, wb_ref, wc_ref, wh_ref, taps_ref, o_ref, acc, rim_acc, padded):
    step = pl.program_id(0)
    h = h_ref[...]
    rim = rim_ref[...]
    for i, w_ref in enumerate((wb_ref, wc_ref, wh_ref)):
        w = w_ref[...]
        part = jnp.dot(h, w, preferred_element_type=jnp.float32)
        rim_part = jnp.dot(rim, w, preferred_element_type=jnp.float32)

        @pl.when(step == 0)
        def _():
            acc[i] = part
            rim_acc[i] = rim_part

        @pl.when(step > 0)
        def _():
            acc[i] += part
            rim_acc[i] += rim_part

    @pl.when(step == pl.num_programs(0) - 1)
    def _():
        def once(x):
            return x.astype(jnp.bfloat16).astype(jnp.float32)

        padded[0:HALO] = once(rim_acc[1]) * once(rim_acc[2])
        padded[HALO:] = once(acc[1]) * once(acc[2])
        taps = taps_ref[...].astype(jnp.float32)
        conv = jnp.zeros((ROWS, 256), jnp.float32)
        for tap in range(3):
            conv = conv + taps[tap : tap + 1] * padded[HALO - 2 + tap : HALO - 2 + tap + ROWS]
        o_ref[...] = (once(acc[0]) * conv).astype(jnp.bfloat16)


def gated_conv(hidden, rim, w_b, w_c, w_h, taps):
    chunk = 512
    weight = pl.BlockSpec((chunk, 256), lambda k: (k, 0))
    return pl.pallas_call(
        conv_kernel,
        out_shape=jax.ShapeDtypeStruct((ROWS, 256), jnp.bfloat16),
        grid=(D // chunk,),
        in_specs=[
            pl.BlockSpec((ROWS, chunk), lambda k: (0, k)),
            pl.BlockSpec((HALO, chunk), lambda k: (0, k)),
            weight,
            weight,
            weight,
            pl.BlockSpec((3, 256), lambda k: (0, 0)),
        ],
        out_specs=pl.BlockSpec((ROWS, 256), lambda k: (0, 0)),
        scratch_shapes=[
            pltpu.VMEM((3, ROWS, 256), jnp.float32),
            pltpu.VMEM((3, HALO, 256), jnp.float32),
            pltpu.VMEM((HALO + ROWS, 256), jnp.float32),
        ],
        compiler_params=pltpu.CompilerParams(vmem_limit_bytes=40 * 2**20),
        name="gated_conv",
    )(hidden, rim, w_b, w_c, w_h, taps)


def attn_kernel(tab, lam, qa_ref, qb_ref, kv_ref, gain_ref, oa_ref, ob_ref, qz, m_s, l_s, acc):
    keys_at_once = 256

    for i, (q_ref, o_ref) in enumerate(((qa_ref, oa_ref), (qb_ref, ob_ref))):
        qb = tab[16 + i]
        lane = lax.broadcasted_iota(jnp.int32, (ROWS, 128), 1)
        qf = q_ref[...].astype(jnp.float32) * (0.125 * LOG2E)
        high = qf.astype(jnp.bfloat16)
        low = (qf - high.astype(jnp.float32)).astype(jnp.bfloat16)
        for h, v in enumerate((high, low)):
            zero = jnp.zeros_like(v)
            qz[0, :, h * 128 : h * 128 + 128] = jnp.where(lane < QK, v, zero)
            qz[1, :, h * 128 : h * 128 + 128] = jnp.where(lane >= QK, v, zero)
        m_s[...] = jnp.full(m_s.shape, -1e30, jnp.float32)
        l_s[...] = jnp.zeros(l_s.shape, jnp.float32)
        acc[...] = jnp.zeros(acc.shape, jnp.float32)

        def chain(first_row, n, pos, first_key, width, masked):
            rows = slice(first_row, first_row + n)
            keys = kv_ref[pos, first_key : first_key + width, 0:128]
            vals = kv_ref[pos, first_key : first_key + width, 128:256]
            s = lax.dot_general(
                qz[:, rows, :].reshape(2 * n, 256),
                jnp.concatenate([keys, keys], axis=1),
                (((1,), (1,)), ((), ())),
                preferred_element_type=jnp.float32,
            ).reshape(2, n, width)
            if masked:
                r = lax.broadcasted_iota(jnp.int32, (2, n, width), 1) + first_row
                k = lax.broadcasted_iota(jnp.int32, (2, n, width), 2) + first_key
                s = jnp.where(k <= r, s, -1e30)
            m_old = m_s[:, rows, :]
            m_new = jnp.maximum(m_old, jnp.max(s, axis=2, keepdims=True))
            alpha = jnp.exp2(m_old - m_new)
            p = jnp.exp2(s - jnp.tile(m_new, (1, 1, width // 128)))
            part = p[:, :, 0:128]
            for w in range(1, width // 128):
                part = part + p[:, :, w * 128 : (w + 1) * 128]
            l_s[:, rows, :] = l_s[:, rows, :] * alpha + part
            m_s[:, rows, :] = m_new
            pv = jnp.dot(
                p.astype(jnp.bfloat16).reshape(2 * n, width),
                vals,
                preferred_element_type=jnp.float32,
            )
            acc[:, rows, :] = acc[:, rows, :] * alpha + pv.reshape(2, n, 128)

        def body(kb, carry):
            pos = tab[kb]
            for j in range(ROWS // keys_at_once):
                chain(0, ROWS, pos, j * keys_at_once, keys_at_once, False)
            return carry

        lax.fori_loop(0, qb, body, 0)
        pos = tab[qb]
        for t in range(ROWS // 256):
            chain(t * 256, 256, pos, 0, 256 * (t + 1), True)
        denom = jnp.sum(l_s[...], axis=2, keepdims=True)
        diff = acc[0] / denom[0] - lam[0] * acc[1] / denom[1]
        mean_square = jnp.mean(diff * diff, axis=1, keepdims=True)
        normed = diff * lax.rsqrt(mean_square + 1e-5) * gain_ref[...].astype(jnp.float32)
        o_ref[...] = normed.astype(jnp.bfloat16)


def attention(tab, lam, q_a, q_b, kv, gain):
    rows = jax.ShapeDtypeStruct((ROWS, 128), jnp.bfloat16)
    full = pl.BlockSpec((ROWS, 128), lambda i, *_: (0, 0))
    return pl.pallas_call(
        attn_kernel,
        out_shape=(rows, rows),
        grid_spec=pltpu.PrefetchScalarGridSpec(
            num_scalar_prefetch=2,
            grid=(1,),
            in_specs=[
                full,
                full,
                pl.BlockSpec((16, ROWS, 256), lambda i, *_: (0, 0, 0)),
                pl.BlockSpec((1, 128), lambda i, *_: (0, 0)),
            ],
            out_specs=(full, full),
            scratch_shapes=[
                pltpu.VMEM((2, ROWS, 256), jnp.bfloat16),
                pltpu.VMEM((2, ROWS, 128), jnp.float32),
                pltpu.VMEM((2, ROWS, 128), jnp.float32),
                pltpu.VMEM((2, ROWS, 128), jnp.float32),
            ],
        ),
        compiler_params=pltpu.CompilerParams(vmem_limit_bytes=60 * 2**20),
        name="attn",
    )(tab, lam, q_a, q_b, kv, gain)


def out_kernel(first, conv_ref, a_ref, b_ref, wc_ref, wa_ref, o_ref):
    own = first[0] == 0
    zero_head = jnp.where(own, a_ref[...], b_ref[...])
    one_head = jnp.where(own, b_ref[...], a_ref[...])
    left = jnp.concatenate([conv_ref[...], zero_head, one_head], axis=1)
    right = jnp.concatenate([wc_ref[...], wa_ref[...]], axis=0)
    o_ref[...] = jnp.dot(left, right, preferred_element_type=jnp.float32).astype(jnp.bfloat16)


def out_projection(first, conv_out, back_a, back_b, w_conv, w_attn):
    width = 512
    head = pl.BlockSpec((ROWS, 128), lambda n, *_: (0, 0))
    weight = pl.BlockSpec((256, width), lambda n, *_: (0, n))
    return pl.pallas_call(
        out_kernel,
        out_shape=jax.ShapeDtypeStruct((ROWS, D), jnp.bfloat16),
        grid_spec=pltpu.PrefetchScalarGridSpec(
            num_scalar_prefetch=1,
            grid=(D // width,),
            in_specs=[
                pl.BlockSpec((ROWS, 256), lambda n, *_: (0, 0)),
                head,
                head,
                weight,
                weight,
            ],
            out_specs=pl.BlockSpec((ROWS, width), lambda n, *_: (0, n)),
        ),
        compiler_params=pltpu.CompilerParams(vmem_limit_bytes=40 * 2**20),
        name="out_projection",
    )(first, conv_out, back_a, back_b, w_conv, w_attn)


def total_over(value, axis, size):
    copies = jnp.broadcast_to(value, (size, *value.shape))
    everything = lax.all_to_all(copies, axis, split_axis=0, concat_axis=0, tiled=True)
    return jnp.sum(everything, axis=0)


def per_device(
    hidden_states,
    w_conv_b,
    w_conv_c,
    w_conv_h,
    conv_taps,
    w_query,
    w_key,
    w_value,
    lambdas,
    head_gain,
    w_out_conv,
    w_out_attn,
    out_gain,
):
    z = lax.axis_index("z")
    x = lax.axis_index("x")
    core = lax.axis_index("c")
    sp = z * 4 + x

    rim = lax.ppermute(
        hidden_states[ROWS - HALO :], ("z", "x"), [(i, i + 1) for i in range(15)]
    )
    other_lambdas = lax.ppermute(lambdas, "c", [(0, 1), (1, 0)])
    plane_lambdas = jnp.where(
        core == 0,
        jnp.concatenate([lambdas, other_lambdas]),
        jnp.concatenate([other_lambdas, lambdas]),
    )
    lam = lax.dynamic_slice_in_dim(plane_lambdas, z, 1)

    first = jnp.where(z < 2, 0, 1).astype(jnp.int32).reshape(1)
    _, _, start_cos, start_sin = rotary_tables()
    q_out, kv_out = project_qkv(
        first,
        hidden_states,
        w_query,
        w_key,
        w_value,
        lax.dynamic_slice_in_dim(jnp.asarray(start_cos), sp, 1, 0),
        lax.dynamic_slice_in_dim(jnp.asarray(start_sin), sp, 1, 0),
    )
    route_a, route_b = forward_route(0), forward_route(1)
    kv_a = lax.ppermute(kv_out[0], ("z", "c"), route_a)
    kv_b = lax.ppermute(kv_out[1], ("z", "c"), route_b)
    q_a = lax.ppermute(q_out[0], ("z", "c"), route_a)
    q_b = lax.ppermute(q_out[1], ("z", "c"), route_b)
    kv = lax.all_gather(jnp.stack([kv_a, kv_b]), ("x", "c"), axis=0, tiled=True)

    conv_out = gated_conv(hidden_states, rim, w_conv_b, w_conv_c, w_conv_h, conv_taps)

    even = (z % 2) == 0
    block = jnp.arange(16, dtype=jnp.int32)
    z_of, x_of = block // 4, block % 4
    core_of = jnp.asarray(CORE_OF_Z, jnp.int32)[z_of]
    round_of = jnp.where((z_of < 2) == even, 0, 1)
    place = (x_of * 2 + core_of) * 2 + round_of
    low_z = jnp.where(core == 0, 0, 1)
    high_z = jnp.where(core == 0, 3, 2)
    own = jnp.stack([jnp.where(even, low_z, high_z), jnp.where(even, high_z, low_z)]) * 4 + x
    tab = jnp.concatenate([place, own]).astype(jnp.int32)
    o_a, o_b = attention(tab, lam, q_a, q_b, kv, head_gain.reshape(1, VD))
    back_a = lax.ppermute(o_a, ("z", "c"), reverse(route_a))
    back_b = lax.ppermute(o_b, ("z", "c"), reverse(route_b))

    partial_value = out_projection(first, conv_out, back_a, back_b, w_out_conv, w_out_attn)
    summed = lax.psum_scatter(partial_value, ("y", "c"), scatter_dimension=1, tiled=True)
    mix_f = summed.astype(jnp.float32)
    width = mix_f.shape[1]
    sums = jnp.concatenate([jnp.sum(mix_f, axis=-1), jnp.sum(mix_f * mix_f, axis=-1)])
    totals = total_over(sums, ("y", "c"), 8)
    mean_value = (totals[:ROWS] / D)[:, None]
    variance = (totals[ROWS:] / D)[:, None] - mean_value * mean_value
    tp = lax.axis_index("y") * 2 + core
    own_gain = lax.dynamic_slice_in_dim(out_gain.astype(jnp.float32), tp * width, width, 0)
    return ((mix_f - mean_value) * lax.rsqrt(variance + 1e-05) * own_gain[None, :]).astype(
        jnp.bfloat16
    )


def solution(mesh):
    chips = Mesh(mesh.devices.reshape(4, 4, 4, 2), ("z", "x", "y", "c"))
    sp, tp = ("z", "x"), ("y", "c")
    return jax.shard_map(
        per_device,
        mesh=chips,
        in_specs=(
            P(sp, None),
            P(None, tp),
            P(None, tp),
            P(None, tp),
            P(None, tp),
            P(None, tp),
            P(None, tp),
            P(None, tp),
            P(tp),
            P(),
            P(tp, None),
            P(tp, None),
            P(),
        ),
        out_specs=P(sp, tp),
        check_vma=False,
    )
```

```python
import jax
import jax.numpy as jnp
import numpy as np
from jax import lax
from jax.experimental import pallas as pl
from jax.experimental.pallas import tpu as pltpu
from jax.sharding import Mesh
from jax.sharding import PartitionSpec as P

D = 4096
QK = 64
VD = 128
ROWS = 768
HALO = 16
LOG2E = 1.4426950408889634

CORE_OF_Z = (0, 1, 1, 0)


def forward_route(round_index):
    route = []
    for z in range(4):
        for c in range(2):
            local = round_index if z < 2 else 1 - round_index
            route.append((z * 2 + c, (2 * c + local) * 2 + CORE_OF_Z[z]))
    return route


def reverse(route):
    return [(b, a) for a, b in route]


def rotary_tables():
    inverse = 10000.0 ** (-np.arange(0, QK, 2, dtype=np.float64) / QK)
    inverse = np.tile(inverse, 128 // inverse.size)
    rows = np.arange(ROWS, dtype=np.float64)[:, None] * inverse
    starts = np.arange(16, dtype=np.float64)[:, None] * ROWS * inverse
    tables = (np.cos(rows), np.sin(rows), np.cos(starts), np.sin(starts))
    return tuple(t.astype(np.float32) for t in tables)


def qkv_kernel(first, h_ref, wq_ref, wk_ref, wv_ref, cr, sr, cs, ss, q_ref, kv_ref, acc):
    step = pl.program_id(0)

    @pl.when(step == 0)
    def _():
        acc[...] = jnp.zeros(acc.shape, jnp.float32)

    h = h_ref[...]
    for i, w_ref in enumerate((wk_ref, wv_ref, wq_ref)):
        acc[i] += jnp.dot(h, w_ref[...], preferred_element_type=jnp.float32)

    @pl.when(step == pl.num_programs(0) - 1)
    def _():
        cosine = cs[...] * cr[...] - ss[...] * sr[...]
        sine = ss[...] * cr[...] + cs[...] * sr[...]
        lane = lax.broadcasted_iota(jnp.int32, (ROWS, 128), 1)
        upper = (lane % QK) < QK // 2

        def rotated(x):
            x = x.astype(jnp.bfloat16).astype(jnp.float32)
            swapped = jnp.where(upper, -pltpu.roll(x, 128 - QK // 2, 1), pltpu.roll(x, QK // 2, 1))
            return (x * cosine + swapped * sine).astype(jnp.bfloat16)

        for local in range(2):
            cols = slice(local * 128, local * 128 + 128)
            at = first[0] if local == 0 else 1 - first[0]
            kv_ref[at, :, 0:128] = rotated(acc[0, :, cols])
            kv_ref[at, :, 128:256] = acc[1, :, cols].astype(jnp.bfloat16)
            q_ref[at] = rotated(acc[2, :, cols])


def project_qkv(first, hidden, w_query, w_key, w_value, start_cos, start_sin):
    chunk = 512
    row_cos, row_sin, _, _ = rotary_tables()
    weight = pl.BlockSpec((chunk, 256), lambda k, *_: (k, 0))
    table = pl.BlockSpec((ROWS, 128), lambda k, *_: (0, 0))
    one = pl.BlockSpec((1, 128), lambda k, *_: (0, 0))
    return pl.pallas_call(
        qkv_kernel,
        out_shape=(
            jax.ShapeDtypeStruct((2, ROWS, 128), jnp.bfloat16),
            jax.ShapeDtypeStruct((2, ROWS, 256), jnp.bfloat16),
        ),
        grid_spec=pltpu.PrefetchScalarGridSpec(
            num_scalar_prefetch=1,
            grid=(D // chunk,),
            in_specs=[
                pl.BlockSpec((ROWS, chunk), lambda k, *_: (0, k)),
                weight,
                weight,
                weight,
                table,
                table,
                one,
                one,
            ],
            out_specs=(
                pl.BlockSpec((2, ROWS, 128), lambda k, *_: (0, 0, 0)),
                pl.BlockSpec((2, ROWS, 256), lambda k, *_: (0, 0, 0)),
            ),
            scratch_shapes=[pltpu.VMEM((3, ROWS, 256), jnp.float32)],
        ),
        compiler_params=pltpu.CompilerParams(vmem_limit_bytes=60 * 2**20),
        cost_estimate=pl.CostEstimate(flops=2 * ROWS * D * 768, bytes_accessed=13 * 2**20, transcendentals=0),
        name="qkv",
    )(first, hidden, w_query, w_key, w_value, row_cos, row_sin, start_cos, start_sin)


def conv_kernel(h_ref, rim_ref, wb_ref, wc_ref, wh_ref, taps_ref, o_ref, acc, rim_acc, padded):
    step = pl.program_id(0)

    @pl.when(step == 0)
    def _():
        acc[...] = jnp.zeros(acc.shape, jnp.float32)
        rim_acc[...] = jnp.zeros(rim_acc.shape, jnp.float32)

    h = h_ref[...]
    rim = rim_ref[...]
    for i, w_ref in enumerate((wb_ref, wc_ref, wh_ref)):
        w = w_ref[...]
        acc[i] += jnp.dot(h, w, preferred_element_type=jnp.float32)
        rim_acc[i] += jnp.dot(rim, w, preferred_element_type=jnp.float32)

    @pl.when(step == pl.num_programs(0) - 1)
    def _():
        def once(x):
            return x.astype(jnp.bfloat16).astype(jnp.float32)

        padded[0:HALO] = once(rim_acc[1]) * once(rim_acc[2])
        padded[HALO:] = once(acc[1]) * once(acc[2])
        taps = taps_ref[...].astype(jnp.float32)
        conv = jnp.zeros((ROWS, 256), jnp.float32)
        for tap in range(3):
            conv = conv + taps[tap : tap + 1] * padded[HALO - 2 + tap : HALO - 2 + tap + ROWS]
        o_ref[...] = (once(acc[0]) * conv).astype(jnp.bfloat16)


def gated_conv(hidden, rim, w_b, w_c, w_h, taps):
    chunk = 512
    weight = pl.BlockSpec((chunk, 256), lambda k: (k, 0))
    return pl.pallas_call(
        conv_kernel,
        out_shape=jax.ShapeDtypeStruct((ROWS, 256), jnp.bfloat16),
        grid=(D // chunk,),
        in_specs=[
            pl.BlockSpec((ROWS, chunk), lambda k: (0, k)),
            pl.BlockSpec((HALO, chunk), lambda k: (0, k)),
            weight,
            weight,
            weight,
            pl.BlockSpec((3, 256), lambda k: (0, 0)),
        ],
        out_specs=pl.BlockSpec((ROWS, 256), lambda k: (0, 0)),
        scratch_shapes=[
            pltpu.VMEM((3, ROWS, 256), jnp.float32),
            pltpu.VMEM((3, HALO, 256), jnp.float32),
            pltpu.VMEM((HALO + ROWS, 256), jnp.float32),
        ],
        compiler_params=pltpu.CompilerParams(vmem_limit_bytes=60 * 2**20),
        cost_estimate=pl.CostEstimate(flops=2 * ROWS * D * 768, bytes_accessed=13 * 2**20, transcendentals=0),
        name="gated_conv",
    )(hidden, rim, w_b, w_c, w_h, taps)


def attn_kernel(tab, lam, qa_ref, qb_ref, kv_ref, gain_ref, _, oa_ref, ob_ref, qz, m_s, l_s, acc):
    keys_at_once = 256

    for i, (q_ref, o_ref) in enumerate(((qa_ref, oa_ref), (qb_ref, ob_ref))):
        qb = tab[16 + i]
        lane = lax.broadcasted_iota(jnp.int32, (ROWS, 128), 1)
        qf = q_ref[...].astype(jnp.float32) * (0.125 * LOG2E)
        high = qf.astype(jnp.bfloat16)
        low = (qf - high.astype(jnp.float32)).astype(jnp.bfloat16)
        for h, v in enumerate((high, low)):
            zero = jnp.zeros_like(v)
            qz[0, :, h * 128 : h * 128 + 128] = jnp.where(lane < QK, v, zero)
            qz[1, :, h * 128 : h * 128 + 128] = jnp.where(lane >= QK, v, zero)
        m_s[...] = jnp.full(m_s.shape, -1e30, jnp.float32)
        l_s[...] = jnp.zeros(l_s.shape, jnp.float32)
        acc[...] = jnp.zeros(acc.shape, jnp.float32)

        def chain(first_row, n, pos, first_key, width, masked):
            rows = slice(first_row, first_row + n)
            keys = kv_ref[pos, first_key : first_key + width, 0:128]
            vals = kv_ref[pos, first_key : first_key + width, 128:256]
            s = lax.dot_general(
                qz[:, rows, :].reshape(2 * n, 256),
                jnp.concatenate([keys, keys], axis=1),
                (((1,), (1,)), ((), ())),
                preferred_element_type=jnp.float32,
            ).reshape(2, n, width)
            if masked:
                r = lax.broadcasted_iota(jnp.int32, (2, n, width), 1) + first_row
                k = lax.broadcasted_iota(jnp.int32, (2, n, width), 2) + first_key
                s = jnp.where(k <= r, s, -1e30)
            m_old = m_s[:, rows, :]
            m_new = jnp.maximum(m_old, jnp.max(s, axis=2, keepdims=True))
            alpha = jnp.exp2(m_old - m_new)
            p = jnp.exp2(s - jnp.tile(m_new, (1, 1, width // 128)))
            part = p[:, :, 0:128]
            for w in range(1, width // 128):
                part = part + p[:, :, w * 128 : (w + 1) * 128]
            l_s[:, rows, :] = l_s[:, rows, :] * alpha + part
            m_s[:, rows, :] = m_new
            pv = jnp.dot(
                p.astype(jnp.bfloat16).reshape(2 * n, width),
                vals,
                preferred_element_type=jnp.float32,
            )
            acc[:, rows, :] = acc[:, rows, :] * alpha + pv.reshape(2, n, 128)

        def body(kb, carry):
            pos = tab[kb]
            for j in range(ROWS // keys_at_once):
                chain(0, ROWS, pos, j * keys_at_once, keys_at_once, False)
            return carry

        lax.fori_loop(0, qb, body, 0)
        pos = tab[qb]
        for t in range(ROWS // 256):
            chain(t * 256, 256, pos, 0, 256 * (t + 1), True)
        denom = jnp.sum(l_s[...], axis=2, keepdims=True)
        diff = acc[0] / denom[0] - lam[0] * acc[1] / denom[1]
        mean_square = jnp.mean(diff * diff, axis=1, keepdims=True)
        normed = diff * lax.rsqrt(mean_square + 1e-5) * gain_ref[...].astype(jnp.float32)
        o_ref[...] = normed.astype(jnp.bfloat16)


def attention(tab, lam, q_a, q_b, kv, gain, before):
    rows = jax.ShapeDtypeStruct((ROWS, 128), jnp.bfloat16)
    full = pl.BlockSpec((ROWS, 128), lambda i, *_: (0, 0))
    return pl.pallas_call(
        attn_kernel,
        out_shape=(rows, rows),
        grid_spec=pltpu.PrefetchScalarGridSpec(
            num_scalar_prefetch=2,
            grid=(1,),
            in_specs=[
                full,
                full,
                pl.BlockSpec((16, ROWS, 256), lambda i, *_: (0, 0, 0)),
                pl.BlockSpec((1, 128), lambda i, *_: (0, 0)),
                pl.BlockSpec(memory_space=pl.ANY),
            ],
            out_specs=(full, full),
            scratch_shapes=[
                pltpu.VMEM((2, ROWS, 256), jnp.bfloat16),
                pltpu.VMEM((2, ROWS, 128), jnp.float32),
                pltpu.VMEM((2, ROWS, 128), jnp.float32),
                pltpu.VMEM((2, ROWS, 128), jnp.float32),
            ],
        ),
        compiler_params=pltpu.CompilerParams(vmem_limit_bytes=60 * 2**20),
        cost_estimate=pl.CostEstimate(flops=40 * 10**9, bytes_accessed=8 * 2**20, transcendentals=0),
        name="attn",
    )(tab, lam, q_a, q_b, kv, gain, before)


def out_kernel(first, conv_ref, a_ref, b_ref, wc_ref, wa_ref, o_ref):
    own = first[0] == 0
    zero_head = jnp.where(own, a_ref[...], b_ref[...])
    one_head = jnp.where(own, b_ref[...], a_ref[...])
    left = jnp.concatenate([conv_ref[...], zero_head, one_head], axis=1)
    right = jnp.concatenate([wc_ref[...], wa_ref[...]], axis=0)
    o_ref[...] = jnp.dot(left, right, preferred_element_type=jnp.float32).astype(jnp.bfloat16)


def out_projection(first, conv_out, back_a, back_b, w_conv, w_attn):
    width = 512
    head = pl.BlockSpec((ROWS, 128), lambda n, *_: (0, 0))
    weight = pl.BlockSpec((256, width), lambda n, *_: (0, n))
    return pl.pallas_call(
        out_kernel,
        out_shape=jax.ShapeDtypeStruct((ROWS, D), jnp.bfloat16),
        grid_spec=pltpu.PrefetchScalarGridSpec(
            num_scalar_prefetch=1,
            grid=(D // width,),
            in_specs=[
                pl.BlockSpec((ROWS, 256), lambda n, *_: (0, 0)),
                head,
                head,
                weight,
                weight,
            ],
            out_specs=pl.BlockSpec((ROWS, width), lambda n, *_: (0, n)),
        ),
        compiler_params=pltpu.CompilerParams(vmem_limit_bytes=60 * 2**20),
        cost_estimate=pl.CostEstimate(flops=2 * ROWS * D * 512, bytes_accessed=11 * 2**20, transcendentals=0),
        name="out_projection",
    )(first, conv_out, back_a, back_b, w_conv, w_attn)


def total_over(value, axis, size):
    copies = jnp.broadcast_to(value, (size, *value.shape))
    everything = lax.all_to_all(copies, axis, split_axis=0, concat_axis=0, tiled=True)
    return jnp.sum(everything, axis=0)


def per_device(
    hidden_states,
    w_conv_b,
    w_conv_c,
    w_conv_h,
    conv_taps,
    w_query,
    w_key,
    w_value,
    lambdas,
    head_gain,
    w_out_conv,
    w_out_attn,
    out_gain,
):
    z = lax.axis_index("z")
    x = lax.axis_index("x")
    core = lax.axis_index("c")
    sp = z * 4 + x

    rim = lax.ppermute(
        hidden_states[ROWS - HALO :], ("z", "x"), [(i, i + 1) for i in range(15)]
    )
    other_lambdas = lax.ppermute(lambdas, "c", [(0, 1), (1, 0)])
    plane_lambdas = jnp.where(
        core == 0,
        jnp.concatenate([lambdas, other_lambdas]),
        jnp.concatenate([other_lambdas, lambdas]),
    )
    lam = lax.dynamic_slice_in_dim(plane_lambdas, z, 1)

    first = jnp.where(z < 2, 0, 1).astype(jnp.int32).reshape(1)
    _, _, start_cos, start_sin = rotary_tables()
    q_out, kv_out = project_qkv(
        first,
        hidden_states,
        w_query,
        w_key,
        w_value,
        lax.dynamic_slice_in_dim(jnp.asarray(start_cos), sp, 1, 0),
        lax.dynamic_slice_in_dim(jnp.asarray(start_sin), sp, 1, 0),
    )
    route_a, route_b = forward_route(0), forward_route(1)
    kv_a = lax.ppermute(kv_out[0], ("z", "c"), route_a)
    kv_b = lax.ppermute(kv_out[1], ("z", "c"), route_b)
    q_a = lax.ppermute(q_out[0], ("z", "c"), route_a)
    q_b = lax.ppermute(q_out[1], ("z", "c"), route_b)
    kv = lax.all_gather(jnp.stack([kv_a, kv_b]), ("x", "c"), axis=0, tiled=True)

    conv_out = gated_conv(hidden_states, rim, w_conv_b, w_conv_c, w_conv_h, conv_taps)

    even = (z % 2) == 0
    block = jnp.arange(16, dtype=jnp.int32)
    z_of, x_of = block // 4, block % 4
    core_of = jnp.asarray(CORE_OF_Z, jnp.int32)[z_of]
    round_of = jnp.where((z_of < 2) == even, 0, 1)
    place = (x_of * 2 + core_of) * 2 + round_of
    low_z = jnp.where(core == 0, 0, 1)
    high_z = jnp.where(core == 0, 3, 2)
    own = jnp.stack([jnp.where(even, low_z, high_z), jnp.where(even, high_z, low_z)]) * 4 + x
    tab = jnp.concatenate([place, own]).astype(jnp.int32)
    o_a, o_b = attention(tab, lam, q_a, q_b, kv, head_gain.reshape(1, VD), conv_out)
    back_a = lax.ppermute(o_a, ("z", "c"), reverse(route_a))
    back_b = lax.ppermute(o_b, ("z", "c"), reverse(route_b))

    partial_value = out_projection(first, conv_out, back_a, back_b, w_out_conv, w_out_attn)
    summed = lax.psum_scatter(partial_value, ("y", "c"), scatter_dimension=1, tiled=True)
    mix_f = summed.astype(jnp.float32)
    width = mix_f.shape[1]
    sums = jnp.concatenate([jnp.sum(mix_f, axis=-1), jnp.sum(mix_f * mix_f, axis=-1)])
    totals = total_over(sums, ("y", "c"), 8)
    mean_value = (totals[:ROWS] / D)[:, None]
    variance = (totals[ROWS:] / D)[:, None] - mean_value * mean_value
    tp = lax.axis_index("y") * 2 + core
    own_gain = lax.dynamic_slice_in_dim(out_gain.astype(jnp.float32), tp * width, width, 0)
    return ((mix_f - mean_value) * lax.rsqrt(variance + 1e-05) * own_gain[None, :]).astype(
        jnp.bfloat16
    )


def solution(mesh):
    chips = Mesh(mesh.devices.reshape(4, 4, 4, 2), ("z", "x", "y", "c"))
    sp, tp = ("z", "x"), ("y", "c")
    return jax.shard_map(
        per_device,
        mesh=chips,
        in_specs=(
            P(sp, None),
            P(None, tp),
            P(None, tp),
            P(None, tp),
            P(None, tp),
            P(None, tp),
            P(None, tp),
            P(None, tp),
            P(tp),
            P(),
            P(tp, None),
            P(tp, None),
            P(),
        ),
        out_specs=P(sp, tp),
        check_vma=False,
    )
```

```python
import jax
import jax.numpy as jnp
import numpy as np
from jax import lax
from jax.experimental import pallas as pl
from jax.experimental.pallas import tpu as pltpu
from jax.sharding import Mesh
from jax.sharding import PartitionSpec as P

D = 4096
QK = 64
VD = 128
ROWS = 768
HALO = 16
LOG2E = 1.4426950408889634

CORE_OF_Z = (0, 1, 1, 0)


def forward_route(round_index):
    route = []
    for z in range(4):
        for c in range(2):
            local = round_index if z < 2 else 1 - round_index
            route.append((z * 2 + c, (2 * c + local) * 2 + CORE_OF_Z[z]))
    return route


def reverse(route):
    return [(b, a) for a, b in route]


def rotary_tables():
    inverse = 10000.0 ** (-np.arange(0, QK, 2, dtype=np.float64) / QK)
    inverse = np.tile(inverse, 128 // inverse.size)
    rows = np.arange(ROWS, dtype=np.float64)[:, None] * inverse
    starts = np.arange(16, dtype=np.float64)[:, None] * ROWS * inverse
    tables = (np.cos(rows), np.sin(rows), np.cos(starts), np.sin(starts))
    return tuple(t.astype(np.float32) for t in tables)


CHUNK = 1024
STEPS = D // CHUNK
AHEAD = 3


def streamed_products(pairs, sem, accs):
    copies = []
    for hbm, buf, by_columns in pairs:
        slot = len(copies)

        def copy(k, hbm=hbm, buf=buf, by_columns=by_columns, slot=slot):
            at = pl.ds(k * CHUNK, CHUNK)
            source = hbm.at[:, at] if by_columns else hbm.at[at, :]
            return pltpu.make_async_copy(source, buf.at[k], sem.at[slot, k])

        copies.append(copy)
    for k in range(AHEAD):
        for copy in copies:
            copy(k).start()
    for acc, _, _ in accs:
        acc[...] = jnp.zeros(acc.shape, jnp.float32)

    def step(k, carry):
        @pl.when(k + AHEAD < STEPS)
        def _():
            for copy in copies:
                copy(k + AHEAD).start()

        for copy in copies:
            copy(k).wait()
        for acc, lhs, weights in accs:
            h = lhs[k]
            for i, w in enumerate(weights):
                acc[i] += jnp.dot(h, w[k], preferred_element_type=jnp.float32)
        return carry

    lax.fori_loop(0, STEPS, step, 0)


def qkv_kernel(
    first, h_ref, wk_ref, wv_ref, wq_ref, cr, sr, cs, ss, q_ref, kv_ref, acc, hb, kb, vb, qb, sem
):
    streamed_products(
        ((h_ref, hb, True), (wk_ref, kb, False), (wv_ref, vb, False), (wq_ref, qb, False)),
        sem,
        ((acc, hb, (kb, vb, qb)),),
    )
    cosine = cs[...] * cr[...] - ss[...] * sr[...]
    sine = ss[...] * cr[...] + cs[...] * sr[...]
    lane = lax.broadcasted_iota(jnp.int32, (ROWS, 128), 1)
    upper = (lane % QK) < QK // 2

    def rotated(x):
        x = x.astype(jnp.bfloat16).astype(jnp.float32)
        swapped = jnp.where(upper, -pltpu.roll(x, 128 - QK // 2, 1), pltpu.roll(x, QK // 2, 1))
        return (x * cosine + swapped * sine).astype(jnp.bfloat16)

    for local in range(2):
        cols = slice(local * 128, local * 128 + 128)
        at = first[0] if local == 0 else 1 - first[0]
        kv_ref[at, :, 0:128] = rotated(acc[0, :, cols])
        kv_ref[at, :, 128:256] = acc[1, :, cols].astype(jnp.bfloat16)
        q_ref[at] = rotated(acc[2, :, cols])


def in_hbm():
    return pl.BlockSpec(memory_space=pl.ANY)


def stream_buffers(weights, rim):
    rows = [pltpu.VMEM((STEPS, ROWS, CHUNK), jnp.bfloat16)]
    if rim:
        rows.append(pltpu.VMEM((STEPS, HALO, CHUNK), jnp.bfloat16))
    return (
        rows
        + [pltpu.VMEM((STEPS, CHUNK, 256), jnp.bfloat16)] * weights
        + [pltpu.SemaphoreType.DMA((weights + len(rows), STEPS))]
    )


def project_qkv(first, hidden, w_query, w_key, w_value, start_cos, start_sin):
    row_cos, row_sin, _, _ = rotary_tables()
    table = pl.BlockSpec((ROWS, 128), lambda k, *_: (0, 0))
    one = pl.BlockSpec((1, 128), lambda k, *_: (0, 0))
    return pl.pallas_call(
        qkv_kernel,
        out_shape=(
            jax.ShapeDtypeStruct((2, ROWS, 128), jnp.bfloat16),
            jax.ShapeDtypeStruct((2, ROWS, 256), jnp.bfloat16),
        ),
        grid_spec=pltpu.PrefetchScalarGridSpec(
            num_scalar_prefetch=1,
            grid=(1,),
            in_specs=[in_hbm(), in_hbm(), in_hbm(), in_hbm(), table, table, one, one],
            out_specs=(
                pl.BlockSpec((2, ROWS, 128), lambda k, *_: (0, 0, 0)),
                pl.BlockSpec((2, ROWS, 256), lambda k, *_: (0, 0, 0)),
            ),
            scratch_shapes=[pltpu.VMEM((3, ROWS, 256), jnp.float32), *stream_buffers(3, False)],
        ),
        compiler_params=pltpu.CompilerParams(vmem_limit_bytes=60 * 2**20),
        cost_estimate=pl.CostEstimate(
            flops=2 * ROWS * D * 768, bytes_accessed=13 * 2**20, transcendentals=0
        ),
        name="qkv",
    )(first, hidden, w_key, w_value, w_query, row_cos, row_sin, start_cos, start_sin)


def conv_kernel(
    h_ref, rim_ref, wb_ref, wc_ref, wh_ref, taps_ref, o_ref, acc, rim_acc, padded, hb, rb, b, c, h, sem
):
    streamed_products(
        (
            (h_ref, hb, True),
            (rim_ref, rb, True),
            (wb_ref, b, False),
            (wc_ref, c, False),
            (wh_ref, h, False),
        ),
        sem,
        ((acc, hb, (b, c, h)), (rim_acc, rb, (b, c, h))),
    )

    def once(x):
        return x.astype(jnp.bfloat16).astype(jnp.float32)

    padded[0:HALO] = once(rim_acc[1]) * once(rim_acc[2])
    padded[HALO:] = once(acc[1]) * once(acc[2])
    taps = taps_ref[...].astype(jnp.float32)
    conv = jnp.zeros((ROWS, 256), jnp.float32)
    for tap in range(3):
        conv = conv + taps[tap : tap + 1] * padded[HALO - 2 + tap : HALO - 2 + tap + ROWS]
    o_ref[...] = (once(acc[0]) * conv).astype(jnp.bfloat16)


def gated_conv(hidden, rim, w_b, w_c, w_h, taps):
    return pl.pallas_call(
        conv_kernel,
        out_shape=jax.ShapeDtypeStruct((ROWS, 256), jnp.bfloat16),
        grid=(1,),
        in_specs=[
            in_hbm(),
            in_hbm(),
            in_hbm(),
            in_hbm(),
            in_hbm(),
            pl.BlockSpec((3, 256), lambda k: (0, 0)),
        ],
        out_specs=pl.BlockSpec((ROWS, 256), lambda k: (0, 0)),
        scratch_shapes=[
            pltpu.VMEM((3, ROWS, 256), jnp.float32),
            pltpu.VMEM((3, HALO, 256), jnp.float32),
            pltpu.VMEM((HALO + ROWS, 256), jnp.float32),
            *stream_buffers(3, True),
        ],
        compiler_params=pltpu.CompilerParams(vmem_limit_bytes=60 * 2**20),
        cost_estimate=pl.CostEstimate(
            flops=2 * ROWS * D * 768, bytes_accessed=13 * 2**20, transcendentals=0
        ),
        name="gated_conv",
    )(hidden, rim, w_b, w_c, w_h, taps)


KEYS_AT_ONCE = 256


def split_query(q_ref, qz):
    lane = lax.broadcasted_iota(jnp.int32, (ROWS, 128), 1)
    qf = q_ref[...].astype(jnp.float32) * (0.125 * LOG2E)
    high = qf.astype(jnp.bfloat16)
    low = (qf - high.astype(jnp.float32)).astype(jnp.bfloat16)
    for h, v in enumerate((high, low)):
        zero = jnp.zeros_like(v)
        qz[0, :, h * 128 : h * 128 + 128] = jnp.where(lane < QK, v, zero)
        qz[1, :, h * 128 : h * 128 + 128] = jnp.where(lane >= QK, v, zero)


def start_state(m_s, l_s, acc):
    m_s[...] = jnp.full(m_s.shape, -1e30, jnp.float32)
    l_s[...] = jnp.zeros(l_s.shape, jnp.float32)
    acc[...] = jnp.zeros(acc.shape, jnp.float32)


def attend(qz, kv_ref, m_s, l_s, acc, first_row, n, place, first_key, width, masked):
    rows = slice(first_row, first_row + n)
    keys = kv_ref[place, first_key : first_key + width, 0:128]
    vals = kv_ref[place, first_key : first_key + width, 128:256]
    s = lax.dot_general(
        qz[:, rows, :].reshape(2 * n, 256),
        jnp.concatenate([keys, keys], axis=1),
        (((1,), (1,)), ((), ())),
        preferred_element_type=jnp.float32,
    ).reshape(2, n, width)
    if masked:
        r = lax.broadcasted_iota(jnp.int32, (2, n, width), 1) + first_row
        k = lax.broadcasted_iota(jnp.int32, (2, n, width), 2) + first_key
        s = jnp.where(k <= r, s, -1e30)
    m_old = m_s[:, rows, :]
    m_new = jnp.maximum(m_old, jnp.max(s, axis=2, keepdims=True))
    alpha = jnp.exp2(m_old - m_new)
    p = jnp.exp2(s - jnp.tile(m_new, (1, 1, width // 128)))
    part = p[:, :, 0:128]
    for w in range(1, width // 128):
        part = part + p[:, :, w * 128 : (w + 1) * 128]
    l_s[:, rows, :] = l_s[:, rows, :] * alpha + part
    m_s[:, rows, :] = m_new
    pv = jnp.dot(
        p.astype(jnp.bfloat16).reshape(2 * n, width), vals, preferred_element_type=jnp.float32
    )
    acc[:, rows, :] = acc[:, rows, :] * alpha + pv.reshape(2, n, 128)


def attend_blocks(first, last, place_of, refs):
    def body(kb, carry):
        place = place_of(kb)
        for j in range(ROWS // KEYS_AT_ONCE):
            attend(*refs, 0, ROWS, place, j * KEYS_AT_ONCE, KEYS_AT_ONCE, False)
        return carry

    lax.fori_loop(first, last, body, 0)


def attend_diagonal(place, refs):
    for t in range(ROWS // 256):
        attend(*refs, t * 256, 256, place, 0, 256 * (t + 1), True)


def finish(lam, gain_ref, o_ref, l_s, acc):
    denom = jnp.sum(l_s[...], axis=2, keepdims=True)
    diff = acc[0] / denom[0] - lam[0] * acc[1] / denom[1]
    mean_square = jnp.mean(diff * diff, axis=1, keepdims=True)
    normed = diff * lax.rsqrt(mean_square + 1e-5) * gain_ref[...].astype(jnp.float32)
    o_ref[...] = normed.astype(jnp.bfloat16)


def low_place(kb):
    return (kb % 4) * 2 + kb // 4


def high_place(kb):
    return (kb % 4) * 2 + 3 - kb // 4


def low_kernel(own, lam, ql_ref, qh_ref, kv_ref, gain_ref, _, o_ref, m_o, l_o, a_o, qz, m_s, l_s, acc):
    split_query(ql_ref, qz)
    start_state(m_s, l_s, acc)
    refs = (qz, kv_ref, m_s, l_s, acc)
    attend_blocks(0, own[0], low_place, refs)
    attend_diagonal(low_place(own[0]), refs)
    finish(lam, gain_ref, o_ref, l_s, acc)
    split_query(qh_ref, qz)
    start_state(m_o, l_o, a_o)
    attend_blocks(0, 8, low_place, (qz, kv_ref, m_o, l_o, a_o))


def high_kernel(own, lam, qh_ref, kv_ref, gain_ref, m_i, l_i, a_i, _, __, o_ref, qz, m_s, l_s, acc):
    split_query(qh_ref, qz)
    m_s[...] = m_i[...]
    l_s[...] = l_i[...]
    acc[...] = a_i[...]
    refs = (qz, kv_ref, m_s, l_s, acc)
    attend_blocks(8, own[1], high_place, refs)
    attend_diagonal(high_place(own[1]), refs)
    finish(lam, gain_ref, o_ref, l_s, acc)


def attention_call(kernel, name, args, outs, unread, blocks):
    def full(shape):
        return pl.BlockSpec(shape, lambda i, *_: (0,) * len(shape))

    return pl.pallas_call(
        kernel,
        out_shape=outs,
        grid_spec=pltpu.PrefetchScalarGridSpec(
            num_scalar_prefetch=2,
            grid=(1,),
            in_specs=[full(a.shape) for a in args[2:]] + [in_hbm() for _ in unread],
            out_specs=tuple(full(o.shape) for o in outs),
            scratch_shapes=[
                pltpu.VMEM((2, ROWS, 256), jnp.bfloat16),
                pltpu.VMEM((2, ROWS, 128), jnp.float32),
                pltpu.VMEM((2, ROWS, 128), jnp.float32),
                pltpu.VMEM((2, ROWS, 128), jnp.float32),
            ],
        ),
        compiler_params=pltpu.CompilerParams(vmem_limit_bytes=60 * 2**20),
        cost_estimate=pl.CostEstimate(
            flops=blocks * 2 * 10**9, bytes_accessed=4 * 2**20, transcendentals=0
        ),
        name=name,
    )(*args, *unread)


def whole_kernel(x_ref, w_ref, *rest):
    before, outs = (rest[0], rest[1:]) if len(rest) == 3 else (None, rest)
    blocks = jnp.concatenate([x_ref[t] for t in range(8)], axis=1)
    total = jnp.dot(blocks, w_ref[...], preferred_element_type=jnp.float32)
    if before is None:
        outs[0][...] = total
        return
    mix = (before[...] + total).astype(jnp.bfloat16)
    outs[0][...] = mix
    wide = mix.astype(jnp.float32)
    square = wide * wide
    high = square.astype(jnp.bfloat16)
    low = (square - high.astype(jnp.float32)).astype(jnp.bfloat16)
    ones = jnp.ones((8, mix.shape[1]), jnp.bfloat16)

    def row_sums(values):
        return lax.dot_general(
            ones, values, (((1,), (1,)), ((), ())), preferred_element_type=jnp.float32
        )

    for copy in range(8):
        outs[1][copy, 0:1] = row_sums(mix)[0:1]
        outs[1][copy, 1:2] = (row_sums(high) + row_sums(low))[0:1]


def whole_product(gathered, weight, before=None):
    width = weight.shape[1]
    last = before is not None
    full = jax.ShapeDtypeStruct((ROWS, width), jnp.bfloat16 if last else jnp.float32)
    sums = jax.ShapeDtypeStruct((8, 2, ROWS), jnp.float32)
    args = (gathered, weight) + ((before,) if last else ())
    return pl.pallas_call(
        whole_kernel,
        out_shape=(full, sums) if last else (full,),
        compiler_params=pltpu.CompilerParams(vmem_limit_bytes=(30 if last else 60) * 2**20),
        cost_estimate=pl.CostEstimate(
            flops=2 * ROWS * 2048 * width, bytes_accessed=7 * 2**20, transcendentals=0
        ),
        name="whole_last" if last else "whole_conv",
    )(*args)


def per_device(
    hidden_states,
    w_conv_b,
    w_conv_c,
    w_conv_h,
    conv_taps,
    w_query,
    w_key,
    w_value,
    lambdas,
    head_gain,
    w_out_conv,
    w_out_attn,
    out_gain,
):
    z = lax.axis_index("z")
    x = lax.axis_index("x")
    core = lax.axis_index("c")
    sp = z * 4 + x

    def columns(weight):
        return lax.all_to_all(weight, ("y", "c"), split_axis=1, concat_axis=0, tiled=True)

    w_conv_columns, w_attn_columns = columns(w_out_conv), columns(w_out_attn)
    rim = lax.ppermute(
        hidden_states[ROWS - HALO :], ("z", "x"), [(i, i + 1) for i in range(15)]
    )
    other_lambdas = lax.ppermute(lambdas, "c", [(0, 1), (1, 0)])
    plane_lambdas = jnp.where(
        core == 0,
        jnp.concatenate([lambdas, other_lambdas]),
        jnp.concatenate([other_lambdas, lambdas]),
    )
    lam = lax.dynamic_slice_in_dim(plane_lambdas, z, 1)

    first = jnp.where(z < 2, 0, 1).astype(jnp.int32).reshape(1)
    _, _, start_cos, start_sin = rotary_tables()
    q_out, kv_out = project_qkv(
        first,
        hidden_states,
        w_query,
        w_key,
        w_value,
        lax.dynamic_slice_in_dim(jnp.asarray(start_cos), sp, 1, 0),
        lax.dynamic_slice_in_dim(jnp.asarray(start_sin), sp, 1, 0),
    )
    route_a, route_b = forward_route(0), forward_route(1)
    kv_a = lax.ppermute(kv_out[0], ("z", "c"), route_a)
    kv_b = lax.ppermute(kv_out[1], ("z", "c"), route_b)
    q_a = lax.ppermute(q_out[0], ("z", "c"), route_a)
    q_b = lax.ppermute(q_out[1], ("z", "c"), route_b)
    even = (z % 2) == 0

    def low_high(a, b):
        return jnp.where(even, a, b), jnp.where(even, b, a)

    kv_low, kv_high = low_high(kv_a, kv_b)
    kv_low = lax.all_gather(kv_low, ("x", "c"), axis=0)
    kv_high = lax.all_gather(kv_high, ("x", "c"), axis=0)

    conv_out = gated_conv(hidden_states, rim, w_conv_b, w_conv_c, w_conv_h, conv_taps)
    conv_all = lax.all_gather(conv_out, ("y", "c"), axis=0)
    (conv_part,) = whole_product(conv_all, w_conv_columns)

    q_low, q_high = low_high(q_a, q_b)
    own_z = jnp.stack([jnp.where(core == 0, 0, 1), jnp.where(core == 0, 3, 2)])
    own = (own_z * 4 + x).astype(jnp.int32)
    gain = head_gain.reshape(1, VD)
    rows = jax.ShapeDtypeStruct((ROWS, VD), jnp.bfloat16)
    state = (jax.ShapeDtypeStruct((2, ROWS, VD), jnp.float32),) * 3
    o_low, *carried = attention_call(
        low_kernel, "attn_low", (own, lam, q_low, q_high, kv_low, gain), (rows, *state), (conv_out,), 12
    )
    (o_high,) = attention_call(
        high_kernel,
        "attn_high",
        (own, lam, q_high, kv_high, gain, *carried),
        (rows,),
        (w_conv_columns, w_attn_columns),
        6,
    )
    o_a, o_b = low_high(o_low, o_high)
    back_a = lax.ppermute(o_a, ("z", "c"), reverse(route_a))
    back_b = lax.ppermute(o_b, ("z", "c"), reverse(route_b))

    own_lane = first[0] == 0
    attn_out = jnp.concatenate(
        [jnp.where(own_lane, back_a, back_b), jnp.where(own_lane, back_b, back_a)], axis=1
    )
    attn_all = lax.all_gather(attn_out, ("y", "c"), axis=0)
    mix, sums = whole_product(attn_all, w_attn_columns, conv_part)
    everything = lax.all_to_all(sums, ("y", "c"), split_axis=0, concat_axis=0, tiled=True)
    totals = jnp.sum(everything, axis=0)
    mix_f = mix.astype(jnp.float32)
    width = mix_f.shape[1]
    mean_value = (totals[0] / D)[:, None]
    variance = (totals[1] / D)[:, None] - mean_value * mean_value
    tp = lax.axis_index("y") * 2 + core
    own_gain = lax.dynamic_slice_in_dim(out_gain.astype(jnp.float32), tp * width, width, 0)
    return ((mix_f - mean_value) * lax.rsqrt(variance + 1e-05) * own_gain[None, :]).astype(
        jnp.bfloat16
    )


def solution(mesh):
    chips = Mesh(mesh.devices.reshape(4, 4, 4, 2), ("z", "x", "y", "c"))
    sp, tp = ("z", "x"), ("y", "c")
    return jax.shard_map(
        per_device,
        mesh=chips,
        in_specs=(
            P(sp, None),
            P(None, tp),
            P(None, tp),
            P(None, tp),
            P(None, tp),
            P(None, tp),
            P(None, tp),
            P(None, tp),
            P(tp),
            P(),
            P(tp, None),
            P(tp, None),
            P(),
        ),
        out_specs=P(sp, tp),
        check_vma=False,
    )
```

```python
import jax
import jax.numpy as jnp
import numpy as np
from jax import lax
from jax.experimental import pallas as pl
from jax.experimental.pallas import tpu as pltpu
from jax.sharding import Mesh
from jax.sharding import PartitionSpec as P

D = 4096
QK = 64
VD = 128
ROWS = 768
HALO = 16

CORE_OF_Z = (0, 1, 1, 0)


def forward_route(round_index):
    route = []
    for z in range(4):
        for c in range(2):
            local = round_index if z < 2 else 1 - round_index
            route.append((z * 2 + c, (2 * c + local) * 2 + CORE_OF_Z[z]))
    return route


def reverse(route):
    return [(b, a) for a, b in route]


GROUP = 64


def rotary_tables():
    inverse = 10000.0 ** (-np.arange(0, QK, 2, dtype=np.float64) / QK)
    inverse = np.tile(inverse, 128 // inverse.size)
    rows = np.arange(GROUP, dtype=np.float64)[:, None] * inverse
    starts = np.arange(0, 16 * ROWS, GROUP, dtype=np.float64)[:, None] * inverse
    tables = (np.cos(rows), np.sin(rows), np.cos(starts), np.sin(starts))
    return tuple(t.astype(np.float32) for t in tables)


CHUNK = 1024
STEPS = D // CHUNK
AHEAD = 3


def streamed_products(pairs, sem, accs):
    copies = []
    for hbm, buf, by_columns in pairs:
        slot = len(copies)

        def copy(k, hbm=hbm, buf=buf, by_columns=by_columns, slot=slot):
            at = pl.ds(k * CHUNK, CHUNK)
            source = hbm.at[:, at] if by_columns else hbm.at[at, :]
            return pltpu.make_async_copy(source, buf.at[k], sem.at[slot, k])

        copies.append(copy)
    for k in range(AHEAD):
        for copy in copies:
            copy(k).start()
    for acc, _, _ in accs:
        acc[...] = jnp.zeros(acc.shape, jnp.float32)

    def step(k, carry):
        @pl.when(k + AHEAD < STEPS)
        def _():
            for copy in copies:
                copy(k + AHEAD).start()

        for copy in copies:
            copy(k).wait()
        for acc, lhs, weights in accs:
            h = lhs[k]
            for i, w in enumerate(weights):
                acc[i] += jnp.dot(h, w[k], preferred_element_type=jnp.float32)
        return carry

    lax.fori_loop(0, STEPS, step, 0)


def qkv_kernel(
    first, h_ref, wk_ref, wv_ref, wq_ref, cr, sr, cs, ss, qa_ref, qb_ref, kva_ref, kvb_ref, acc, hb, kb, vb, qb, sem
):
    streamed_products(
        ((h_ref, hb, True), (wk_ref, kb, False), (wv_ref, vb, False), (wq_ref, qb, False)),
        sem,
        ((acc, hb, (kb, vb, qb)),),
    )
    groups = range(ROWS // GROUP)
    cosine = jnp.concatenate(
        [cs[g : g + 1] * cr[...] - ss[g : g + 1] * sr[...] for g in groups], axis=0
    )
    sine = jnp.concatenate(
        [ss[g : g + 1] * cr[...] + cs[g : g + 1] * sr[...] for g in groups], axis=0
    )
    lane = lax.broadcasted_iota(jnp.int32, (ROWS, 128), 1)
    upper = (lane % QK) < QK // 2

    def rotated(x):
        x = x.astype(jnp.bfloat16).astype(jnp.float32)
        swapped = jnp.where(upper, -pltpu.roll(x, 128 - QK // 2, 1), pltpu.roll(x, QK // 2, 1))
        return (x * cosine + swapped * sine).astype(jnp.bfloat16)

    keys = [rotated(acc[0, :, i * 128 : i * 128 + 128]) for i in range(2)]
    vals = [acc[1, :, i * 128 : i * 128 + 128].astype(jnp.bfloat16) for i in range(2)]
    queries = [rotated(acc[2, :, i * 128 : i * 128 + 128]) for i in range(2)]
    for flip, q_ref, kv_ref in ((0, qa_ref, kva_ref), (1, qb_ref, kvb_ref)):
        take = first[0] == flip
        kv_ref[:, 0:128] = jnp.where(take, keys[0], keys[1])
        kv_ref[:, 128:256] = jnp.where(take, vals[0], vals[1])
        q_ref[...] = jnp.where(take, queries[0], queries[1])


def in_hbm():
    return pl.BlockSpec(memory_space=pltpu.HBM)


def stream_buffers(weights, rim):
    rows = [pltpu.VMEM((STEPS, ROWS, CHUNK), jnp.bfloat16)]
    if rim:
        rows.append(pltpu.VMEM((STEPS, HALO, CHUNK), jnp.bfloat16))
    return (
        rows
        + [pltpu.VMEM((STEPS, CHUNK, 256), jnp.bfloat16)] * weights
        + [pltpu.SemaphoreType.DMA((weights + len(rows), STEPS))]
    )


def project_qkv(first, hidden, w_query, w_key, w_value, start_cos, start_sin):
    row_cos, row_sin, _, _ = rotary_tables()
    table = pl.BlockSpec((GROUP, 128), lambda k, *_: (0, 0))
    one = pl.BlockSpec((ROWS // GROUP, 128), lambda k, *_: (0, 0))
    return pl.pallas_call(
        qkv_kernel,
        out_shape=tuple(
            jax.ShapeDtypeStruct((ROWS, width), jnp.bfloat16) for width in (128, 128, 256, 256)
        ),
        grid_spec=pltpu.PrefetchScalarGridSpec(
            num_scalar_prefetch=1,
            grid=(1,),
            in_specs=[in_hbm(), in_hbm(), in_hbm(), in_hbm(), table, table, one, one],
            out_specs=tuple(
                pl.BlockSpec((ROWS, width), lambda k, *_: (0, 0)) for width in (128, 128, 256, 256)
            ),
            scratch_shapes=[pltpu.VMEM((3, ROWS, 256), jnp.float32), *stream_buffers(3, False)],
        ),
        compiler_params=pltpu.CompilerParams(vmem_limit_bytes=60 * 2**20),
        cost_estimate=pl.CostEstimate(
            flops=2 * ROWS * D * 768, bytes_accessed=13 * 2**20, transcendentals=0
        ),
        name="qkv",
    )(first, hidden, w_key, w_value, w_query, row_cos, row_sin, start_cos, start_sin)


def conv_kernel(
    h_ref, rim_ref, wb_ref, wc_ref, wh_ref, taps_ref, o_ref, acc, rim_acc, padded, hb, rb, b, c, h, sem
):
    streamed_products(
        (
            (h_ref, hb, True),
            (rim_ref, rb, True),
            (wb_ref, b, False),
            (wc_ref, c, False),
            (wh_ref, h, False),
        ),
        sem,
        ((acc, hb, (b, c, h)), (rim_acc, rb, (b, c, h))),
    )

    def once(x):
        return x.astype(jnp.bfloat16).astype(jnp.float32)

    padded[0:HALO] = once(rim_acc[1]) * once(rim_acc[2])
    padded[HALO:] = once(acc[1]) * once(acc[2])
    taps = taps_ref[...].astype(jnp.float32)
    conv = jnp.zeros((ROWS, 256), jnp.float32)
    for tap in range(3):
        conv = conv + taps[tap : tap + 1] * padded[HALO - 2 + tap : HALO - 2 + tap + ROWS]
    o_ref[...] = (once(acc[0]) * conv).astype(jnp.bfloat16)


def gated_conv(hidden, rim, w_b, w_c, w_h, taps):
    return pl.pallas_call(
        conv_kernel,
        out_shape=jax.ShapeDtypeStruct((ROWS, 256), jnp.bfloat16),
        grid=(1,),
        in_specs=[
            in_hbm(),
            in_hbm(),
            in_hbm(),
            in_hbm(),
            in_hbm(),
            pl.BlockSpec((3, 256), lambda k: (0, 0)),
        ],
        out_specs=pl.BlockSpec((ROWS, 256), lambda k: (0, 0)),
        scratch_shapes=[
            pltpu.VMEM((3, ROWS, 256), jnp.float32),
            pltpu.VMEM((3, HALO, 256), jnp.float32),
            pltpu.VMEM((HALO + ROWS, 256), jnp.float32),
            *stream_buffers(3, True),
        ],
        compiler_params=pltpu.CompilerParams(vmem_limit_bytes=60 * 2**20),
        cost_estimate=pl.CostEstimate(
            flops=2 * ROWS * D * 768, bytes_accessed=13 * 2**20, transcendentals=0
        ),
        name="gated_conv",
    )(hidden, rim, w_b, w_c, w_h, taps)


KEYS_AT_ONCE = 256


def split_maps(q, qz):
    lane = lax.broadcasted_iota(jnp.int32, (ROWS, 128), 1)
    q = q * jnp.bfloat16(0.125)
    qz[0] = jnp.where(lane < QK, q, jnp.zeros_like(q))
    qz[1] = jnp.where(lane >= QK, q, jnp.zeros_like(q))


def start_state(m_s, l_s, acc):
    m_s[...] = jnp.full(m_s.shape, -1e30, jnp.float32)
    l_s[...] = jnp.zeros(l_s.shape, jnp.float32)
    acc[...] = jnp.zeros(acc.shape, jnp.float32)


def attend(qz, kv_ref, m_s, l_s, acc, first_row, n, place, first_key, width, masked):
    rows = slice(first_row, first_row + n)
    keys = kv_ref[place, first_key : first_key + width, 0:128]
    vals = kv_ref[place, first_key : first_key + width, 128:256]
    s = lax.dot_general(
        qz[:, rows, :].reshape(2 * n, 128),
        keys,
        (((1,), (1,)), ((), ())),
        preferred_element_type=jnp.float32,
    ).reshape(2, n, width)
    if masked:
        r = lax.broadcasted_iota(jnp.int32, (2, n, width), 1) + first_row
        k = lax.broadcasted_iota(jnp.int32, (2, n, width), 2) + first_key
        s = jnp.where(k <= r, s, -1e30)
    m_old = m_s[:, rows, :]
    m_new = jnp.maximum(m_old, jnp.max(s, axis=2, keepdims=True))
    alpha = jnp.exp(m_old - m_new)
    p = jnp.exp(s - jnp.tile(m_new, (1, 1, width // 128)))
    part = p[:, :, 0:128]
    for w in range(1, width // 128):
        part = part + p[:, :, w * 128 : (w + 1) * 128]
    l_s[:, rows, :] = l_s[:, rows, :] * alpha + part
    m_s[:, rows, :] = m_new
    pv = jnp.dot(
        p.astype(jnp.bfloat16).reshape(2 * n, width), vals, preferred_element_type=jnp.float32
    )
    acc[:, rows, :] = acc[:, rows, :] * alpha + pv.reshape(2, n, 128)


def attend_blocks(first, count, place_of, refs):
    def block(kb):
        place = place_of(kb)
        for j in range(ROWS // KEYS_AT_ONCE):
            attend(*refs, 0, ROWS, place, j * KEYS_AT_ONCE, KEYS_AT_ONCE, False)

    def body(pair, carry):
        block(first + 2 * pair)
        block(first + 2 * pair + 1)
        return carry

    lax.fori_loop(0, count // 2, body, 0)

    @pl.when(count % 2 == 1)
    def _():
        block(first + count - 1)


def attend_diagonal(place, refs):
    for t in range(ROWS // 256):
        attend(*refs, t * 256, 256, place, 0, 256 * (t + 1), True)


def finish(lam, gain_ref, l_s, acc):
    denom = jnp.sum(l_s[...], axis=2, keepdims=True)
    diff = acc[0] / denom[0] - lam[0] * acc[1] / denom[1]
    mean_square = jnp.mean(diff * diff, axis=1, keepdims=True)
    normed = diff * lax.rsqrt(mean_square + 1e-5) * gain_ref[...].astype(jnp.float32)
    return normed.astype(jnp.bfloat16)


def low_place(kb):
    return (kb % 4) * 2 + kb // 4


def high_place(kb):
    return (kb % 4) * 2 + 3 - kb // 4


def low_kernel(own, lam, qa_ref, qb_ref, kv_ref, gain_ref, _, o_ref, m_o, l_o, a_o, qz):
    step = pl.program_id(0)
    split_maps(jnp.where(step == own[2], qa_ref[...], qb_ref[...]), qz)
    start_state(m_o, l_o, a_o)
    refs = (qz, kv_ref, m_o, l_o, a_o)
    attend_blocks(0, jnp.where(step == 0, own[0], 8), low_place, refs)

    @pl.when(step == 0)
    def _():
        attend_diagonal(low_place(own[0]), refs)
        o_ref[...] = finish(lam, gain_ref, l_o, a_o)


def high_kernel(
    own, lam, qa_ref, qb_ref, kv_ref, gain_ref, low_ref, m_i, l_i, a_i, _, oa_ref, ob_ref, qz
):
    low_first = own[2] == 0
    split_maps(jnp.where(low_first, qb_ref[...], qa_ref[...]), qz)
    refs = (qz, kv_ref, m_i, l_i, a_i)
    attend_blocks(8, own[1] - 8, high_place, refs)
    attend_diagonal(high_place(own[1]), refs)
    high = finish(lam, gain_ref, l_i, a_i)
    oa_ref[...] = jnp.where(low_first, low_ref[...], high)
    ob_ref[...] = jnp.where(low_first, high, low_ref[...])


def attention_call(kernel, steps, args, outs, unread, blocks):
    def full(shape):
        return pl.BlockSpec(shape, lambda i, *_: (0,) * len(shape))

    return pl.pallas_call(
        kernel,
        out_shape=outs,
        grid_spec=pltpu.PrefetchScalarGridSpec(
            num_scalar_prefetch=2,
            grid=(steps,),
            in_specs=[full(a.shape) for a in args[2:]] + [in_hbm() for _ in unread],
            out_specs=tuple(full(o.shape) for o in outs),
            scratch_shapes=[pltpu.VMEM((2, ROWS, 128), jnp.bfloat16)],
        ),
        compiler_params=pltpu.CompilerParams(vmem_limit_bytes=60 * 2**20),
        cost_estimate=pl.CostEstimate(
            flops=blocks * 2 * 10**9, bytes_accessed=4 * 2**20, transcendentals=0
        ),
    )(*args, *unread)


def column_kernel(wc_ref, wa_ref, o_ref, sem):
    width = o_ref.shape[3]
    copies = [
        pltpu.make_async_copy(
            w_ref.at[:, pl.ds(t * width, width)], o_ref.at[t, i], sem.at[i, t]
        )
        for i, w_ref in enumerate((wc_ref, wa_ref))
        for t in range(8)
    ]
    for copy in copies:
        copy.start()
    for copy in copies:
        copy.wait()


def column_blocks(w_conv, w_attn):
    return pl.pallas_call(
        column_kernel,
        out_shape=jax.ShapeDtypeStruct((8, 2, 256, D // 8), jnp.bfloat16),
        in_specs=[in_hbm(), in_hbm()],
        out_specs=in_hbm(),
        scratch_shapes=[pltpu.SemaphoreType.DMA((2, 8))],
        name="column_blocks",
    )(w_conv, w_attn)


def whole_conv_kernel(x_ref, w_ref, o_ref):
    left = jnp.concatenate([x_ref[t] for t in range(8)], axis=1)
    right = jnp.concatenate([w_ref[t, 0] for t in range(8)], axis=0)
    o_ref[...] = jnp.dot(left, right, preferred_element_type=jnp.float32)


def whole_last_kernel(first, x_ref, w_ref, before_ref, mix_ref, sums_ref, xb, wb, acc, sem):
    copies = []
    for t in range(8):
        copies.append(pltpu.make_async_copy(x_ref.at[t], xb.at[t], sem.at[0, t]))
        copies.append(pltpu.make_async_copy(w_ref.at[t, 1], wb.at[t], sem.at[1, t]))
    head = pltpu.make_async_copy(before_ref, acc, sem.at[2, 0])
    head.start()
    for copy in copies:
        copy.start()
    head.wait()
    for t in range(8):
        copies[2 * t].wait()
        copies[2 * t + 1].wait()
        right = jnp.concatenate(
            [
                wb[t, pl.ds(pl.multiple_of(first[0] * VD, VD), VD), :],
                wb[t, pl.ds(pl.multiple_of((1 - first[0]) * VD, VD), VD), :],
            ],
            axis=0,
        )
        acc[...] += jnp.dot(xb[t], right, preferred_element_type=jnp.float32)
    mix = acc[...].astype(jnp.bfloat16)
    mix_ref[...] = mix
    wide = mix.astype(jnp.float32)
    square = wide * wide
    high = square.astype(jnp.bfloat16)
    low = (square - high.astype(jnp.float32)).astype(jnp.bfloat16)
    ones = jnp.ones((8, mix.shape[1]), jnp.bfloat16)

    def row_sums(values):
        return lax.dot_general(
            ones, values, (((1,), (1,)), ((), ())), preferred_element_type=jnp.float32
        )[0:1]

    sums = jnp.concatenate([row_sums(mix), row_sums(high) + row_sums(low)], axis=0)
    for copy in range(8):
        sums_ref[copy] = sums


def whole_conv(gathered, weights):
    width = weights.shape[3]
    return pl.pallas_call(
        whole_conv_kernel,
        out_shape=jax.ShapeDtypeStruct((ROWS, width), jnp.float32),
        grid=(1,),
        in_specs=[
            pl.BlockSpec(gathered.shape, lambda i: (0, 0, 0)),
            pl.BlockSpec((8, 1, 256, width), lambda i: (0, 0, 0, 0)),
        ],
        out_specs=pl.BlockSpec((ROWS, width), lambda i: (0, 0)),
        compiler_params=pltpu.CompilerParams(vmem_limit_bytes=60 * 2**20),
        cost_estimate=pl.CostEstimate(
            flops=2 * ROWS * 2048 * width, bytes_accessed=7 * 2**20, transcendentals=0
        ),
        name="whole_conv",
    )(gathered, weights)


def whole_last(first, gathered, weights, before):
    width = weights.shape[3]
    return pl.pallas_call(
        whole_last_kernel,
        out_shape=(
            jax.ShapeDtypeStruct((ROWS, width), jnp.bfloat16),
            jax.ShapeDtypeStruct((8, 2, ROWS), jnp.float32),
        ),
        grid_spec=pltpu.PrefetchScalarGridSpec(
            num_scalar_prefetch=1,
            grid=(1,),
            in_specs=[in_hbm(), in_hbm(), in_hbm()],
            out_specs=(
                pl.BlockSpec((ROWS, width), lambda i, *_: (0, 0)),
                pl.BlockSpec((8, 2, ROWS), lambda i, *_: (0, 0, 0)),
            ),
            scratch_shapes=[
                pltpu.VMEM((8, ROWS, 256), jnp.bfloat16),
                pltpu.VMEM((8, 256, width), jnp.bfloat16),
                pltpu.VMEM((ROWS, width), jnp.float32),
                pltpu.SemaphoreType.DMA((3, 8)),
            ],
        ),
        compiler_params=pltpu.CompilerParams(vmem_limit_bytes=60 * 2**20),
        cost_estimate=pl.CostEstimate(
            flops=2 * ROWS * 2048 * width, bytes_accessed=7 * 2**20, transcendentals=0
        ),
        name="whole_last",
    )(first, gathered, weights, before)


def per_device(
    hidden_states,
    w_conv_b,
    w_conv_c,
    w_conv_h,
    conv_taps,
    w_query,
    w_key,
    w_value,
    lambdas,
    head_gain,
    w_out_conv,
    w_out_attn,
    out_gain,
):
    z = lax.axis_index("z")
    x = lax.axis_index("x")
    core = lax.axis_index("c")
    sp = z * 4 + x

    z_core = ("z", "c")
    rim = lax.ppermute(hidden_states[ROWS - HALO :], ("z", "x"), [(i, i + 1) for i in range(15)])
    other_lambdas = lax.ppermute(lambdas, "c", [(0, 1), (1, 0)])

    first = jnp.where(z < 2, 0, 1).astype(jnp.int32).reshape(1)
    _, _, start_cos, start_sin = rotary_tables()
    groups = ROWS // GROUP
    q_a, q_b, kv_a, kv_b = project_qkv(
        first,
        hidden_states,
        w_query,
        w_key,
        w_value,
        lax.dynamic_slice_in_dim(jnp.asarray(start_cos), sp * groups, groups, 0),
        lax.dynamic_slice_in_dim(jnp.asarray(start_sin), sp * groups, groups, 0),
    )
    route_a, route_b = forward_route(0), forward_route(1)
    kv_a = lax.ppermute(kv_a, z_core, route_a)
    kv_b = lax.ppermute(kv_b, z_core, route_b)
    q_a = lax.ppermute(q_a, z_core, route_a)
    q_b = lax.ppermute(q_b, z_core, route_b)
    even = (z % 2) == 0
    kv_low = lax.all_gather(jnp.where(even, kv_a, kv_b), ("x", "c"), axis=0)
    kv_high = lax.all_gather(jnp.where(even, kv_b, kv_a), ("x", "c"), axis=0)

    conv_out = gated_conv(hidden_states, rim, w_conv_b, w_conv_c, w_conv_h, conv_taps)
    conv_all = lax.all_gather(conv_out, ("y", "c"), axis=0)

    w_out = lax.all_to_all(
        column_blocks(w_out_conv, w_out_attn),
        ("y", "c"),
        split_axis=0,
        concat_axis=0,
        tiled=True,
    )

    plane_lambdas = jnp.where(
        core == 0,
        jnp.concatenate([lambdas, other_lambdas]),
        jnp.concatenate([other_lambdas, lambdas]),
    )
    lam = lax.dynamic_slice_in_dim(plane_lambdas, z, 1)
    low_z, high_z = jnp.where(core == 0, 0, 1), jnp.where(core == 0, 3, 2)
    own = jnp.stack([low_z * 4 + x, high_z * 4 + x, z % 2]).astype(jnp.int32)
    gain = head_gain.reshape(1, VD)
    rows = jax.ShapeDtypeStruct((ROWS, VD), jnp.bfloat16)
    state = (jax.ShapeDtypeStruct((2, ROWS, VD), jnp.float32),) * 3
    o_low, *carried = attention_call(
        low_kernel, 2, (own, lam, q_a, q_b, kv_low, gain), (rows, *state), (conv_out,), 12
    )
    o_a, o_b = attention_call(
        high_kernel,
        1,
        (own, lam, q_a, q_b, kv_high, gain, o_low, *carried),
        (rows, rows),
        (w_out,),
        6,
    )
    back_a = lax.ppermute(o_a, z_core, reverse(route_a))
    back_b = lax.ppermute(o_b, z_core, reverse(route_b))
    attn_all = lax.all_gather(jnp.concatenate([back_a, back_b], axis=1), ("y", "c"), axis=0)
    conv_part = whole_conv(conv_all, w_out)
    mix, sums = whole_last(first, attn_all, w_out, conv_part)
    everything = lax.all_to_all(sums, ("y", "c"), split_axis=0, concat_axis=0, tiled=True)
    totals = jnp.sum(everything, axis=0)
    mix_f = mix.astype(jnp.float32)
    width = mix_f.shape[1]
    mean_value = (totals[0] / D)[:, None]
    variance = (totals[1] / D)[:, None] - mean_value * mean_value
    tp = lax.axis_index("y") * 2 + core
    own_gain = lax.dynamic_slice_in_dim(out_gain.astype(jnp.float32), tp * width, width, 0)
    return ((mix_f - mean_value) * lax.rsqrt(variance + 1e-05) * own_gain[None, :]).astype(
        jnp.bfloat16
    )


def solution(mesh):
    chips = Mesh(mesh.devices.reshape(4, 4, 4, 2), ("z", "x", "y", "c"))
    sp, tp = ("z", "x"), ("y", "c")
    return jax.shard_map(
        per_device,
        mesh=chips,
        in_specs=(
            P(sp, None),
            P(None, tp),
            P(None, tp),
            P(None, tp),
            P(None, tp),
            P(None, tp),
            P(None, tp),
            P(None, tp),
            P(tp),
            P(),
            P(tp, None),
            P(tp, None),
            P(),
        ),
        out_specs=P(sp, tp),
        check_vma=False,
    )
```

```python
import jax
import jax.numpy as jnp
import numpy as np
from jax import lax
from jax.experimental import pallas as pl
from jax.experimental.pallas import tpu as pltpu
from jax.sharding import Mesh
from jax.sharding import PartitionSpec as P

D = 4096
QK = 64
VD = 128
ROWS = 768
HALO = 16
LOG2E = 1.4426950408889634

CORE_OF_Z = (0, 1, 1, 0)


def forward_route(round_index):
    route = []
    for z in range(4):
        for c in range(2):
            local = round_index if z < 2 else 1 - round_index
            route.append((z * 2 + c, (2 * c + local) * 2 + CORE_OF_Z[z]))
    return route


def reverse(route):
    return [(b, a) for a, b in route]


GROUP = 96


def rotary_tables():
    inverse = 10000.0 ** (-np.arange(0, QK, 2, dtype=np.float64) / QK)
    inverse = np.tile(inverse, 128 // inverse.size)
    rows = np.arange(GROUP, dtype=np.float64)[:, None] * inverse
    starts = np.arange(0, 16 * ROWS, GROUP, dtype=np.float64)[:, None] * inverse
    tables = (np.cos(rows), np.sin(rows), np.cos(starts), np.sin(starts))
    return tuple(t.astype(np.float32) for t in tables)


CHUNK = 1024
STEPS = D // CHUNK
AHEAD = 3


def streamed_products(pairs, sem, accs):
    copies = []
    for hbm, buf, by_columns in pairs:
        slot = len(copies)

        def copy(k, hbm=hbm, buf=buf, by_columns=by_columns, slot=slot):
            at = pl.ds(k * CHUNK, CHUNK)
            source = hbm.at[:, at] if by_columns else hbm.at[at, :]
            return pltpu.make_async_copy(source, buf.at[k], sem.at[slot, k])

        copies.append(copy)
    for k in range(AHEAD):
        for copy in copies:
            copy(k).start()
    for acc, _, _ in accs:
        acc[...] = jnp.zeros(acc.shape, jnp.float32)

    def step(k, carry):
        @pl.when(k + AHEAD < STEPS)
        def _():
            for copy in copies:
                copy(k + AHEAD).start()

        for copy in copies:
            copy(k).wait()
        for acc, lhs, weights in accs:
            h = lhs[k]
            for i, w in enumerate(weights):
                acc[i] += jnp.dot(h, w[k], preferred_element_type=jnp.float32)
        return carry

    lax.fori_loop(0, STEPS, step, 0)


def rotation(cr, sr, cs, ss):
    groups = range(ROWS // GROUP)
    cosine = jnp.concatenate(
        [cs[g : g + 1] * cr[...] - ss[g : g + 1] * sr[...] for g in groups], axis=0
    )
    sine = jnp.concatenate(
        [ss[g : g + 1] * cr[...] + cs[g : g + 1] * sr[...] for g in groups], axis=0
    )
    lane = lax.broadcasted_iota(jnp.int32, (ROWS, 128), 1)
    upper = (lane % QK) < QK // 2

    def rotated(x):
        x = x.astype(jnp.bfloat16).astype(jnp.float32)
        swapped = jnp.where(upper, -pltpu.roll(x, 128 - QK // 2, 1), pltpu.roll(x, QK // 2, 1))
        return x * cosine + swapped * sine

    return rotated


def kv_kernel(
    where, h_ref, wk_ref, wv_ref, cr, sr, cs, ss, kva_ref, kvb_ref, acc, hb, kb, vb, sem
):
    streamed_products(
        ((h_ref, hb, True), (wk_ref, kb, False), (wv_ref, vb, False)),
        sem,
        ((acc, hb, (kb, vb)),),
    )
    rotated = rotation(cr, sr, cs, ss)
    keys = [rotated(acc[0, :, i * 128 : i * 128 + 128]).astype(jnp.bfloat16) for i in range(2)]
    vals = [acc[1, :, i * 128 : i * 128 + 128].astype(jnp.bfloat16) for i in range(2)]
    for flip, kv_ref in ((0, kva_ref), (1, kvb_ref)):
        take = where[1] == flip
        kv_ref[:, 0:128] = jnp.where(take, keys[0], keys[1])
        kv_ref[:, 128:256] = jnp.where(take, vals[0], vals[1])


def q_kernel(where, h_ref, wq_ref, cr, sr, cs, ss, _, qa_ref, qb_ref, acc, hb, qb, sem):
    streamed_products(((h_ref, hb, True), (wq_ref, qb, False)), sem, ((acc, hb, (qb,)),))
    rotated = rotation(cr, sr, cs, ss)
    queries = [
        (rotated(acc[0, :, i * 128 : i * 128 + 128]) * (LOG2E / 8)).astype(jnp.bfloat16)
        for i in range(2)
    ]
    for flip, q_ref in ((0, qa_ref), (1, qb_ref)):
        q_ref[...] = jnp.where(where[1] == flip, queries[0], queries[1])


def in_hbm():
    return pl.BlockSpec(memory_space=pltpu.HBM)


def stream_buffers(weights, rim):
    rows = [pltpu.VMEM((STEPS, ROWS, CHUNK), jnp.bfloat16)]
    if rim:
        rows.append(pltpu.VMEM((STEPS, HALO, CHUNK), jnp.bfloat16))
    return (
        rows
        + [pltpu.VMEM((STEPS, CHUNK, 256), jnp.bfloat16)] * weights
        + [pltpu.SemaphoreType.DMA((weights + len(rows), STEPS))]
    )


def project(kernel, width, where, hidden, weights, unread=()):
    row_cos, row_sin, start_cos, start_sin = rotary_tables()
    table = pl.BlockSpec((GROUP, 128), lambda k, *_: (0, 0))
    starts = pl.BlockSpec((ROWS // GROUP, 128), lambda k, where: (where[0], 0))
    out = jax.ShapeDtypeStruct((ROWS, width), jnp.bfloat16)
    count = len(weights)
    return pl.pallas_call(
        kernel,
        out_shape=(out, out),
        grid_spec=pltpu.PrefetchScalarGridSpec(
            num_scalar_prefetch=1,
            grid=(1,),
            in_specs=[in_hbm()] * (1 + count)
            + [table, table, starts, starts]
            + [in_hbm()] * len(unread),
            out_specs=(pl.BlockSpec((ROWS, width), lambda k, *_: (0, 0)),) * 2,
            scratch_shapes=[
                pltpu.VMEM((count, ROWS, 256), jnp.float32),
                *stream_buffers(count, False),
            ],
        ),
        compiler_params=pltpu.CompilerParams(vmem_limit_bytes=60 * 2**20),
        cost_estimate=pl.CostEstimate(
            flops=2 * ROWS * D * 256 * count,
            bytes_accessed=(6 + 2 * count) * 2**20,
            transcendentals=0,
        ),
    )(where, hidden, *weights, row_cos, row_sin, start_cos, start_sin, *unread)


def conv_kernel(
    h_ref, rim_ref, wb_ref, wc_ref, wh_ref, taps_ref, o_ref, acc, rim_acc, padded, hb, rb, b, c, h, sem
):
    streamed_products(
        (
            (h_ref, hb, True),
            (rim_ref, rb, True),
            (wb_ref, b, False),
            (wc_ref, c, False),
            (wh_ref, h, False),
        ),
        sem,
        ((acc, hb, (b, c, h)), (rim_acc, rb, (b, c, h))),
    )

    def once(x):
        return x.astype(jnp.bfloat16).astype(jnp.float32)

    padded[0:HALO] = once(rim_acc[1]) * once(rim_acc[2])
    padded[HALO:] = once(acc[1]) * once(acc[2])
    taps = taps_ref[...].astype(jnp.float32)
    conv = jnp.zeros((ROWS, 256), jnp.float32)
    for tap in range(3):
        conv = conv + taps[tap : tap + 1] * padded[HALO - 2 + tap : HALO - 2 + tap + ROWS]
    o_ref[...] = (once(acc[0]) * conv).astype(jnp.bfloat16)


def gated_conv(hidden, rim, w_b, w_c, w_h, taps):
    return pl.pallas_call(
        conv_kernel,
        out_shape=jax.ShapeDtypeStruct((ROWS, 256), jnp.bfloat16),
        grid=(1,),
        in_specs=[
            in_hbm(),
            in_hbm(),
            in_hbm(),
            in_hbm(),
            in_hbm(),
            pl.BlockSpec((3, 256), lambda k: (0, 0)),
        ],
        out_specs=pl.BlockSpec((ROWS, 256), lambda k: (0, 0)),
        scratch_shapes=[
            pltpu.VMEM((3, ROWS, 256), jnp.float32),
            pltpu.VMEM((3, HALO, 256), jnp.float32),
            pltpu.VMEM((HALO + ROWS, 256), jnp.float32),
            *stream_buffers(3, True),
        ],
        compiler_params=pltpu.CompilerParams(vmem_limit_bytes=60 * 2**20),
        cost_estimate=pl.CostEstimate(
            flops=2 * ROWS * D * 768, bytes_accessed=13 * 2**20, transcendentals=0
        ),
        name="gated_conv",
    )(hidden, rim, w_b, w_c, w_h, taps)


KEYS_AT_ONCE = 256


def split_maps(q, qz):
    lane = lax.broadcasted_iota(jnp.int32, (ROWS, 128), 1)
    qz[0] = jnp.where(lane < QK, q, jnp.zeros_like(q))
    qz[1] = jnp.where(lane >= QK, q, jnp.zeros_like(q))


def start_state(m_s, l_s, acc):
    m_s[...] = jnp.full(m_s.shape, -1e30, jnp.float32)
    l_s[...] = jnp.zeros(l_s.shape, jnp.float32)
    acc[...] = jnp.zeros(acc.shape, jnp.float32)


def attend(qz, kv_ref, m_s, l_s, acc, first_row, n, place, first_key, width, masked):
    rows = slice(first_row, first_row + n)
    keys = kv_ref[place, first_key : first_key + width, 0:128]
    vals = kv_ref[place, first_key : first_key + width, 128:256]
    s = lax.dot_general(
        qz[:, rows, :].reshape(2 * n, 128),
        keys,
        (((1,), (1,)), ((), ())),
        preferred_element_type=jnp.float32,
    ).reshape(2, n, width)
    if masked:
        r = lax.broadcasted_iota(jnp.int32, (2, n, width), 1) + first_row
        k = lax.broadcasted_iota(jnp.int32, (2, n, width), 2) + first_key
        s = jnp.where(k <= r, s, -1e30)
    m_old = m_s[:, rows, :]
    m_new = jnp.maximum(m_old, jnp.max(s, axis=2, keepdims=True))
    alpha = jnp.exp2(m_old - m_new)
    p = jnp.exp2(s - jnp.tile(m_new, (1, 1, width // 128)))
    part = p[:, :, 0:128]
    for w in range(1, width // 128):
        part = part + p[:, :, w * 128 : (w + 1) * 128]
    l_s[:, rows, :] = l_s[:, rows, :] * alpha + part
    m_s[:, rows, :] = m_new
    pv = jnp.dot(
        p.astype(jnp.bfloat16).reshape(2 * n, width), vals, preferred_element_type=jnp.float32
    )
    acc[:, rows, :] = acc[:, rows, :] * alpha + pv.reshape(2, n, 128)


def attend_blocks(first, count, place_of, refs):
    def block(kb):
        place = place_of(kb)
        for j in range(ROWS // KEYS_AT_ONCE):
            attend(*refs, 0, ROWS, place, j * KEYS_AT_ONCE, KEYS_AT_ONCE, False)

    def body(pair, carry):
        block(first + 2 * pair)
        block(first + 2 * pair + 1)
        return carry

    lax.fori_loop(0, count // 2, body, 0)

    @pl.when(count % 2 == 1)
    def _():
        block(first + count - 1)


def attend_diagonal(place, refs):
    for t in range(ROWS // 256):
        attend(*refs, t * 256, 256, place, 0, 256 * (t + 1), True)


def finish(lam, gain_ref, l_s, acc):
    denom = jnp.sum(l_s[...], axis=2, keepdims=True)
    diff = acc[0] / denom[0] - lam[0] * acc[1] / denom[1]
    mean_square = jnp.mean(diff * diff, axis=1, keepdims=True)
    normed = diff * lax.rsqrt(mean_square + 1e-5) * gain_ref[...].astype(jnp.float32)
    return normed.astype(jnp.bfloat16)


def low_place(kb):
    return (kb % 4) * 2 + kb // 4


def high_place(kb):
    return (kb % 4) * 2 + 3 - kb // 4


def low_kernel(own, lam, qa_ref, qb_ref, kv_ref, gain_ref, _, o_ref, m_o, l_o, a_o, qz):
    step = pl.program_id(0)
    split_maps(jnp.where(step == own[2], qa_ref[...], qb_ref[...]), qz)
    start_state(m_o, l_o, a_o)
    refs = (qz, kv_ref, m_o, l_o, a_o)
    attend_blocks(0, jnp.where(step == 0, own[0], 8), low_place, refs)

    @pl.when(step == 0)
    def _():
        attend_diagonal(low_place(own[0]), refs)
        o_ref[...] = finish(lam, gain_ref, l_o, a_o)


def high_kernel(
    own, lam, qa_ref, qb_ref, kv_ref, gain_ref, low_ref, m_i, l_i, a_i, _, oa_ref, ob_ref, qz
):
    low_first = own[2] == 0
    split_maps(jnp.where(low_first, qb_ref[...], qa_ref[...]), qz)
    refs = (qz, kv_ref, m_i, l_i, a_i)
    attend_blocks(8, own[1] - 8, high_place, refs)
    attend_diagonal(high_place(own[1]), refs)
    high = finish(lam, gain_ref, l_i, a_i)
    oa_ref[...] = jnp.where(low_first, low_ref[...], high)
    ob_ref[...] = jnp.where(low_first, high, low_ref[...])


def attention_call(kernel, steps, args, outs, unread, blocks):
    def full(shape):
        return pl.BlockSpec(shape, lambda i, *_: (0,) * len(shape))

    return pl.pallas_call(
        kernel,
        out_shape=outs,
        grid_spec=pltpu.PrefetchScalarGridSpec(
            num_scalar_prefetch=2,
            grid=(steps,),
            in_specs=[full(a.shape) for a in args[2:]] + [in_hbm() for _ in unread],
            out_specs=tuple(full(o.shape) for o in outs),
            scratch_shapes=[pltpu.VMEM((2, ROWS, 128), jnp.bfloat16)],
        ),
        compiler_params=pltpu.CompilerParams(vmem_limit_bytes=60 * 2**20),
        cost_estimate=pl.CostEstimate(
            flops=blocks * 2 * 10**9, bytes_accessed=4 * 2**20, transcendentals=0
        ),
    )(*args, *unread)


def column_kernel(wc_ref, wa_ref, o_ref, buf, sem):
    width = o_ref.shape[3]
    loads = [
        pltpu.make_async_copy(w_ref, buf.at[i], sem.at[i, 8])
        for i, w_ref in enumerate((wc_ref, wa_ref))
    ]
    for load in loads:
        load.start()
    stores = []
    for i in range(2):
        loads[i].wait()
        for t in range(8):
            stores.append(
                pltpu.make_async_copy(
                    buf.at[i, :, pl.ds(t * width, width)], o_ref.at[t, i], sem.at[i, t]
                )
            )
            stores[-1].start()
    for store in stores:
        store.wait()


def column_blocks(w_conv, w_attn):
    return pl.pallas_call(
        column_kernel,
        out_shape=jax.ShapeDtypeStruct((8, 2, 256, D // 8), jnp.bfloat16),
        in_specs=[in_hbm(), in_hbm()],
        out_specs=in_hbm(),
        scratch_shapes=[pltpu.VMEM((2, 256, D), jnp.bfloat16), pltpu.SemaphoreType.DMA((2, 9))],
        compiler_params=pltpu.CompilerParams(vmem_limit_bytes=60 * 2**20),
        cost_estimate=pl.CostEstimate(
            flops=3 * 10**9, bytes_accessed=9 * 2**20, transcendentals=0
        ),
        name="column_blocks",
    )(w_conv, w_attn)


def whole_conv_kernel(x_ref, w_ref, o_ref):
    left = jnp.concatenate([x_ref[t] for t in range(8)], axis=1)
    right = jnp.concatenate([w_ref[t, 0] for t in range(8)], axis=0)
    o_ref[...] = jnp.dot(left, right, preferred_element_type=jnp.float32)


def whole_last_kernel(first, x_ref, w_ref, before_ref, mix_ref, sums_ref, xb, wb, acc, sem):
    copies = []
    for t in range(8):
        copies.append(pltpu.make_async_copy(x_ref.at[t], xb.at[t], sem.at[0, t]))
        copies.append(pltpu.make_async_copy(w_ref.at[t, 1], wb.at[t], sem.at[1, t]))
    head = pltpu.make_async_copy(before_ref, acc, sem.at[2, 0])
    head.start()
    for copy in copies:
        copy.start()
    head.wait()
    for t in range(8):
        copies[2 * t].wait()
        copies[2 * t + 1].wait()
        right = jnp.concatenate(
            [
                wb[t, pl.ds(pl.multiple_of(first[0] * VD, VD), VD), :],
                wb[t, pl.ds(pl.multiple_of((1 - first[0]) * VD, VD), VD), :],
            ],
            axis=0,
        )
        acc[...] += jnp.dot(xb[t], right, preferred_element_type=jnp.float32)
    mix = acc[...].astype(jnp.bfloat16)
    mix_ref[...] = mix
    wide = mix.astype(jnp.float32)
    square = wide * wide
    high = square.astype(jnp.bfloat16)
    low = (square - high.astype(jnp.float32)).astype(jnp.bfloat16)
    ones = jnp.ones((8, mix.shape[1]), jnp.bfloat16)

    def row_sums(values):
        return lax.dot_general(
            ones, values, (((1,), (1,)), ((), ())), preferred_element_type=jnp.float32
        )

    row = lax.broadcasted_iota(jnp.int32, (8, ROWS), 0)
    squares = jnp.where(row == 1, row_sums(high) + row_sums(low), 0.0)
    sums = jnp.where(row == 0, row_sums(mix), squares)
    for copy in range(8):
        sums_ref[copy] = sums


def whole_conv(gathered, weights):
    width = weights.shape[3]
    return pl.pallas_call(
        whole_conv_kernel,
        out_shape=jax.ShapeDtypeStruct((ROWS, width), jnp.float32),
        grid=(1,),
        in_specs=[
            pl.BlockSpec(gathered.shape, lambda i: (0, 0, 0)),
            pl.BlockSpec((8, 1, 256, width), lambda i: (0, 0, 0, 0)),
        ],
        out_specs=pl.BlockSpec((ROWS, width), lambda i: (0, 0)),
        compiler_params=pltpu.CompilerParams(vmem_limit_bytes=60 * 2**20),
        cost_estimate=pl.CostEstimate(
            flops=2 * ROWS * 2048 * width, bytes_accessed=7 * 2**20, transcendentals=0
        ),
        name="whole_conv",
    )(gathered, weights)


def whole_last(first, gathered, weights, before):
    width = weights.shape[3]
    return pl.pallas_call(
        whole_last_kernel,
        out_shape=(
            jax.ShapeDtypeStruct((ROWS, width), jnp.bfloat16),
            jax.ShapeDtypeStruct((8, 8, ROWS), jnp.float32),
        ),
        grid_spec=pltpu.PrefetchScalarGridSpec(
            num_scalar_prefetch=1,
            grid=(1,),
            in_specs=[in_hbm(), in_hbm(), in_hbm()],
            out_specs=(
                pl.BlockSpec((ROWS, width), lambda i, *_: (0, 0)),
                pl.BlockSpec((8, 8, ROWS), lambda i, *_: (0, 0, 0)),
            ),
            scratch_shapes=[
                pltpu.VMEM((8, ROWS, 256), jnp.bfloat16),
                pltpu.VMEM((8, 256, width), jnp.bfloat16),
                pltpu.VMEM((ROWS, width), jnp.float32),
                pltpu.SemaphoreType.DMA((3, 8)),
            ],
        ),
        compiler_params=pltpu.CompilerParams(vmem_limit_bytes=60 * 2**20),
        cost_estimate=pl.CostEstimate(
            flops=2 * ROWS * 2048 * width, bytes_accessed=7 * 2**20, transcendentals=0
        ),
        name="whole_last",
    )(first, gathered, weights, before)


def norm_kernel(own, mix_ref, sums_ref, gain_ref, o_ref):
    sums = sums_ref[...].reshape(64, ROWS)
    row = lax.broadcasted_iota(jnp.int32, (64, 128), 0) % 8

    def column(which):
        total = lax.dot_general(
            sums,
            jnp.where(row == which, 1.0, 0.0),
            (((0,), (0,)), ((), ())),
            preferred_element_type=jnp.float32,
            precision=lax.Precision.HIGHEST,
        )
        return total * (1.0 / D)

    mean = column(0)
    variance = column(1) - mean * mean
    scale = lax.rsqrt(variance + 1e-5)
    gain = gain_ref[...].astype(jnp.float32)
    for at in range(0, mix_ref.shape[1], 128):
        mix = mix_ref[:, at : at + 128].astype(jnp.float32)
        o_ref[:, at : at + 128] = ((mix - mean) * scale * gain[:, at : at + 128]).astype(
            jnp.bfloat16
        )


def layer_norm(own, mix, sums, gain):
    width = mix.shape[1]
    return pl.pallas_call(
        norm_kernel,
        out_shape=jax.ShapeDtypeStruct(mix.shape, jnp.bfloat16),
        grid_spec=pltpu.PrefetchScalarGridSpec(
            num_scalar_prefetch=1,
            grid=(1,),
            in_specs=[
                pl.BlockSpec(mix.shape, lambda i, *_: (0, 0)),
                pl.BlockSpec(sums.shape, lambda i, *_: (0, 0, 0)),
                pl.BlockSpec((1, width), lambda i, own: (0, own[0])),
            ],
            out_specs=pl.BlockSpec(mix.shape, lambda i, *_: (0, 0)),
        ),
        name="norm",
    )(own, mix, sums, gain)


def per_device(
    hidden_states,
    w_conv_b,
    w_conv_c,
    w_conv_h,
    conv_taps,
    w_query,
    w_key,
    w_value,
    lambdas,
    head_gain,
    w_out_conv,
    w_out_attn,
    out_gain,
):
    z = lax.axis_index("z")
    x = lax.axis_index("x")
    core = lax.axis_index("c")
    sp = z * 4 + x

    z_core = ("z", "c")
    rim = lax.ppermute(hidden_states[ROWS - HALO :], ("z", "x"), [(i, i + 1) for i in range(15)])
    other_lambdas = lax.ppermute(lambdas, "c", [(0, 1), (1, 0)])

    first = jnp.where(z < 2, 0, 1).astype(jnp.int32).reshape(1)
    where = jnp.stack([sp, jnp.where(z < 2, 0, 1)]).astype(jnp.int32)
    route_a, route_b = forward_route(0), forward_route(1)
    kv_a, kv_b = project(kv_kernel, 256, where, hidden_states, (w_key, w_value))
    blocks = column_blocks(w_out_conv, w_out_attn)
    q_a, q_b = project(q_kernel, 128, where, hidden_states, (w_query,), (kv_a,))
    kv_a = lax.ppermute(kv_a, z_core, route_a)
    kv_b = lax.ppermute(kv_b, z_core, route_b)
    q_a = lax.ppermute(q_a, z_core, route_a)
    q_b = lax.ppermute(q_b, z_core, route_b)
    even = (z % 2) == 0
    kv_low, kv_high = jnp.where(even, kv_a, kv_b), jnp.where(even, kv_b, kv_a)
    kv_low = lax.all_gather(kv_low, ("x", "c"), axis=0)
    kv_high = lax.all_gather(kv_high, ("x", "c"), axis=0)

    conv_out = gated_conv(hidden_states, rim, w_conv_b, w_conv_c, w_conv_h, conv_taps)
    conv_all = lax.all_gather(conv_out, ("y", "c"), axis=0)

    w_out = lax.all_to_all(
        blocks,
        ("y", "c"),
        split_axis=0,
        concat_axis=0,
        tiled=True,
    )

    plane_lambdas = jnp.where(
        core == 0,
        jnp.concatenate([lambdas, other_lambdas]),
        jnp.concatenate([other_lambdas, lambdas]),
    )
    lam = lax.dynamic_slice_in_dim(plane_lambdas, z, 1)
    low_z, high_z = jnp.where(core == 0, 0, 1), jnp.where(core == 0, 3, 2)
    own = jnp.stack([low_z * 4 + x, high_z * 4 + x, z % 2]).astype(jnp.int32)
    gain = head_gain.reshape(1, VD)
    rows = jax.ShapeDtypeStruct((ROWS, VD), jnp.bfloat16)
    state = (jax.ShapeDtypeStruct((2, ROWS, VD), jnp.float32),) * 3
    o_low, *carried = attention_call(
        low_kernel, 2, (own, lam, q_a, q_b, kv_low, gain), (rows, *state), (conv_out,), 12
    )
    o_a, o_b = attention_call(
        high_kernel,
        1,
        (own, lam, q_a, q_b, kv_high, gain, o_low, *carried),
        (rows, rows),
        (w_out,),
        6,
    )
    back_a = lax.ppermute(o_a, z_core, reverse(route_a))
    back_b = lax.ppermute(o_b, z_core, reverse(route_b))
    attn_all = lax.all_gather(jnp.concatenate([back_a, back_b], axis=1), ("y", "c"), axis=0)
    conv_part = whole_conv(conv_all, w_out)
    mix, sums = whole_last(first, attn_all, w_out, conv_part)
    everything = lax.all_to_all(sums, ("y", "c"), split_axis=0, concat_axis=0, tiled=True)
    tp = (lax.axis_index("y") * 2 + core).astype(jnp.int32).reshape(1)
    return layer_norm(tp, mix, everything, out_gain.reshape(1, D))


def solution(mesh):
    chips = Mesh(mesh.devices.reshape(4, 4, 4, 2), ("z", "x", "y", "c"))
    sp, tp = ("z", "x"), ("y", "c")
    return jax.shard_map(
        per_device,
        mesh=chips,
        in_specs=(
            P(sp, None),
            P(None, tp),
            P(None, tp),
            P(None, tp),
            P(None, tp),
            P(None, tp),
            P(None, tp),
            P(None, tp),
            P(tp),
            P(),
            P(tp, None),
            P(tp, None),
            P(),
        ),
        out_specs=P(sp, tp),
        check_vma=False,
    )
```

```python
import jax
import jax.numpy as jnp
import numpy as np
from jax import lax
from jax.experimental import pallas as pl
from jax.experimental.pallas import tpu as pltpu
from jax.sharding import Mesh
from jax.sharding import PartitionSpec as P

D = 4096
QK = 64
VD = 128
ROWS = 768
HALO = 16
LOG2E = 1.4426950408889634

CORE_OF_Z = (0, 1, 1, 0)


def forward_route(round_index):
    route = []
    for z in range(4):
        for c in range(2):
            local = round_index if z < 2 else 1 - round_index
            route.append((z * 2 + c, (2 * c + local) * 2 + CORE_OF_Z[z]))
    return route


def reverse(route):
    return [(b, a) for a, b in route]


GROUP = 96


def rotary_tables():
    inverse = 10000.0 ** (-np.arange(0, QK, 2, dtype=np.float64) / QK)
    inverse = np.tile(inverse, 128 // inverse.size)
    rows = np.arange(GROUP, dtype=np.float64)[:, None] * inverse
    starts = np.arange(0, 16 * ROWS, GROUP, dtype=np.float64)[:, None] * inverse
    tables = (np.cos(rows), np.sin(rows), np.cos(starts), np.sin(starts))
    return tuple(t.astype(np.float32) for t in tables)


CHUNK = 1024
STEPS = D // CHUNK
AHEAD = 3


def streamed_products(pairs, sem, accs):
    copies = []
    for hbm, buf, by_columns in pairs:
        slot = len(copies)

        def copy(k, hbm=hbm, buf=buf, by_columns=by_columns, slot=slot):
            at = pl.ds(k * CHUNK, CHUNK)
            source = hbm.at[:, at] if by_columns else hbm.at[at, :]
            return pltpu.make_async_copy(source, buf.at[k], sem.at[slot, k])

        copies.append(copy)
    for k in range(AHEAD):
        for copy in copies:
            copy(k).start()
    for acc, _, _ in accs:
        acc[...] = jnp.zeros(acc.shape, jnp.float32)

    def step(k, carry):
        @pl.when(k + AHEAD < STEPS)
        def _():
            for copy in copies:
                copy(k + AHEAD).start()

        for copy in copies:
            copy(k).wait()
        for acc, lhs, weights in accs:
            h = lhs[k]
            for i, w in enumerate(weights):
                acc[i] += jnp.dot(h, w[k], preferred_element_type=jnp.float32)
        return carry

    lax.fori_loop(0, STEPS, step, 0)


def rotation(cr, sr, cs, ss):
    groups = range(ROWS // GROUP)
    cosine = jnp.concatenate(
        [cs[g : g + 1] * cr[...] - ss[g : g + 1] * sr[...] for g in groups], axis=0
    )
    sine = jnp.concatenate(
        [ss[g : g + 1] * cr[...] + cs[g : g + 1] * sr[...] for g in groups], axis=0
    )
    lane = lax.broadcasted_iota(jnp.int32, (ROWS, 128), 1)
    upper = (lane % QK) < QK // 2

    def rotated(x):
        x = x.astype(jnp.bfloat16).astype(jnp.float32)
        swapped = jnp.where(upper, -pltpu.roll(x, 128 - QK // 2, 1), pltpu.roll(x, QK // 2, 1))
        return x * cosine + swapped * sine

    return rotated


def qkv_kernel(
    where, h_ref, wk_ref, wv_ref, wq_ref, cr, sr, cs, ss, a_ref, b_ref, rim_ref, acc, hb, kb, vb, qb, sem
):
    streamed_products(
        ((h_ref, hb, True), (wk_ref, kb, False), (wv_ref, vb, False), (wq_ref, qb, False)),
        sem,
        ((acc, hb, (kb, vb, qb)),),
    )
    for k in range(STEPS):
        rim_ref[:, k * CHUNK : (k + 1) * CHUNK] = hb[k, ROWS - HALO :, :]
    rotated = rotation(cr, sr, cs, ss)
    heads = []
    for i in range(2):
        cols = slice(i * 128, i * 128 + 128)
        query = rotated(acc[2, :, cols]) * (LOG2E / 8)
        parts = (rotated(acc[0, :, cols]), acc[1, :, cols], query)
        heads.append([part.astype(jnp.bfloat16) for part in parts])
    for flip, o_ref in ((0, a_ref), (1, b_ref)):
        for i in range(3):
            o_ref[:, i * 128 : i * 128 + 128] = jnp.where(
                where[1] == flip, heads[0][i], heads[1][i]
            )


def in_hbm():
    return pl.BlockSpec(memory_space=pltpu.HBM)


def stream_buffers(weights, rim):
    rows = [pltpu.VMEM((STEPS, ROWS, CHUNK), jnp.bfloat16)]
    if rim:
        rows.append(pltpu.VMEM((STEPS, HALO, CHUNK), jnp.bfloat16))
    return (
        rows
        + [pltpu.VMEM((STEPS, CHUNK, 256), jnp.bfloat16)] * weights
        + [pltpu.SemaphoreType.DMA((weights + len(rows), STEPS))]
    )


def project(where, hidden, w_key, w_value, w_query):
    row_cos, row_sin, start_cos, start_sin = rotary_tables()
    table = pl.BlockSpec((GROUP, 128), lambda k, *_: (0, 0))
    starts = pl.BlockSpec((ROWS // GROUP, 128), lambda k, where: (where[0], 0))
    shapes = ((ROWS, 384), (ROWS, 384), (HALO, D))
    return pl.pallas_call(
        qkv_kernel,
        out_shape=tuple(jax.ShapeDtypeStruct(shape, jnp.bfloat16) for shape in shapes),
        grid_spec=pltpu.PrefetchScalarGridSpec(
            num_scalar_prefetch=1,
            grid=(1,),
            in_specs=[in_hbm()] * 4 + [table, table, starts, starts],
            out_specs=tuple(pl.BlockSpec(shape, lambda k, *_: (0, 0)) for shape in shapes),
            scratch_shapes=[pltpu.VMEM((3, ROWS, 256), jnp.float32), *stream_buffers(3, False)],
        ),
        compiler_params=pltpu.CompilerParams(vmem_limit_bytes=60 * 2**20),
        cost_estimate=pl.CostEstimate(
            flops=2 * ROWS * D * 768, bytes_accessed=13 * 2**20, transcendentals=0
        ),
        name="qkv",
    )(where, hidden, w_key, w_value, w_query, row_cos, row_sin, start_cos, start_sin)


PARCEL = ROWS + 4 * 256


def conv_kernel(
    h_ref, rim_ref, wb_ref, wc_ref, wh_ref, oc_ref, oa_ref, taps_ref, parcel_ref,
    acc, rim_acc, padded, staged, out_w, load_sem, store_sem, hb, rb, b, c, h, sem
):
    loads = [
        pltpu.make_async_copy(w_ref, out_w.at[i], load_sem.at[i])
        for i, w_ref in enumerate((oc_ref, oa_ref))
    ]
    for load in loads:
        load.start()
    streamed_products(
        (
            (h_ref, hb, True),
            (rim_ref, rb, True),
            (wb_ref, b, False),
            (wc_ref, c, False),
            (wh_ref, h, False),
        ),
        sem,
        ((acc, hb, (b, c, h)), (rim_acc, rb, (b, c, h))),
    )
    stores = []

    def store(source, t, part, first_row, count):
        stores.append(
            pltpu.make_async_copy(
                source, parcel_ref.at[t, pl.ds(first_row, count)], store_sem.at[t, part]
            )
        )
        stores[-1].start()

    for i in range(2):
        loads[i].wait()
        for t in range(8):
            for half in range(2):
                part = 2 * i + half
                column = pl.ds((2 * t + half) * 256, 256)
                store(out_w.at[i, :, column], t, part, ROWS + part * 256, 256)

    def once(x):
        return x.astype(jnp.bfloat16).astype(jnp.float32)

    padded[0:HALO] = once(rim_acc[1]) * once(rim_acc[2])
    padded[HALO:] = once(acc[1]) * once(acc[2])
    taps = taps_ref[...].astype(jnp.float32)
    conv = jnp.zeros((ROWS, 256), jnp.float32)
    for tap in range(3):
        conv = conv + taps[tap : tap + 1] * padded[HALO - 2 + tap : HALO - 2 + tap + ROWS]
    staged[...] = (once(acc[0]) * conv).astype(jnp.bfloat16)
    for t in range(8):
        store(staged, t, 4, 0, ROWS)
    for copy in stores:
        copy.wait()


def gated_conv(hidden, rim, w_b, w_c, w_h, w_out_conv, w_out_attn, taps):
    return pl.pallas_call(
        conv_kernel,
        out_shape=jax.ShapeDtypeStruct((8, PARCEL, 256), jnp.bfloat16),
        grid=(1,),
        in_specs=[in_hbm()] * 7 + [pl.BlockSpec((3, 256), lambda k: (0, 0))],
        out_specs=in_hbm(),
        scratch_shapes=[
            pltpu.VMEM((3, ROWS, 256), jnp.float32),
            pltpu.VMEM((3, HALO, 256), jnp.float32),
            pltpu.VMEM((HALO + ROWS, 256), jnp.float32),
            pltpu.VMEM((ROWS, 256), jnp.bfloat16),
            pltpu.VMEM((2, 256, D), jnp.bfloat16),
            pltpu.SemaphoreType.DMA((2,)),
            pltpu.SemaphoreType.DMA((8, 5)),
            *stream_buffers(3, True),
        ],
        compiler_params=pltpu.CompilerParams(vmem_limit_bytes=60 * 2**20),
        cost_estimate=pl.CostEstimate(
            flops=2 * ROWS * D * 768, bytes_accessed=24 * 2**20, transcendentals=0
        ),
        name="gated_conv",
    )(hidden, rim, w_b, w_c, w_h, w_out_conv, w_out_attn, taps)


KEYS_AT_ONCE = 256


def split_maps(q, qz):
    lane = lax.broadcasted_iota(jnp.int32, (ROWS, 128), 1)
    qz[0] = jnp.where(lane < QK, q, jnp.zeros_like(q))
    qz[1] = jnp.where(lane >= QK, q, jnp.zeros_like(q))


def start_state(m_s, l_s, acc):
    m_s[...] = jnp.full(m_s.shape, -1e30, jnp.float32)
    l_s[...] = jnp.zeros(l_s.shape, jnp.float32)
    acc[...] = jnp.zeros(acc.shape, jnp.float32)


def attend(qz, kv_ref, m_s, l_s, acc, first_row, n, place, first_key, width, masked):
    rows = slice(first_row, first_row + n)
    keys = kv_ref[place, first_key : first_key + width, 0:128]
    vals = kv_ref[place, first_key : first_key + width, 128:256]
    s = lax.dot_general(
        qz[:, rows, :].reshape(2 * n, 128),
        keys,
        (((1,), (1,)), ((), ())),
        preferred_element_type=jnp.float32,
    ).reshape(2, n, width)
    if masked:
        r = lax.broadcasted_iota(jnp.int32, (2, n, width), 1) + first_row
        k = lax.broadcasted_iota(jnp.int32, (2, n, width), 2) + first_key
        s = jnp.where(k <= r, s, -1e30)
    m_old = m_s[:, rows, :]
    m_new = jnp.maximum(m_old, jnp.max(s, axis=2, keepdims=True))
    alpha = jnp.exp2(m_old - m_new)
    p = jnp.exp2(s - jnp.tile(m_new, (1, 1, width // 128)))
    part = p[:, :, 0:128]
    for w in range(1, width // 128):
        part = part + p[:, :, w * 128 : (w + 1) * 128]
    l_s[:, rows, :] = l_s[:, rows, :] * alpha + part
    m_s[:, rows, :] = m_new
    pv = jnp.dot(
        p.astype(jnp.bfloat16).reshape(2 * n, width), vals, preferred_element_type=jnp.float32
    )
    acc[:, rows, :] = acc[:, rows, :] * alpha + pv.reshape(2, n, 128)


def attend_blocks(first, count, place_of, refs):
    def block(kb):
        place = place_of(kb)
        for j in range(ROWS // KEYS_AT_ONCE):
            attend(*refs, 0, ROWS, place, j * KEYS_AT_ONCE, KEYS_AT_ONCE, False)

    def body(pair, carry):
        block(first + 2 * pair)
        block(first + 2 * pair + 1)
        return carry

    lax.fori_loop(0, count // 2, body, 0)

    @pl.when(count % 2 == 1)
    def _():
        block(first + count - 1)


def attend_diagonal(place, refs):
    for t in range(ROWS // 256):
        attend(*refs, t * 256, 256, place, 0, 256 * (t + 1), True)


def finish(lam, gain_ref, l_s, acc):
    denom = jnp.sum(l_s[...], axis=2, keepdims=True)
    diff = acc[0] / denom[0] - lam[0] * acc[1] / denom[1]
    mean_square = jnp.mean(diff * diff, axis=1, keepdims=True)
    normed = diff * lax.rsqrt(mean_square + 1e-5) * gain_ref[...].astype(jnp.float32)
    return normed.astype(jnp.bfloat16)


def low_place(kb):
    return (kb % 4) * 2 + kb // 4


def high_place(kb):
    return (kb % 4) * 2 + 3 - kb // 4


def low_kernel(own, lam, ql_ref, qh_ref, kv_ref, gain_ref, o_ref, m_o, l_o, a_o, qz):
    step = pl.program_id(0)
    split_maps(jnp.where(step == 0, ql_ref[...], qh_ref[...]), qz)
    start_state(m_o, l_o, a_o)
    refs = (qz, kv_ref, m_o, l_o, a_o)
    attend_blocks(0, jnp.where(step == 0, own[0], 8), low_place, refs)

    @pl.when(step == 0)
    def _():
        attend_diagonal(low_place(own[0]), refs)
        o_ref[...] = finish(lam, gain_ref, l_o, a_o)


def high_kernel(
    own, lam, qh_ref, kv_ref, gain_ref, low_ref, m_i, l_i, a_i, oa_ref, ob_ref, qz
):
    low_first = own[2] == 0
    split_maps(qh_ref[...], qz)
    refs = (qz, kv_ref, m_i, l_i, a_i)
    attend_blocks(8, own[1] - 8, high_place, refs)
    attend_diagonal(high_place(own[1]), refs)
    high = finish(lam, gain_ref, l_i, a_i)
    oa_ref[...] = jnp.where(low_first, low_ref[...], high)
    ob_ref[...] = jnp.where(low_first, high, low_ref[...])


def attention_call(kernel, steps, args, outs, unread, blocks):
    def full(shape):
        return pl.BlockSpec(shape, lambda i, *_: (0,) * len(shape))

    return pl.pallas_call(
        kernel,
        out_shape=outs,
        grid_spec=pltpu.PrefetchScalarGridSpec(
            num_scalar_prefetch=2,
            grid=(steps,),
            in_specs=[full(a.shape) for a in args[2:]] + [in_hbm() for _ in unread],
            out_specs=tuple(full(o.shape) for o in outs),
            scratch_shapes=[pltpu.VMEM((2, ROWS, 128), jnp.bfloat16)],
        ),
        compiler_params=pltpu.CompilerParams(vmem_limit_bytes=60 * 2**20),
        cost_estimate=pl.CostEstimate(
            flops=blocks * 2 * 10**9, bytes_accessed=4 * 2**20, transcendentals=0
        ),
    )(*args, *unread)


def whole_conv_kernel(parcel_ref, o_ref):
    left = jnp.concatenate([parcel_ref[t, 0:ROWS] for t in range(8)], axis=1)
    for half in range(2):
        at = ROWS + half * 256
        right = jnp.concatenate([parcel_ref[t, at : at + 256] for t in range(8)], axis=0)
        o_ref[:, half * 256 : half * 256 + 256] = jnp.dot(
            left, right, preferred_element_type=jnp.float32
        )


def whole_last_kernel(first, x_ref, parcel_ref, before_ref, mix_ref, sums_ref, xb, wb, acc, sem):
    copies = []
    for t in range(8):
        source = parcel_ref.at[t, pl.ds(ROWS + 512, 512)]
        copies.append(pltpu.make_async_copy(x_ref.at[t], xb.at[t], sem.at[0, t]))
        copies.append(pltpu.make_async_copy(source, wb.at[t], sem.at[1, t]))
    head = pltpu.make_async_copy(before_ref, acc, sem.at[2, 0])
    head.start()
    for copy in copies:
        copy.start()
    head.wait()
    for t in range(8):
        copies[2 * t].wait()
        copies[2 * t + 1].wait()
        for half in range(2):
            right = jnp.concatenate(
                [
                    wb[t, pl.ds(pl.multiple_of(half * 256 + first[0] * VD, VD), VD), :],
                    wb[t, pl.ds(pl.multiple_of(half * 256 + (1 - first[0]) * VD, VD), VD), :],
                ],
                axis=0,
            )
            acc[:, half * 256 : half * 256 + 256] += jnp.dot(
                xb[t], right, preferred_element_type=jnp.float32
            )
    mix = acc[...].astype(jnp.bfloat16)
    mix_ref[...] = mix
    wide = mix.astype(jnp.float32)
    square = wide * wide
    high = square.astype(jnp.bfloat16)
    low = (square - high.astype(jnp.float32)).astype(jnp.bfloat16)
    ones = jnp.ones((8, mix.shape[1]), jnp.bfloat16)

    def row_sums(values):
        return lax.dot_general(
            ones, values, (((1,), (1,)), ((), ())), preferred_element_type=jnp.float32
        )

    squares = row_sums(high) + row_sums(low)
    sums = jnp.concatenate([row_sums(mix)[0:1], squares[0:1]], axis=0)
    for copy in range(8):
        sums_ref[copy] = sums


def whole_conv(parcels):
    return pl.pallas_call(
        whole_conv_kernel,
        out_shape=jax.ShapeDtypeStruct((ROWS, D // 8), jnp.float32),
        grid=(1,),
        in_specs=[pl.BlockSpec((8, ROWS + 512, 256), lambda i: (0, 0, 0))],
        out_specs=pl.BlockSpec((ROWS, D // 8), lambda i: (0, 0)),
        compiler_params=pltpu.CompilerParams(vmem_limit_bytes=60 * 2**20),
        cost_estimate=pl.CostEstimate(
            flops=2 * ROWS * 2048 * D // 8, bytes_accessed=7 * 2**20, transcendentals=0
        ),
        name="whole_conv",
    )(parcels)


def whole_last(first, gathered, parcels, before):
    width = D // 8
    return pl.pallas_call(
        whole_last_kernel,
        out_shape=(
            jax.ShapeDtypeStruct((ROWS, width), jnp.bfloat16),
            jax.ShapeDtypeStruct((8, 2, ROWS), jnp.float32),
        ),
        grid_spec=pltpu.PrefetchScalarGridSpec(
            num_scalar_prefetch=1,
            grid=(1,),
            in_specs=[in_hbm(), in_hbm(), in_hbm()],
            out_specs=(
                pl.BlockSpec((ROWS, width), lambda i, *_: (0, 0)),
                pl.BlockSpec((8, 2, ROWS), lambda i, *_: (0, 0, 0)),
            ),
            scratch_shapes=[
                pltpu.VMEM((8, ROWS, 256), jnp.bfloat16),
                pltpu.VMEM((8, 512, 256), jnp.bfloat16),
                pltpu.VMEM((ROWS, width), jnp.float32),
                pltpu.SemaphoreType.DMA((3, 8)),
            ],
        ),
        compiler_params=pltpu.CompilerParams(vmem_limit_bytes=60 * 2**20),
        cost_estimate=pl.CostEstimate(
            flops=2 * ROWS * 2048 * width, bytes_accessed=7 * 2**20, transcendentals=0
        ),
        name="whole_last",
    )(first, gathered, parcels, before)


def norm_kernel(own, mix_ref, sums_ref, gain_ref, o_ref):
    ones = jnp.ones((8, 128), jnp.float32)

    def column(which):
        total = lax.dot_general(
            sums_ref[:, which, :],
            ones,
            (((0,), (0,)), ((), ())),
            preferred_element_type=jnp.float32,
            precision=lax.Precision.HIGHEST,
        )
        return total * (1.0 / D)

    mean = column(0)
    variance = column(1) - mean * mean
    scale = lax.rsqrt(variance + 1e-5)
    gain = gain_ref[...].astype(jnp.float32)
    for at in range(0, mix_ref.shape[1], 128):
        mix = mix_ref[:, at : at + 128].astype(jnp.float32)
        o_ref[:, at : at + 128] = ((mix - mean) * scale * gain[:, at : at + 128]).astype(
            jnp.bfloat16
        )


def layer_norm(own, mix, sums, gain):
    width = mix.shape[1]
    return pl.pallas_call(
        norm_kernel,
        out_shape=jax.ShapeDtypeStruct(mix.shape, jnp.bfloat16),
        grid_spec=pltpu.PrefetchScalarGridSpec(
            num_scalar_prefetch=1,
            grid=(1,),
            in_specs=[
                pl.BlockSpec(mix.shape, lambda i, *_: (0, 0)),
                pl.BlockSpec(sums.shape, lambda i, *_: (0, 0, 0)),
                pl.BlockSpec((1, width), lambda i, own: (0, own[0])),
            ],
            out_specs=pl.BlockSpec(mix.shape, lambda i, *_: (0, 0)),
        ),
        name="norm",
    )(own, mix, sums, gain)


def per_device(
    hidden_states,
    w_conv_b,
    w_conv_c,
    w_conv_h,
    conv_taps,
    w_query,
    w_key,
    w_value,
    lambdas,
    head_gain,
    w_out_conv,
    w_out_attn,
    out_gain,
):
    z = lax.axis_index("z")
    x = lax.axis_index("x")
    core = lax.axis_index("c")
    sp = z * 4 + x

    z_core = ("z", "c")
    other_lambdas = lax.ppermute(lambdas, "c", [(0, 1), (1, 0)])

    first = jnp.where(z < 2, 0, 1).astype(jnp.int32).reshape(1)
    where = jnp.stack([sp, jnp.where(z < 2, 0, 1)]).astype(jnp.int32)
    route_a, route_b = forward_route(0), forward_route(1)
    head_a, head_b, last_rows = project(where, hidden_states, w_key, w_value, w_query)
    rim = lax.ppermute(last_rows, ("z", "x"), [(i, i + 1) for i in range(15)])
    head_a = lax.ppermute(head_a, z_core, route_a)
    head_b = lax.ppermute(head_b, z_core, route_b)
    parcels = gated_conv(
        hidden_states,
        rim,
        w_conv_b,
        w_conv_c,
        w_conv_h,
        w_out_conv,
        w_out_attn,
        conv_taps,
    )
    parcels = lax.all_to_all(parcels, ("y", "c"), split_axis=0, concat_axis=0, tiled=True)
    even = (z % 2) == 0
    kv, q = slice(0, 256), slice(256, 384)
    kv_low = jnp.where(even, head_a[:, kv], head_b[:, kv])
    kv_high = jnp.where(even, head_b[:, kv], head_a[:, kv])
    q_low = jnp.where(even, head_a[:, q], head_b[:, q])
    q_high = jnp.where(even, head_b[:, q], head_a[:, q])
    kv_low = lax.all_gather(kv_low, ("x", "c"), axis=0)
    kv_high = lax.all_gather(kv_high, ("x", "c"), axis=0)

    plane_lambdas = jnp.where(
        core == 0,
        jnp.concatenate([lambdas, other_lambdas]),
        jnp.concatenate([other_lambdas, lambdas]),
    )
    lam = lax.dynamic_slice_in_dim(plane_lambdas, z, 1)
    low_z, high_z = jnp.where(core == 0, 0, 1), jnp.where(core == 0, 3, 2)
    own = jnp.stack([low_z * 4 + x, high_z * 4 + x, z % 2]).astype(jnp.int32)
    gain = head_gain.reshape(1, VD)
    rows = jax.ShapeDtypeStruct((ROWS, VD), jnp.bfloat16)
    state = (jax.ShapeDtypeStruct((2, ROWS, VD), jnp.float32),) * 3
    o_low, *carried = attention_call(
        low_kernel, 2, (own, lam, q_low, q_high, kv_low, gain), (rows, *state), (), 12
    )
    o_a, o_b = attention_call(
        high_kernel, 1, (own, lam, q_high, kv_high, gain, o_low, *carried), (rows, rows), (), 6
    )
    back_a = lax.ppermute(o_a, z_core, reverse(route_a))
    back_b = lax.ppermute(o_b, z_core, reverse(route_b))
    attn_all = lax.all_gather(jnp.concatenate([back_a, back_b], axis=1), ("y", "c"), axis=0)
    conv_part = whole_conv(parcels)
    mix, sums = whole_last(first, attn_all, parcels, conv_part)
    everything = lax.all_to_all(sums, ("y", "c"), split_axis=0, concat_axis=0, tiled=True)
    tp = (lax.axis_index("y") * 2 + core).astype(jnp.int32).reshape(1)
    return layer_norm(tp, mix, everything, out_gain.reshape(1, D))


def solution(mesh):
    chips = Mesh(mesh.devices.reshape(4, 4, 4, 2), ("z", "x", "y", "c"))
    sp, tp = ("z", "x"), ("y", "c")
    return jax.shard_map(
        per_device,
        mesh=chips,
        in_specs=(
            P(sp, None),
            P(None, tp),
            P(None, tp),
            P(None, tp),
            P(None, tp),
            P(None, tp),
            P(None, tp),
            P(None, tp),
            P(tp),
            P(),
            P(tp, None),
            P(tp, None),
            P(),
        ),
        out_specs=P(sp, tp),
        check_vma=False,
    )
```

```python
import jax
import jax.numpy as jnp
import numpy as np
from jax import lax
from jax.experimental import pallas as pl
from jax.experimental.pallas import tpu as pltpu
from jax.sharding import Mesh
from jax.sharding import PartitionSpec as P

D = 4096
QK = 64
VD = 128
ROWS = 768
HALO = 16
LOG2E = 1.4426950408889634

CORE_OF_Z = (0, 1, 1, 0)


def forward_route(round_index):
    route = []
    for z in range(4):
        for c in range(2):
            local = round_index if z < 2 else 1 - round_index
            route.append((z * 2 + c, (2 * c + local) * 2 + CORE_OF_Z[z]))
    return route


def reverse(route):
    return [(b, a) for a, b in route]


GROUP = 96


def rotary_tables():
    inverse = 10000.0 ** (-np.arange(0, QK, 2, dtype=np.float64) / QK)
    inverse = np.tile(inverse, 128 // inverse.size)
    rows = np.arange(GROUP, dtype=np.float64)[:, None] * inverse
    starts = np.arange(0, 16 * ROWS, GROUP, dtype=np.float64)[:, None] * inverse
    tables = (np.cos(rows), np.sin(rows), np.cos(starts), np.sin(starts))
    return tuple(t.astype(np.float32) for t in tables)


CHUNK = 1024
STEPS = D // CHUNK
AHEAD = 3


def streamed_products(pairs, sem, accs):
    copies = []
    for hbm, buf, by_columns in pairs:
        slot = len(copies)

        def copy(k, hbm=hbm, buf=buf, by_columns=by_columns, slot=slot):
            at = pl.ds(k * CHUNK, CHUNK)
            source = hbm.at[:, at] if by_columns else hbm.at[at, :]
            return pltpu.make_async_copy(source, buf.at[k], sem.at[slot, k])

        copies.append(copy)
    for k in range(AHEAD):
        for copy in copies:
            copy(k).start()
    for acc, _, _ in accs:
        acc[...] = jnp.zeros(acc.shape, jnp.float32)

    def step(k, carry):
        @pl.when(k + AHEAD < STEPS)
        def _():
            for copy in copies:
                copy(k + AHEAD).start()

        for copy in copies:
            copy(k).wait()
        for acc, lhs, weights in accs:
            h = lhs[k]
            for i, w in enumerate(weights):
                acc[i] += jnp.dot(h, w[k], preferred_element_type=jnp.float32)
        return carry

    lax.fori_loop(0, STEPS, step, 0)


def rotation(cr, sr, cs, ss):
    groups = range(ROWS // GROUP)
    cosine = jnp.concatenate(
        [cs[g : g + 1] * cr[...] - ss[g : g + 1] * sr[...] for g in groups], axis=0
    )
    sine = jnp.concatenate(
        [ss[g : g + 1] * cr[...] + cs[g : g + 1] * sr[...] for g in groups], axis=0
    )
    lane = lax.broadcasted_iota(jnp.int32, (ROWS, 128), 1)
    upper = (lane % QK) < QK // 2

    def rotated(x):
        x = x.astype(jnp.bfloat16).astype(jnp.float32)
        swapped = jnp.where(upper, -pltpu.roll(x, 128 - QK // 2, 1), pltpu.roll(x, QK // 2, 1))
        return x * cosine + swapped * sine

    return rotated


def qkv_kernel(
    where, h_ref, wk_ref, wv_ref, wq_ref, cr, sr, cs, ss, a_ref, b_ref, rim_ref, acc, hb, kb, vb, qb, sem
):
    streamed_products(
        ((h_ref, hb, True), (wk_ref, kb, False), (wv_ref, vb, False), (wq_ref, qb, False)),
        sem,
        ((acc, hb, (kb, vb, qb)),),
    )
    for k in range(STEPS):
        rim_ref[:, k * CHUNK : (k + 1) * CHUNK] = hb[k, ROWS - HALO :, :]
    rotated = rotation(cr, sr, cs, ss)
    heads = []
    for i in range(2):
        cols = slice(i * 128, i * 128 + 128)
        query = rotated(acc[2, :, cols]) * (LOG2E / 8)
        parts = (rotated(acc[0, :, cols]), acc[1, :, cols], query)
        heads.append([part.astype(jnp.bfloat16) for part in parts])
    for flip, o_ref in ((0, a_ref), (1, b_ref)):
        for i in range(3):
            o_ref[:, i * 128 : i * 128 + 128] = jnp.where(
                where[1] == flip, heads[0][i], heads[1][i]
            )


def in_hbm():
    return pl.BlockSpec(memory_space=pltpu.HBM)


def stream_buffers(weights, rim):
    rows = [pltpu.VMEM((STEPS, ROWS, CHUNK), jnp.bfloat16)]
    if rim:
        rows.append(pltpu.VMEM((STEPS, HALO, CHUNK), jnp.bfloat16))
    return (
        rows
        + [pltpu.VMEM((STEPS, CHUNK, 256), jnp.bfloat16)] * weights
        + [pltpu.SemaphoreType.DMA((weights + len(rows), STEPS))]
    )


def project(where, hidden, w_key, w_value, w_query):
    row_cos, row_sin, start_cos, start_sin = rotary_tables()
    table = pl.BlockSpec((GROUP, 128), lambda k, *_: (0, 0))
    starts = pl.BlockSpec((ROWS // GROUP, 128), lambda k, where: (where[0], 0))
    shapes = ((ROWS, 384), (ROWS, 384), (HALO, D))
    return pl.pallas_call(
        qkv_kernel,
        out_shape=tuple(jax.ShapeDtypeStruct(shape, jnp.bfloat16) for shape in shapes),
        grid_spec=pltpu.PrefetchScalarGridSpec(
            num_scalar_prefetch=1,
            grid=(1,),
            in_specs=[in_hbm()] * 4 + [table, table, starts, starts],
            out_specs=tuple(pl.BlockSpec(shape, lambda k, *_: (0, 0)) for shape in shapes),
            scratch_shapes=[pltpu.VMEM((3, ROWS, 256), jnp.float32), *stream_buffers(3, False)],
        ),
        compiler_params=pltpu.CompilerParams(vmem_limit_bytes=60 * 2**20),
        cost_estimate=pl.CostEstimate(
            flops=2 * ROWS * D * 768, bytes_accessed=13 * 2**20, transcendentals=0
        ),
        name="qkv",
    )(where, hidden, w_key, w_value, w_query, row_cos, row_sin, start_cos, start_sin)


def conv_kernel(
    h_ref, rim_ref, wb_ref, wc_ref, wh_ref, taps_ref, o_ref, acc, rim_acc, padded, hb, rb, b, c, h, sem
):
    streamed_products(
        (
            (h_ref, hb, True),
            (rim_ref, rb, True),
            (wb_ref, b, False),
            (wc_ref, c, False),
            (wh_ref, h, False),
        ),
        sem,
        ((acc, hb, (b, c, h)), (rim_acc, rb, (b, c, h))),
    )

    def once(x):
        return x.astype(jnp.bfloat16).astype(jnp.float32)

    padded[0:HALO] = once(rim_acc[1]) * once(rim_acc[2])
    padded[HALO:] = once(acc[1]) * once(acc[2])
    taps = taps_ref[...].astype(jnp.float32)
    conv = jnp.zeros((ROWS, 256), jnp.float32)
    for tap in range(3):
        conv = conv + taps[tap : tap + 1] * padded[HALO - 2 + tap : HALO - 2 + tap + ROWS]
    o_ref[...] = (once(acc[0]) * conv).astype(jnp.bfloat16)


def gated_conv(hidden, rim, w_b, w_c, w_h, taps):
    return pl.pallas_call(
        conv_kernel,
        out_shape=jax.ShapeDtypeStruct((ROWS, 256), jnp.bfloat16),
        grid=(1,),
        in_specs=[
            in_hbm(),
            in_hbm(),
            in_hbm(),
            in_hbm(),
            in_hbm(),
            pl.BlockSpec((3, 256), lambda k: (0, 0)),
        ],
        out_specs=pl.BlockSpec((ROWS, 256), lambda k: (0, 0)),
        scratch_shapes=[
            pltpu.VMEM((3, ROWS, 256), jnp.float32),
            pltpu.VMEM((3, HALO, 256), jnp.float32),
            pltpu.VMEM((HALO + ROWS, 256), jnp.float32),
            *stream_buffers(3, True),
        ],
        compiler_params=pltpu.CompilerParams(vmem_limit_bytes=60 * 2**20),
        cost_estimate=pl.CostEstimate(
            flops=2 * ROWS * D * 768, bytes_accessed=13 * 2**20, transcendentals=0
        ),
        name="gated_conv",
    )(hidden, rim, w_b, w_c, w_h, taps)


KEYS_AT_ONCE = 256


def split_maps(q, qz):
    lane = lax.broadcasted_iota(jnp.int32, (ROWS, 128), 1)
    qz[0] = jnp.where(lane < QK, q, jnp.zeros_like(q))
    qz[1] = jnp.where(lane >= QK, q, jnp.zeros_like(q))


def start_state(m_s, l_s, acc):
    m_s[...] = jnp.full(m_s.shape, -1e30, jnp.float32)
    l_s[...] = jnp.zeros(l_s.shape, jnp.float32)
    acc[...] = jnp.zeros(acc.shape, jnp.float32)


def attend(qz, kv_ref, m_s, l_s, acc, first_row, n, place, first_key, width, masked):
    rows = slice(first_row, first_row + n)
    keys = kv_ref[place, first_key : first_key + width, 0:128]
    vals = kv_ref[place, first_key : first_key + width, 128:256]
    s = lax.dot_general(
        qz[:, rows, :].reshape(2 * n, 128),
        keys,
        (((1,), (1,)), ((), ())),
        preferred_element_type=jnp.float32,
    ).reshape(2, n, width)
    if masked:
        r = lax.broadcasted_iota(jnp.int32, (2, n, width), 1) + first_row
        k = lax.broadcasted_iota(jnp.int32, (2, n, width), 2) + first_key
        s = jnp.where(k <= r, s, -1e30)
    m_old = m_s[:, rows, :]
    m_new = jnp.maximum(m_old, jnp.max(s, axis=2, keepdims=True))
    alpha = jnp.exp2(m_old - m_new)
    p = jnp.exp2(s - jnp.tile(m_new, (1, 1, width // 128)))
    part = p[:, :, 0:128]
    for w in range(1, width // 128):
        part = part + p[:, :, w * 128 : (w + 1) * 128]
    l_s[:, rows, :] = l_s[:, rows, :] * alpha + part
    m_s[:, rows, :] = m_new
    pv = jnp.dot(
        p.astype(jnp.bfloat16).reshape(2 * n, width), vals, preferred_element_type=jnp.float32
    )
    acc[:, rows, :] = acc[:, rows, :] * alpha + pv.reshape(2, n, 128)


def attend_blocks(first, count, slot_of, ready, refs):
    def block(kb):
        for j in range(ROWS // KEYS_AT_ONCE):
            attend(*refs, 0, ROWS, slot_of(kb), j * KEYS_AT_ONCE, KEYS_AT_ONCE, False)

    def body(pair, carry):
        kb = first + 2 * pair
        ready(kb)
        ready(kb + 1)
        block(kb)
        block(kb + 1)
        return carry

    lax.fori_loop(0, count // 2, body, 0)

    @pl.when(count % 2 == 1)
    def _():
        ready(first + count - 1)
        block(first + count - 1)


def attend_diagonal(place, refs):
    for t in range(ROWS // 256):
        attend(*refs, t * 256, 256, place, 0, 256 * (t + 1), True)


def finish(lam, gain_ref, l_s, acc):
    denom = jnp.sum(l_s[...], axis=2, keepdims=True)
    diff = acc[0] / denom[0] - lam[0] * acc[1] / denom[1]
    mean_square = jnp.mean(diff * diff, axis=1, keepdims=True)
    normed = diff * lax.rsqrt(mean_square + 1e-5) * gain_ref[...].astype(jnp.float32)
    return normed.astype(jnp.bfloat16)


def low_place(kb):
    return (kb % 4) * 2 + kb // 4


def high_place(kb):
    return (kb % 4) * 2 + 3 - kb // 4


def low_kernel(own, lam, ql_ref, qh_ref, gain_ref, kv_hbm, _, o_ref, m_o, l_o, a_o, qz, kv_ref, sem):
    step = pl.program_id(0)

    def load(kb):
        return pltpu.make_async_copy(kv_hbm.at[low_place(kb)], kv_ref.at[kb], sem.at[kb])

    @pl.when(step == 0)
    def _():
        for kb in range(8):
            load(kb).start()

    def ready(kb):
        @pl.when(jnp.logical_or(step == 0, kb > own[0]))
        def _():
            load(kb).wait()

    split_maps(jnp.where(step == 0, ql_ref[...], qh_ref[...]), qz)
    start_state(m_o, l_o, a_o)
    refs = (qz, kv_ref, m_o, l_o, a_o)
    attend_blocks(0, jnp.where(step == 0, own[0], 8), lambda kb: kb, ready, refs)

    @pl.when(step == 0)
    def _():
        load(own[0]).wait()
        attend_diagonal(own[0], refs)
        o_ref[...] = finish(lam, gain_ref, l_o, a_o)


def high_kernel(
    own, lam, qh_ref, gain_ref, low_ref, m_i, l_i, a_i, kv_hbm, oa_ref, ob_ref, qz, kv_ref, sem
):
    def load(kb):
        slot = kb - 8
        return pltpu.make_async_copy(kv_hbm.at[high_place(kb)], kv_ref.at[slot], sem.at[slot])

    for kb in range(8, 16):

        @pl.when(kb <= own[1])
        def _(kb=kb):
            load(kb).start()

    split_maps(qh_ref[...], qz)
    refs = (qz, kv_ref, m_i, l_i, a_i)
    attend_blocks(8, own[1] - 8, lambda kb: kb - 8, lambda kb: load(kb).wait(), refs)
    load(own[1]).wait()
    attend_diagonal(own[1] - 8, refs)
    high = finish(lam, gain_ref, l_i, a_i)
    low_first = own[2] == 0
    oa_ref[...] = jnp.where(low_first, low_ref[...], high)
    ob_ref[...] = jnp.where(low_first, high, low_ref[...])


def attention_call(kernel, steps, args, outs, unread, blocks):
    def full(shape):
        return pl.BlockSpec(shape, lambda i, *_: (0,) * len(shape))

    return pl.pallas_call(
        kernel,
        out_shape=outs,
        grid_spec=pltpu.PrefetchScalarGridSpec(
            num_scalar_prefetch=2,
            grid=(steps,),
            in_specs=[full(a.shape) for a in args[2:]] + [in_hbm() for _ in unread],
            out_specs=tuple(full(o.shape) for o in outs),
            scratch_shapes=[
                pltpu.VMEM((2, ROWS, 128), jnp.bfloat16),
                pltpu.VMEM((8, ROWS, 256), jnp.bfloat16),
                pltpu.SemaphoreType.DMA((8,)),
            ],
        ),
        compiler_params=pltpu.CompilerParams(vmem_limit_bytes=60 * 2**20),
        cost_estimate=pl.CostEstimate(
            flops=blocks * 2 * 10**9, bytes_accessed=4 * 2**20, transcendentals=0
        ),
    )(*args, *unread)


def column_kernel(wc_ref, wa_ref, o_ref, buf, sem):
    width = o_ref.shape[3]
    loads = [
        pltpu.make_async_copy(w_ref, buf.at[i], sem.at[i, 8])
        for i, w_ref in enumerate((wc_ref, wa_ref))
    ]
    for load in loads:
        load.start()
    stores = []
    for i in range(2):
        loads[i].wait()
        for t in range(8):
            stores.append(
                pltpu.make_async_copy(
                    buf.at[i, :, pl.ds(t * width, width)], o_ref.at[t, i], sem.at[i, t]
                )
            )
            stores[-1].start()
    for store in stores:
        store.wait()


def column_blocks(w_conv, w_attn):
    return pl.pallas_call(
        column_kernel,
        out_shape=jax.ShapeDtypeStruct((8, 2, 256, D // 8), jnp.bfloat16),
        in_specs=[in_hbm(), in_hbm()],
        out_specs=in_hbm(),
        scratch_shapes=[pltpu.VMEM((2, 256, D), jnp.bfloat16), pltpu.SemaphoreType.DMA((2, 9))],
        compiler_params=pltpu.CompilerParams(vmem_limit_bytes=60 * 2**20),
        cost_estimate=pl.CostEstimate(
            flops=3 * 10**9, bytes_accessed=9 * 2**20, transcendentals=0
        ),
        name="column_blocks",
    )(w_conv, w_attn)


def whole_conv_kernel(x_ref, w_ref, o_ref):
    left = jnp.concatenate([x_ref[t] for t in range(8)], axis=1)
    right = jnp.concatenate([w_ref[t, 0] for t in range(8)], axis=0)
    o_ref[...] = jnp.dot(left, right, preferred_element_type=jnp.float32)


def whole_last_kernel(first, x_ref, w_ref, before_ref, mix_ref, sums_ref, xb, wb, acc, sem):
    copies = []
    for t in range(8):
        copies.append(pltpu.make_async_copy(x_ref.at[t], xb.at[t], sem.at[0, t]))
        copies.append(pltpu.make_async_copy(w_ref.at[t, 1], wb.at[t], sem.at[1, t]))
    head = pltpu.make_async_copy(before_ref, acc, sem.at[2, 0])
    head.start()
    for copy in copies:
        copy.start()
    head.wait()
    for t in range(8):
        copies[2 * t].wait()
        copies[2 * t + 1].wait()
        right = jnp.concatenate(
            [
                wb[t, pl.ds(pl.multiple_of(first[0] * VD, VD), VD), :],
                wb[t, pl.ds(pl.multiple_of((1 - first[0]) * VD, VD), VD), :],
            ],
            axis=0,
        )
        acc[...] += jnp.dot(xb[t], right, preferred_element_type=jnp.float32)
    mix = acc[...].astype(jnp.bfloat16)
    mix_ref[...] = mix
    wide = mix.astype(jnp.float32)
    square = wide * wide
    high = square.astype(jnp.bfloat16)
    low = (square - high.astype(jnp.float32)).astype(jnp.bfloat16)
    ones = jnp.ones((8, mix.shape[1]), jnp.bfloat16)

    def row_sums(values):
        return lax.dot_general(
            ones, values, (((1,), (1,)), ((), ())), preferred_element_type=jnp.float32
        )

    squares = row_sums(high) + row_sums(low)
    sums = jnp.concatenate([row_sums(mix)[0:1], squares[0:1]], axis=0)
    for copy in range(8):
        sums_ref[copy] = sums


def whole_conv(gathered, weights):
    width = weights.shape[3]
    return pl.pallas_call(
        whole_conv_kernel,
        out_shape=jax.ShapeDtypeStruct((ROWS, width), jnp.float32),
        grid=(1,),
        in_specs=[
            pl.BlockSpec(gathered.shape, lambda i: (0, 0, 0)),
            pl.BlockSpec((8, 1, 256, width), lambda i: (0, 0, 0, 0)),
        ],
        out_specs=pl.BlockSpec((ROWS, width), lambda i: (0, 0)),
        compiler_params=pltpu.CompilerParams(vmem_limit_bytes=60 * 2**20),
        cost_estimate=pl.CostEstimate(
            flops=2 * ROWS * 2048 * width, bytes_accessed=7 * 2**20, transcendentals=0
        ),
        name="whole_conv",
    )(gathered, weights)


def whole_last(first, gathered, weights, before):
    width = weights.shape[3]
    return pl.pallas_call(
        whole_last_kernel,
        out_shape=(
            jax.ShapeDtypeStruct((ROWS, width), jnp.bfloat16),
            jax.ShapeDtypeStruct((8, 2, ROWS), jnp.float32),
        ),
        grid_spec=pltpu.PrefetchScalarGridSpec(
            num_scalar_prefetch=1,
            grid=(1,),
            in_specs=[in_hbm(), in_hbm(), in_hbm()],
            out_specs=(
                pl.BlockSpec((ROWS, width), lambda i, *_: (0, 0)),
                pl.BlockSpec((8, 2, ROWS), lambda i, *_: (0, 0, 0)),
            ),
            scratch_shapes=[
                pltpu.VMEM((8, ROWS, 256), jnp.bfloat16),
                pltpu.VMEM((8, 256, width), jnp.bfloat16),
                pltpu.VMEM((ROWS, width), jnp.float32),
                pltpu.SemaphoreType.DMA((3, 8)),
            ],
        ),
        compiler_params=pltpu.CompilerParams(vmem_limit_bytes=60 * 2**20),
        cost_estimate=pl.CostEstimate(
            flops=2 * ROWS * 2048 * width, bytes_accessed=7 * 2**20, transcendentals=0
        ),
        name="whole_last",
    )(first, gathered, weights, before)


def norm_kernel(own, mix_ref, sums_ref, gain_ref, o_ref):
    ones = jnp.ones((8, 128), jnp.float32)

    def column(which):
        total = lax.dot_general(
            sums_ref[:, which, :],
            ones,
            (((0,), (0,)), ((), ())),
            preferred_element_type=jnp.float32,
            precision=lax.Precision.HIGHEST,
        )
        return total * (1.0 / D)

    mean = column(0)
    variance = column(1) - mean * mean
    scale = lax.rsqrt(variance + 1e-5)
    gain = gain_ref[...].astype(jnp.float32)
    for at in range(0, mix_ref.shape[1], 128):
        mix = mix_ref[:, at : at + 128].astype(jnp.float32)
        o_ref[:, at : at + 128] = ((mix - mean) * scale * gain[:, at : at + 128]).astype(
            jnp.bfloat16
        )


def layer_norm(own, mix, sums, gain):
    width = mix.shape[1]
    return pl.pallas_call(
        norm_kernel,
        out_shape=jax.ShapeDtypeStruct(mix.shape, jnp.bfloat16),
        grid_spec=pltpu.PrefetchScalarGridSpec(
            num_scalar_prefetch=1,
            grid=(1,),
            in_specs=[
                pl.BlockSpec(mix.shape, lambda i, *_: (0, 0)),
                pl.BlockSpec(sums.shape, lambda i, *_: (0, 0, 0)),
                pl.BlockSpec((1, width), lambda i, own: (0, own[0])),
            ],
            out_specs=pl.BlockSpec(mix.shape, lambda i, *_: (0, 0)),
        ),
        name="norm",
    )(own, mix, sums, gain)


def per_device(
    hidden_states,
    w_conv_b,
    w_conv_c,
    w_conv_h,
    conv_taps,
    w_query,
    w_key,
    w_value,
    lambdas,
    head_gain,
    w_out_conv,
    w_out_attn,
    out_gain,
):
    z = lax.axis_index("z")
    x = lax.axis_index("x")
    core = lax.axis_index("c")
    sp = z * 4 + x

    z_core = ("z", "c")
    other_lambdas = lax.ppermute(lambdas, "c", [(0, 1), (1, 0)])

    first = jnp.where(z < 2, 0, 1).astype(jnp.int32).reshape(1)
    where = jnp.stack([sp, jnp.where(z < 2, 0, 1)]).astype(jnp.int32)
    route_a, route_b = forward_route(0), forward_route(1)
    head_a, head_b, last_rows = project(where, hidden_states, w_key, w_value, w_query)
    rim = lax.ppermute(last_rows, ("z", "x"), [(i, i + 1) for i in range(15)])
    head_a = lax.ppermute(head_a, z_core, route_a)
    head_b = lax.ppermute(head_b, z_core, route_b)
    blocks = column_blocks(w_out_conv, w_out_attn)
    w_out = lax.all_to_all(blocks, ("y", "c"), split_axis=0, concat_axis=0, tiled=True)
    even = (z % 2) == 0
    kv, q = slice(0, 256), slice(256, 384)
    kv_low = jnp.where(even, head_a[:, kv], head_b[:, kv])
    kv_high = jnp.where(even, head_b[:, kv], head_a[:, kv])
    q_low = jnp.where(even, head_a[:, q], head_b[:, q])
    q_high = jnp.where(even, head_b[:, q], head_a[:, q])
    kv_low = lax.all_gather(kv_low, ("x", "c"), axis=0)
    kv_high = lax.all_gather(kv_high, ("x", "c"), axis=0)

    conv_out = gated_conv(hidden_states, rim, w_conv_b, w_conv_c, w_conv_h, conv_taps)
    conv_all = lax.all_gather(conv_out, ("y", "c"), axis=0)

    plane_lambdas = jnp.where(
        core == 0,
        jnp.concatenate([lambdas, other_lambdas]),
        jnp.concatenate([other_lambdas, lambdas]),
    )
    lam = lax.dynamic_slice_in_dim(plane_lambdas, z, 1)
    low_z, high_z = jnp.where(core == 0, 0, 1), jnp.where(core == 0, 3, 2)
    own = jnp.stack([low_z * 4 + x, high_z * 4 + x, z % 2]).astype(jnp.int32)
    gain = head_gain.reshape(1, VD)
    rows = jax.ShapeDtypeStruct((ROWS, VD), jnp.bfloat16)
    state = (jax.ShapeDtypeStruct((2, ROWS, VD), jnp.float32),) * 3
    o_low, *carried = attention_call(
        low_kernel, 2, (own, lam, q_low, q_high, gain), (rows, *state), (kv_low, conv_out), 12
    )
    o_a, o_b = attention_call(
        high_kernel, 1, (own, lam, q_high, gain, o_low, *carried), (rows, rows), (kv_high,), 6
    )
    back_a = lax.ppermute(o_a, z_core, reverse(route_a))
    back_b = lax.ppermute(o_b, z_core, reverse(route_b))
    attn_all = lax.all_gather(jnp.concatenate([back_a, back_b], axis=1), ("y", "c"), axis=0)
    conv_part = whole_conv(conv_all, w_out)
    mix, sums = whole_last(first, attn_all, w_out, conv_part)
    everything = lax.all_to_all(sums, ("y", "c"), split_axis=0, concat_axis=0, tiled=True)
    tp = (lax.axis_index("y") * 2 + core).astype(jnp.int32).reshape(1)
    return layer_norm(tp, mix, everything, out_gain.reshape(1, D))


def solution(mesh):
    chips = Mesh(mesh.devices.reshape(4, 4, 4, 2), ("z", "x", "y", "c"))
    sp, tp = ("z", "x"), ("y", "c")
    return jax.shard_map(
        per_device,
        mesh=chips,
        in_specs=(
            P(sp, None),
            P(None, tp),
            P(None, tp),
            P(None, tp),
            P(None, tp),
            P(None, tp),
            P(None, tp),
            P(None, tp),
            P(tp),
            P(),
            P(tp, None),
            P(tp, None),
            P(),
        ),
        out_specs=P(sp, tp),
        check_vma=False,
    )
```

```python
import jax
import jax.numpy as jnp
import numpy as np
from jax import lax
from jax.experimental import pallas as pl
from jax.experimental.pallas import tpu as pltpu
from jax.sharding import Mesh
from jax.sharding import PartitionSpec as P

D = 4096
QK = 64
VD = 128
ROWS = 768
HALO = 16
LOG2E = 1.4426950408889634

CORE_OF_Z = (0, 1, 1, 0)


def forward_route(round_index):
    route = []
    for z in range(4):
        for c in range(2):
            local = round_index if z < 2 else 1 - round_index
            route.append((z * 2 + c, (2 * c + local) * 2 + CORE_OF_Z[z]))
    return route


def reverse(route):
    return [(b, a) for a, b in route]


GROUP = 96


def rotary_tables():
    inverse = 10000.0 ** (-np.arange(0, QK, 2, dtype=np.float64) / QK)
    inverse = np.tile(inverse, 128 // inverse.size)
    rows = np.arange(GROUP, dtype=np.float64)[:, None] * inverse
    starts = np.arange(0, 16 * ROWS, GROUP, dtype=np.float64)[:, None] * inverse
    tables = (np.cos(rows), np.sin(rows), np.cos(starts), np.sin(starts))
    return tuple(t.astype(np.float32) for t in tables)


CHUNK = 1024
STEPS = D // CHUNK
AHEAD = 3


def streamed_products(pairs, sem, accs):
    copies = []
    for hbm, buf, by_columns in pairs:
        slot = len(copies)

        def copy(k, hbm=hbm, buf=buf, by_columns=by_columns, slot=slot):
            at = pl.ds(k * CHUNK, CHUNK)
            source = hbm.at[:, at] if by_columns else hbm.at[at, :]
            return pltpu.make_async_copy(source, buf.at[k], sem.at[slot, k])

        copies.append(copy)
    for k in range(AHEAD):
        for copy in copies:
            copy(k).start()
    for acc, _, _ in accs:
        acc[...] = jnp.zeros(acc.shape, jnp.float32)

    def step(k, carry):
        @pl.when(k + AHEAD < STEPS)
        def _():
            for copy in copies:
                copy(k + AHEAD).start()

        for copy in copies:
            copy(k).wait()
        for acc, lhs, weights in accs:
            h = lhs[k]
            for i, w in enumerate(weights):
                acc[i] += jnp.dot(h, w[k], preferred_element_type=jnp.float32)
        return carry

    lax.fori_loop(0, STEPS, step, 0)


def rotation(cr, sr, cs, ss):
    groups = range(ROWS // GROUP)
    cosine = jnp.concatenate(
        [cs[g : g + 1] * cr[...] - ss[g : g + 1] * sr[...] for g in groups], axis=0
    )
    sine = jnp.concatenate(
        [ss[g : g + 1] * cr[...] + cs[g : g + 1] * sr[...] for g in groups], axis=0
    )
    lane = lax.broadcasted_iota(jnp.int32, (ROWS, 128), 1)
    upper = (lane % QK) < QK // 2

    def rotated(x):
        x = x.astype(jnp.bfloat16).astype(jnp.float32)
        swapped = jnp.where(upper, -pltpu.roll(x, 128 - QK // 2, 1), pltpu.roll(x, QK // 2, 1))
        return x * cosine + swapped * sine

    return rotated


def qkv_kernel(
    where, h_ref, wk_ref, wv_ref, wq_ref, cr, sr, cs, ss, kva_ref, kvb_ref, qa_ref, qb_ref, rim_ref, acc, hb, kb, vb, qb, sem
):
    streamed_products(
        ((h_ref, hb, True), (wk_ref, kb, False), (wv_ref, vb, False), (wq_ref, qb, False)),
        sem,
        ((acc, hb, (kb, vb, qb)),),
    )
    for k in range(STEPS):
        rim_ref[:, k * CHUNK : (k + 1) * CHUNK] = hb[k, ROWS - HALO :, :]
    rotated = rotation(cr, sr, cs, ss)
    heads = []
    for i in range(2):
        cols = slice(i * 128, i * 128 + 128)
        query = rotated(acc[2, :, cols]) * (LOG2E / 8)
        parts = (rotated(acc[0, :, cols]), acc[1, :, cols], query)
        heads.append([part.astype(jnp.bfloat16) for part in parts])
    for flip, kv_ref, q_ref in ((0, kva_ref, qa_ref), (1, kvb_ref, qb_ref)):
        key, value, query = (
            jnp.where(where[1] == flip, heads[0][i], heads[1][i]) for i in range(3)
        )
        kv_ref[:, 0:128] = key
        kv_ref[:, 128:256] = value
        q_ref[...] = query


def in_hbm():
    return pl.BlockSpec(memory_space=pltpu.HBM)


def stream_buffers(weights, rim):
    rows = [pltpu.VMEM((STEPS, ROWS, CHUNK), jnp.bfloat16)]
    if rim:
        rows.append(pltpu.VMEM((STEPS, HALO, CHUNK), jnp.bfloat16))
    return (
        rows
        + [pltpu.VMEM((STEPS, CHUNK, 256), jnp.bfloat16)] * weights
        + [pltpu.SemaphoreType.DMA((weights + len(rows), STEPS))]
    )


def project(where, hidden, w_key, w_value, w_query):
    row_cos, row_sin, start_cos, start_sin = rotary_tables()
    table = pl.BlockSpec((GROUP, 128), lambda k, *_: (0, 0))
    starts = pl.BlockSpec((ROWS // GROUP, 128), lambda k, where: (where[0], 0))
    shapes = ((ROWS, 256), (ROWS, 256), (ROWS, 128), (ROWS, 128), (HALO, D))
    return pl.pallas_call(
        qkv_kernel,
        out_shape=tuple(jax.ShapeDtypeStruct(shape, jnp.bfloat16) for shape in shapes),
        grid_spec=pltpu.PrefetchScalarGridSpec(
            num_scalar_prefetch=1,
            grid=(1,),
            in_specs=[in_hbm()] * 4 + [table, table, starts, starts],
            out_specs=tuple(pl.BlockSpec(shape, lambda k, *_: (0, 0)) for shape in shapes),
            scratch_shapes=[pltpu.VMEM((3, ROWS, 256), jnp.float32), *stream_buffers(3, False)],
        ),
        compiler_params=pltpu.CompilerParams(vmem_limit_bytes=60 * 2**20),
        cost_estimate=pl.CostEstimate(
            flops=2 * ROWS * D * 768, bytes_accessed=13 * 2**20, transcendentals=0
        ),
        name="qkv",
    )(where, hidden, w_key, w_value, w_query, row_cos, row_sin, start_cos, start_sin)


def conv_kernel(
    h_ref, rim_ref, wb_ref, wc_ref, wh_ref, taps_ref, _, o_ref, acc, rim_acc, padded, hb, rb, b, c, h, sem
):
    streamed_products(
        (
            (h_ref, hb, True),
            (rim_ref, rb, True),
            (wb_ref, b, False),
            (wc_ref, c, False),
            (wh_ref, h, False),
        ),
        sem,
        ((acc, hb, (b, c, h)), (rim_acc, rb, (b, c, h))),
    )

    def once(x):
        return x.astype(jnp.bfloat16).astype(jnp.float32)

    padded[0:HALO] = once(rim_acc[1]) * once(rim_acc[2])
    padded[HALO:] = once(acc[1]) * once(acc[2])
    taps = taps_ref[...].astype(jnp.float32)
    conv = jnp.zeros((ROWS, 256), jnp.float32)
    for tap in range(3):
        conv = conv + taps[tap : tap + 1] * padded[HALO - 2 + tap : HALO - 2 + tap + ROWS]
    o_ref[...] = (once(acc[0]) * conv).astype(jnp.bfloat16)


def gated_conv(hidden, rim, w_b, w_c, w_h, taps, before):
    return pl.pallas_call(
        conv_kernel,
        out_shape=jax.ShapeDtypeStruct((ROWS, 256), jnp.bfloat16),
        grid=(1,),
        in_specs=[
            in_hbm(),
            in_hbm(),
            in_hbm(),
            in_hbm(),
            in_hbm(),
            pl.BlockSpec((3, 256), lambda k: (0, 0)),
            in_hbm(),
        ],
        out_specs=pl.BlockSpec((ROWS, 256), lambda k: (0, 0)),
        scratch_shapes=[
            pltpu.VMEM((3, ROWS, 256), jnp.float32),
            pltpu.VMEM((3, HALO, 256), jnp.float32),
            pltpu.VMEM((HALO + ROWS, 256), jnp.float32),
            *stream_buffers(3, True),
        ],
        compiler_params=pltpu.CompilerParams(vmem_limit_bytes=60 * 2**20),
        cost_estimate=pl.CostEstimate(
            flops=2 * ROWS * D * 768, bytes_accessed=13 * 2**20, transcendentals=0
        ),
        name="gated_conv",
    )(hidden, rim, w_b, w_c, w_h, taps, before)


KEYS_AT_ONCE = 256


def split_maps(q, qz):
    lane = lax.broadcasted_iota(jnp.int32, (ROWS, 128), 1)
    qz[0] = jnp.where(lane < QK, q, jnp.zeros_like(q))
    qz[1] = jnp.where(lane >= QK, q, jnp.zeros_like(q))


def start_state(m_s, l_s, acc):
    m_s[...] = jnp.full(m_s.shape, -1e30, jnp.float32)
    l_s[...] = jnp.zeros(l_s.shape, jnp.float32)
    acc[...] = jnp.zeros(acc.shape, jnp.float32)


def attend(qz, kv_ref, m_s, l_s, acc, first_row, n, place, first_key, width, masked):
    rows = slice(first_row, first_row + n)
    keys = kv_ref[place, first_key : first_key + width, 0:128]
    vals = kv_ref[place, first_key : first_key + width, 128:256]
    s = lax.dot_general(
        qz[:, rows, :].reshape(2 * n, 128),
        keys,
        (((1,), (1,)), ((), ())),
        preferred_element_type=jnp.float32,
    ).reshape(2, n, width)
    if masked:
        r = lax.broadcasted_iota(jnp.int32, (2, n, width), 1) + first_row
        k = lax.broadcasted_iota(jnp.int32, (2, n, width), 2) + first_key
        s = jnp.where(k <= r, s, -1e30)
    m_old = m_s[:, rows, :]
    m_new = jnp.maximum(m_old, jnp.max(s, axis=2, keepdims=True))
    alpha = jnp.exp2(m_old - m_new)
    p = jnp.exp2(s - jnp.tile(m_new, (1, 1, width // 128)))
    part = p[:, :, 0:128]
    for w in range(1, width // 128):
        part = part + p[:, :, w * 128 : (w + 1) * 128]
    l_s[:, rows, :] = l_s[:, rows, :] * alpha + part
    m_s[:, rows, :] = m_new
    pv = jnp.dot(
        p.astype(jnp.bfloat16).reshape(2 * n, width), vals, preferred_element_type=jnp.float32
    )
    acc[:, rows, :] = acc[:, rows, :] * alpha + pv.reshape(2, n, 128)


def attend_blocks(first, count, slot_of, ready, refs):
    def block(kb):
        for j in range(ROWS // KEYS_AT_ONCE):
            attend(*refs, 0, ROWS, slot_of(kb), j * KEYS_AT_ONCE, KEYS_AT_ONCE, False)

    def body(pair, carry):
        kb = first + 2 * pair
        ready(kb)
        ready(kb + 1)
        block(kb)
        block(kb + 1)
        return carry

    lax.fori_loop(0, count // 2, body, 0)

    @pl.when(count % 2 == 1)
    def _():
        ready(first + count - 1)
        block(first + count - 1)


def attend_diagonal(place, refs):
    for t in range(ROWS // 256):
        attend(*refs, t * 256, 256, place, 0, 256 * (t + 1), True)


def finish(lam, gain_ref, l_s, acc):
    denom = jnp.sum(l_s[...], axis=2, keepdims=True)
    diff = acc[0] / denom[0] - lam[0] * acc[1] / denom[1]
    mean_square = jnp.mean(diff * diff, axis=1, keepdims=True)
    normed = diff * lax.rsqrt(mean_square + 1e-5) * gain_ref[...].astype(jnp.float32)
    return normed.astype(jnp.bfloat16)


def low_place(kb):
    return (kb % 4) * 2 + kb // 4


def high_place(kb):
    return (kb % 4) * 2 + 3 - kb // 4


def low_kernel(own, lam, ql_ref, qh_ref, gain_ref, kv_hbm, _, o_ref, m_o, l_o, a_o, qz, kv_ref, sem):
    step = pl.program_id(0)

    def load(kb):
        return pltpu.make_async_copy(kv_hbm.at[low_place(kb)], kv_ref.at[kb], sem.at[kb])

    @pl.when(step == 0)
    def _():
        for kb in range(8):
            load(kb).start()

    def ready(kb):
        @pl.when(jnp.logical_or(step == 0, kb > own[0]))
        def _():
            load(kb).wait()

    split_maps(jnp.where(step == 0, ql_ref[...], qh_ref[...]), qz)
    start_state(m_o, l_o, a_o)
    refs = (qz, kv_ref, m_o, l_o, a_o)
    attend_blocks(0, jnp.where(step == 0, own[0], 8), lambda kb: kb, ready, refs)

    @pl.when(step == 0)
    def _():
        load(own[0]).wait()
        attend_diagonal(own[0], refs)
        o_ref[...] = finish(lam, gain_ref, l_o, a_o)


def high_kernel(
    own, lam, qh_ref, gain_ref, low_ref, m_i, l_i, a_i, kv_hbm, oa_ref, ob_ref, qz, kv_ref, sem
):
    def load(kb):
        slot = kb - 8
        return pltpu.make_async_copy(kv_hbm.at[high_place(kb)], kv_ref.at[slot], sem.at[slot])

    for kb in range(8, 16):

        @pl.when(kb <= own[1])
        def _(kb=kb):
            load(kb).start()

    split_maps(qh_ref[...], qz)
    refs = (qz, kv_ref, m_i, l_i, a_i)
    attend_blocks(8, own[1] - 8, lambda kb: kb - 8, lambda kb: load(kb).wait(), refs)
    load(own[1]).wait()
    attend_diagonal(own[1] - 8, refs)
    high = finish(lam, gain_ref, l_i, a_i)
    low_first = own[2] == 0
    oa_ref[...] = jnp.where(low_first, low_ref[...], high)
    ob_ref[...] = jnp.where(low_first, high, low_ref[...])


def attention_call(kernel, steps, args, outs, unread, blocks):
    def full(shape):
        return pl.BlockSpec(shape, lambda i, *_: (0,) * len(shape))

    return pl.pallas_call(
        kernel,
        out_shape=outs,
        grid_spec=pltpu.PrefetchScalarGridSpec(
            num_scalar_prefetch=2,
            grid=(steps,),
            in_specs=[full(a.shape) for a in args[2:]] + [in_hbm() for _ in unread],
            out_specs=tuple(full(o.shape) for o in outs),
            scratch_shapes=[
                pltpu.VMEM((2, ROWS, 128), jnp.bfloat16),
                pltpu.VMEM((8, ROWS, 256), jnp.bfloat16),
                pltpu.SemaphoreType.DMA((8,)),
            ],
        ),
        compiler_params=pltpu.CompilerParams(vmem_limit_bytes=60 * 2**20),
        cost_estimate=pl.CostEstimate(
            flops=blocks * 2 * 10**9, bytes_accessed=4 * 2**20, transcendentals=0
        ),
    )(*args, *unread)


def column_kernel(wc_ref, wa_ref, _, o_ref, buf, sem):
    width = o_ref.shape[3]
    loads = [
        pltpu.make_async_copy(w_ref, buf.at[i], sem.at[i, 8])
        for i, w_ref in enumerate((wc_ref, wa_ref))
    ]
    for load in loads:
        load.start()
    stores = []
    for i in range(2):
        loads[i].wait()
        for t in range(8):
            stores.append(
                pltpu.make_async_copy(
                    buf.at[i, :, pl.ds(t * width, width)], o_ref.at[t, i], sem.at[i, t]
                )
            )
            stores[-1].start()
    for store in stores:
        store.wait()


def column_blocks(w_conv, w_attn, before):
    return pl.pallas_call(
        column_kernel,
        out_shape=jax.ShapeDtypeStruct((8, 2, 256, D // 8), jnp.bfloat16),
        in_specs=[in_hbm(), in_hbm(), in_hbm()],
        out_specs=in_hbm(),
        scratch_shapes=[pltpu.VMEM((2, 256, D), jnp.bfloat16), pltpu.SemaphoreType.DMA((2, 9))],
        compiler_params=pltpu.CompilerParams(vmem_limit_bytes=60 * 2**20),
        cost_estimate=pl.CostEstimate(
            flops=3 * 10**9, bytes_accessed=9 * 2**20, transcendentals=0
        ),
        name="column_blocks",
    )(w_conv, w_attn, before)


def whole_conv_kernel(x_ref, w_ref, o_ref):
    left = jnp.concatenate([x_ref[t] for t in range(8)], axis=1)
    right = jnp.concatenate([w_ref[t, 0] for t in range(8)], axis=0)
    o_ref[...] = jnp.dot(left, right, preferred_element_type=jnp.float32)


def whole_last_kernel(first, x_ref, w_ref, before_ref, mix_ref, sums_ref, xb, wb, acc, sem):
    copies = []
    for t in range(8):
        copies.append(pltpu.make_async_copy(x_ref.at[t], xb.at[t], sem.at[0, t]))
        copies.append(pltpu.make_async_copy(w_ref.at[t, 1], wb.at[t], sem.at[1, t]))
    head = pltpu.make_async_copy(before_ref, acc, sem.at[2, 0])
    head.start()
    for copy in copies:
        copy.start()
    head.wait()
    for t in range(8):
        copies[2 * t].wait()
        copies[2 * t + 1].wait()
        right = jnp.concatenate(
            [
                wb[t, pl.ds(pl.multiple_of(first[0] * VD, VD), VD), :],
                wb[t, pl.ds(pl.multiple_of((1 - first[0]) * VD, VD), VD), :],
            ],
            axis=0,
        )
        acc[...] += jnp.dot(xb[t], right, preferred_element_type=jnp.float32)
    mix = acc[...].astype(jnp.bfloat16)
    mix_ref[...] = mix
    wide = mix.astype(jnp.float32)
    square = wide * wide
    high = square.astype(jnp.bfloat16)
    low = (square - high.astype(jnp.float32)).astype(jnp.bfloat16)
    ones = jnp.ones((8, mix.shape[1]), jnp.bfloat16)

    def row_sums(values):
        return lax.dot_general(
            ones, values, (((1,), (1,)), ((), ())), preferred_element_type=jnp.float32
        )

    squares = row_sums(high) + row_sums(low)
    sums = jnp.concatenate([row_sums(mix)[0:1], squares[0:1]], axis=0)
    for copy in range(8):
        sums_ref[copy] = sums


def whole_conv(gathered, weights):
    width = weights.shape[3]
    return pl.pallas_call(
        whole_conv_kernel,
        out_shape=jax.ShapeDtypeStruct((ROWS, width), jnp.float32),
        grid=(1,),
        in_specs=[
            pl.BlockSpec(gathered.shape, lambda i: (0, 0, 0)),
            pl.BlockSpec((8, 1, 256, width), lambda i: (0, 0, 0, 0)),
        ],
        out_specs=pl.BlockSpec((ROWS, width), lambda i: (0, 0)),
        compiler_params=pltpu.CompilerParams(vmem_limit_bytes=60 * 2**20),
        cost_estimate=pl.CostEstimate(
            flops=2 * ROWS * 2048 * width, bytes_accessed=7 * 2**20, transcendentals=0
        ),
        name="whole_conv",
    )(gathered, weights)


def whole_last(first, gathered, weights, before):
    width = weights.shape[3]
    return pl.pallas_call(
        whole_last_kernel,
        out_shape=(
            jax.ShapeDtypeStruct((ROWS, width), jnp.bfloat16),
            jax.ShapeDtypeStruct((8, 2, ROWS), jnp.float32),
        ),
        grid_spec=pltpu.PrefetchScalarGridSpec(
            num_scalar_prefetch=1,
            grid=(1,),
            in_specs=[in_hbm(), in_hbm(), in_hbm()],
            out_specs=(
                pl.BlockSpec((ROWS, width), lambda i, *_: (0, 0)),
                pl.BlockSpec((8, 2, ROWS), lambda i, *_: (0, 0, 0)),
            ),
            scratch_shapes=[
                pltpu.VMEM((8, ROWS, 256), jnp.bfloat16),
                pltpu.VMEM((8, 256, width), jnp.bfloat16),
                pltpu.VMEM((ROWS, width), jnp.float32),
                pltpu.SemaphoreType.DMA((3, 8)),
            ],
        ),
        compiler_params=pltpu.CompilerParams(vmem_limit_bytes=60 * 2**20),
        cost_estimate=pl.CostEstimate(
            flops=2 * ROWS * 2048 * width, bytes_accessed=7 * 2**20, transcendentals=0
        ),
        name="whole_last",
    )(first, gathered, weights, before)


def norm_kernel(own, mix_ref, sums_ref, gain_ref, o_ref):
    ones = jnp.ones((8, 128), jnp.float32)

    def column(which):
        total = lax.dot_general(
            sums_ref[:, which, :],
            ones,
            (((0,), (0,)), ((), ())),
            preferred_element_type=jnp.float32,
            precision=lax.Precision.HIGHEST,
        )
        return total * (1.0 / D)

    mean = column(0)
    variance = column(1) - mean * mean
    scale = lax.rsqrt(variance + 1e-5)
    gain = gain_ref[...].astype(jnp.float32)
    for at in range(0, mix_ref.shape[1], 128):
        mix = mix_ref[:, at : at + 128].astype(jnp.float32)
        o_ref[:, at : at + 128] = ((mix - mean) * scale * gain[:, at : at + 128]).astype(
            jnp.bfloat16
        )


def layer_norm(own, mix, sums, gain):
    width = mix.shape[1]
    return pl.pallas_call(
        norm_kernel,
        out_shape=jax.ShapeDtypeStruct(mix.shape, jnp.bfloat16),
        grid_spec=pltpu.PrefetchScalarGridSpec(
            num_scalar_prefetch=1,
            grid=(1,),
            in_specs=[
                pl.BlockSpec(mix.shape, lambda i, *_: (0, 0)),
                pl.BlockSpec(sums.shape, lambda i, *_: (0, 0, 0)),
                pl.BlockSpec((1, width), lambda i, own: (0, own[0])),
            ],
            out_specs=pl.BlockSpec(mix.shape, lambda i, *_: (0, 0)),
        ),
        name="norm",
    )(own, mix, sums, gain)


def per_device(
    hidden_states,
    w_conv_b,
    w_conv_c,
    w_conv_h,
    conv_taps,
    w_query,
    w_key,
    w_value,
    lambdas,
    head_gain,
    w_out_conv,
    w_out_attn,
    out_gain,
):
    z = lax.axis_index("z")
    x = lax.axis_index("x")
    core = lax.axis_index("c")
    sp = z * 4 + x

    z_core = ("z", "c")
    other_lambdas = lax.ppermute(lambdas, "c", [(0, 1), (1, 0)])

    first = jnp.where(z < 2, 0, 1).astype(jnp.int32).reshape(1)
    where = jnp.stack([sp, jnp.where(z < 2, 0, 1)]).astype(jnp.int32)
    route_a, route_b = forward_route(0), forward_route(1)
    head_a, head_b, q_a, q_b, last_rows = project(where, hidden_states, w_key, w_value, w_query)
    rim = lax.ppermute(last_rows, ("z", "x"), [(i, i + 1) for i in range(15)])
    head_a = lax.ppermute(head_a, z_core, route_a)
    head_b = lax.ppermute(head_b, z_core, route_b)
    q_a = lax.ppermute(q_a, z_core, route_a)
    q_b = lax.ppermute(q_b, z_core, route_b)
    even = (z % 2) == 0
    own_low = jnp.where(even, head_a, head_b)
    own_high = jnp.where(even, head_b, head_a)
    q_low = jnp.where(even, q_a, q_b)
    q_high = jnp.where(even, q_b, q_a)
    kv_low = lax.all_gather(own_low, ("x", "c"), axis=0)
    kv_high = lax.all_gather(own_high, ("x", "c"), axis=0)

    blocks = column_blocks(w_out_conv, w_out_attn, own_low)
    w_out = lax.all_to_all(blocks, ("y", "c"), split_axis=0, concat_axis=0, tiled=True)
    conv_out = gated_conv(
        hidden_states, rim, w_conv_b, w_conv_c, w_conv_h, conv_taps, own_low
    )
    conv_all = lax.all_gather(conv_out, ("y", "c"), axis=0)

    plane_lambdas = jnp.where(
        core == 0,
        jnp.concatenate([lambdas, other_lambdas]),
        jnp.concatenate([other_lambdas, lambdas]),
    )
    lam = lax.dynamic_slice_in_dim(plane_lambdas, z, 1)
    low_z, high_z = jnp.where(core == 0, 0, 1), jnp.where(core == 0, 3, 2)
    own = jnp.stack([low_z * 4 + x, high_z * 4 + x, z % 2]).astype(jnp.int32)
    gain = head_gain.reshape(1, VD)
    rows = jax.ShapeDtypeStruct((ROWS, VD), jnp.bfloat16)
    state = (jax.ShapeDtypeStruct((2, ROWS, VD), jnp.float32),) * 3
    o_low, *carried = attention_call(
        low_kernel, 2, (own, lam, q_low, q_high, gain), (rows, *state), (kv_low, conv_out), 12
    )
    o_a, o_b = attention_call(
        high_kernel, 1, (own, lam, q_high, gain, o_low, *carried), (rows, rows), (kv_high,), 6
    )
    back_a = lax.ppermute(o_a, z_core, reverse(route_a))
    back_b = lax.ppermute(o_b, z_core, reverse(route_b))
    attn_all = lax.all_gather(jnp.concatenate([back_a, back_b], axis=1), ("y", "c"), axis=0)
    conv_part = whole_conv(conv_all, w_out)
    mix, sums = whole_last(first, attn_all, w_out, conv_part)
    everything = lax.all_to_all(sums, ("y", "c"), split_axis=0, concat_axis=0, tiled=True)
    tp = (lax.axis_index("y") * 2 + core).astype(jnp.int32).reshape(1)
    return layer_norm(tp, mix, everything, out_gain.reshape(1, D))


def solution(mesh):
    chips = Mesh(mesh.devices.reshape(4, 4, 4, 2), ("z", "x", "y", "c"))
    sp, tp = ("z", "x"), ("y", "c")
    return jax.shard_map(
        per_device,
        mesh=chips,
        in_specs=(
            P(sp, None),
            P(None, tp),
            P(None, tp),
            P(None, tp),
            P(None, tp),
            P(None, tp),
            P(None, tp),
            P(None, tp),
            P(tp),
            P(),
            P(tp, None),
            P(tp, None),
            P(),
        ),
        out_specs=P(sp, tp),
        check_vma=False,
    )
```

```python
import jax
import jax.numpy as jnp
import numpy as np
from jax import lax
from jax.experimental import pallas as pl
from jax.experimental.pallas import tpu as pltpu
from jax.sharding import Mesh
from jax.sharding import PartitionSpec as P

D = 4096
QK = 64
VD = 128
ROWS = 768
HALO = 16
LOG2E = 1.4426950408889634

CORE_OF_Z = (0, 1, 1, 0)


def forward_route(round_index):
    route = []
    for z in range(4):
        for c in range(2):
            local = round_index if z < 2 else 1 - round_index
            route.append((z * 2 + c, (2 * c + local) * 2 + CORE_OF_Z[z]))
    return route


def reverse(route):
    return [(b, a) for a, b in route]


GROUP = 96


def rotary_tables():
    inverse = 10000.0 ** (-np.arange(0, QK, 2, dtype=np.float64) / QK)
    inverse = np.tile(inverse, 128 // inverse.size)
    rows = np.arange(GROUP, dtype=np.float64)[:, None] * inverse
    starts = np.arange(0, 16 * ROWS, GROUP, dtype=np.float64)[:, None] * inverse
    tables = (np.cos(rows), np.sin(rows), np.cos(starts), np.sin(starts))
    return tuple(t.astype(np.float32) for t in tables)


CHUNK = 1024
STEPS = D // CHUNK
AHEAD = 3


def streamed_products(pairs, sem, accs):
    copies = []
    for hbm, buf, by_columns in pairs:
        slot = len(copies)

        def copy(k, hbm=hbm, buf=buf, by_columns=by_columns, slot=slot):
            at = pl.ds(k * CHUNK, CHUNK)
            source = hbm.at[:, at] if by_columns else hbm.at[at, :]
            return pltpu.make_async_copy(source, buf.at[k], sem.at[slot, k])

        copies.append(copy)
    for k in range(AHEAD):
        for copy in copies:
            copy(k).start()
    for acc, _, _ in accs:
        acc[...] = jnp.zeros(acc.shape, jnp.float32)

    def step(k, carry):
        @pl.when(k + AHEAD < STEPS)
        def _():
            for copy in copies:
                copy(k + AHEAD).start()

        for copy in copies:
            copy(k).wait()
        for acc, lhs, weights in accs:
            h = lhs[k]
            for i, w in enumerate(weights):
                acc[i] += jnp.dot(h, w[k], preferred_element_type=jnp.float32)
        return carry

    lax.fori_loop(0, STEPS, step, 0)


def rotation(cr, sr, cs, ss):
    groups = range(ROWS // GROUP)
    cosine = jnp.concatenate(
        [cs[g : g + 1] * cr[...] - ss[g : g + 1] * sr[...] for g in groups], axis=0
    )
    sine = jnp.concatenate(
        [ss[g : g + 1] * cr[...] + cs[g : g + 1] * sr[...] for g in groups], axis=0
    )
    lane = lax.broadcasted_iota(jnp.int32, (ROWS, 128), 1)
    upper = (lane % QK) < QK // 2

    def rotated(x):
        x = x.astype(jnp.bfloat16).astype(jnp.float32)
        swapped = jnp.where(upper, -pltpu.roll(x, 128 - QK // 2, 1), pltpu.roll(x, QK // 2, 1))
        return x * cosine + swapped * sine

    return rotated


def qkv_kernel(
    where, h_ref, wk_ref, wv_ref, wq_ref, cr, sr, cs, ss, kva_ref, kvb_ref, qa_ref, qb_ref, rim_ref, acc, hb, kb, vb, qb, sem
):
    streamed_products(
        ((h_ref, hb, True), (wk_ref, kb, False), (wv_ref, vb, False), (wq_ref, qb, False)),
        sem,
        ((acc, hb, (kb, vb, qb)),),
    )
    for k in range(STEPS):
        rim_ref[:, k * CHUNK : (k + 1) * CHUNK] = hb[k, ROWS - HALO :, :]
    rotated = rotation(cr, sr, cs, ss)
    heads = []
    for i in range(2):
        cols = slice(i * 128, i * 128 + 128)
        query = rotated(acc[2, :, cols]) * (LOG2E / 8)
        parts = (rotated(acc[0, :, cols]), acc[1, :, cols], query)
        heads.append([part.astype(jnp.bfloat16) for part in parts])
    for flip, kv_ref, q_ref in ((0, kva_ref, qa_ref), (1, kvb_ref, qb_ref)):
        key, value, query = (
            jnp.where(where[1] == flip, heads[0][i], heads[1][i]) for i in range(3)
        )
        kv_ref[:, 0:128] = key
        kv_ref[:, 128:256] = value
        q_ref[...] = query


def in_hbm():
    return pl.BlockSpec(memory_space=pltpu.HBM)


def stream_buffers(weights, rim):
    rows = [pltpu.VMEM((STEPS, ROWS, CHUNK), jnp.bfloat16)]
    if rim:
        rows.append(pltpu.VMEM((STEPS, HALO, CHUNK), jnp.bfloat16))
    return (
        rows
        + [pltpu.VMEM((STEPS, CHUNK, 256), jnp.bfloat16)] * weights
        + [pltpu.SemaphoreType.DMA((weights + len(rows), STEPS))]
    )


def project(where, hidden, w_key, w_value, w_query):
    row_cos, row_sin, start_cos, start_sin = rotary_tables()
    table = pl.BlockSpec((GROUP, 128), lambda k, *_: (0, 0))
    starts = pl.BlockSpec((ROWS // GROUP, 128), lambda k, where: (where[0], 0))
    shapes = ((ROWS, 256), (ROWS, 256), (ROWS, 128), (ROWS, 128), (HALO, D))
    return pl.pallas_call(
        qkv_kernel,
        out_shape=tuple(jax.ShapeDtypeStruct(shape, jnp.bfloat16) for shape in shapes),
        grid_spec=pltpu.PrefetchScalarGridSpec(
            num_scalar_prefetch=1,
            grid=(1,),
            in_specs=[in_hbm()] * 4 + [table, table, starts, starts],
            out_specs=tuple(pl.BlockSpec(shape, lambda k, *_: (0, 0)) for shape in shapes),
            scratch_shapes=[pltpu.VMEM((3, ROWS, 256), jnp.float32), *stream_buffers(3, False)],
        ),
        compiler_params=pltpu.CompilerParams(vmem_limit_bytes=60 * 2**20),
        cost_estimate=pl.CostEstimate(
            flops=2 * ROWS * D * 768, bytes_accessed=13 * 2**20, transcendentals=0
        ),
        name="qkv",
    )(where, hidden, w_key, w_value, w_query, row_cos, row_sin, start_cos, start_sin)


def conv_kernel(
    h_ref, rim_ref, wb_ref, wc_ref, wh_ref, taps_ref, _, o_ref, acc, rim_acc, padded, hb, rb, b, c, h, sem
):
    streamed_products(
        (
            (h_ref, hb, True),
            (rim_ref, rb, True),
            (wb_ref, b, False),
            (wc_ref, c, False),
            (wh_ref, h, False),
        ),
        sem,
        ((acc, hb, (b, c, h)), (rim_acc, rb, (b, c, h))),
    )

    def once(x):
        return x.astype(jnp.bfloat16).astype(jnp.float32)

    padded[0:HALO] = once(rim_acc[1]) * once(rim_acc[2])
    padded[HALO:] = once(acc[1]) * once(acc[2])
    taps = taps_ref[...].astype(jnp.float32)
    conv = jnp.zeros((ROWS, 256), jnp.float32)
    for tap in range(3):
        conv = conv + taps[tap : tap + 1] * padded[HALO - 2 + tap : HALO - 2 + tap + ROWS]
    o_ref[...] = (once(acc[0]) * conv).astype(jnp.bfloat16)


def gated_conv(hidden, rim, w_b, w_c, w_h, taps, before):
    return pl.pallas_call(
        conv_kernel,
        out_shape=jax.ShapeDtypeStruct((ROWS, 256), jnp.bfloat16),
        grid=(1,),
        in_specs=[
            in_hbm(),
            in_hbm(),
            in_hbm(),
            in_hbm(),
            in_hbm(),
            pl.BlockSpec((3, 256), lambda k: (0, 0)),
            in_hbm(),
        ],
        out_specs=pl.BlockSpec((ROWS, 256), lambda k: (0, 0)),
        scratch_shapes=[
            pltpu.VMEM((3, ROWS, 256), jnp.float32),
            pltpu.VMEM((3, HALO, 256), jnp.float32),
            pltpu.VMEM((HALO + ROWS, 256), jnp.float32),
            *stream_buffers(3, True),
        ],
        compiler_params=pltpu.CompilerParams(vmem_limit_bytes=60 * 2**20),
        cost_estimate=pl.CostEstimate(
            flops=2 * ROWS * D * 768, bytes_accessed=13 * 2**20, transcendentals=0
        ),
        name="gated_conv",
    )(hidden, rim, w_b, w_c, w_h, taps, before)


KEYS_AT_ONCE = 256


def split_maps(q, qz):
    lane = lax.broadcasted_iota(jnp.int32, (ROWS, 128), 1)
    qz[0] = jnp.where(lane < QK, q, jnp.zeros_like(q))
    qz[1] = jnp.where(lane >= QK, q, jnp.zeros_like(q))


def start_state(m_s, l_s, acc):
    m_s[...] = jnp.full(m_s.shape, -1e30, jnp.float32)
    l_s[...] = jnp.zeros(l_s.shape, jnp.float32)
    acc[...] = jnp.zeros(acc.shape, jnp.float32)


def attend(qz, kv_ref, m_s, l_s, acc, first_row, n, place, first_key, width, masked):
    rows = slice(first_row, first_row + n)
    keys = kv_ref[place, first_key : first_key + width, 0:128]
    vals = kv_ref[place, first_key : first_key + width, 128:256]
    s = lax.dot_general(
        qz[:, rows, :].reshape(2 * n, 128),
        keys,
        (((1,), (1,)), ((), ())),
        preferred_element_type=jnp.float32,
    ).reshape(2, n, width)
    if masked:
        r = lax.broadcasted_iota(jnp.int32, (2, n, width), 1) + first_row
        k = lax.broadcasted_iota(jnp.int32, (2, n, width), 2) + first_key
        s = jnp.where(k <= r, s, -1e30)
    m_old = m_s[:, rows, :]
    m_new = jnp.maximum(m_old, jnp.max(s, axis=2, keepdims=True))
    alpha = jnp.exp2(m_old - m_new)
    p = jnp.exp2(s - jnp.tile(m_new, (1, 1, width // 128)))
    part = p[:, :, 0:128]
    for w in range(1, width // 128):
        part = part + p[:, :, w * 128 : (w + 1) * 128]
    l_s[:, rows, :] = l_s[:, rows, :] * alpha + part
    m_s[:, rows, :] = m_new
    pv = jnp.dot(
        p.astype(jnp.bfloat16).reshape(2 * n, width), vals, preferred_element_type=jnp.float32
    )
    acc[:, rows, :] = acc[:, rows, :] * alpha + pv.reshape(2, n, 128)


def attend_blocks(first, count, slot_of, ready, refs):
    def block(kb):
        for j in range(ROWS // KEYS_AT_ONCE):
            attend(*refs, 0, ROWS, slot_of(kb), j * KEYS_AT_ONCE, KEYS_AT_ONCE, False)

    def body(pair, carry):
        kb = first + 2 * pair
        ready(kb)
        ready(kb + 1)
        block(kb)
        block(kb + 1)
        return carry

    lax.fori_loop(0, count // 2, body, 0)

    @pl.when(count % 2 == 1)
    def _():
        ready(first + count - 1)
        block(first + count - 1)


def attend_diagonal(place, refs):
    for t in range(ROWS // 256):
        attend(*refs, t * 256, 256, place, 0, 256 * (t + 1), True)


def finish(lam, gain_ref, l_s, acc):
    denom = jnp.sum(l_s[...], axis=2, keepdims=True)
    diff = acc[0] / denom[0] - lam[0] * acc[1] / denom[1]
    mean_square = jnp.mean(diff * diff, axis=1, keepdims=True)
    normed = diff * lax.rsqrt(mean_square + 1e-5) * gain_ref[...].astype(jnp.float32)
    return normed.astype(jnp.bfloat16)


def low_place(kb):
    return (kb % 4) * 2 + kb // 4


def high_place(kb):
    return (kb % 4) * 2 + 3 - kb // 4


def low_kernel(own, lam, ql_ref, qh_ref, gain_ref, kv_hbm, _, o_ref, m_o, l_o, a_o, qz, kv_ref, sem):
    step = pl.program_id(0)

    def load(kb):
        return pltpu.make_async_copy(kv_hbm.at[low_place(kb)], kv_ref.at[kb], sem.at[kb])

    @pl.when(step == 0)
    def _():
        for kb in range(8):
            load(kb).start()

    def ready(kb):
        @pl.when(jnp.logical_or(step == 0, kb > own[0]))
        def _():
            load(kb).wait()

    split_maps(jnp.where(step == 0, ql_ref[...], qh_ref[...]), qz)
    start_state(m_o, l_o, a_o)
    refs = (qz, kv_ref, m_o, l_o, a_o)
    attend_blocks(0, jnp.where(step == 0, own[0], 8), lambda kb: kb, ready, refs)

    @pl.when(step == 0)
    def _():
        load(own[0]).wait()
        attend_diagonal(own[0], refs)
        o_ref[...] = finish(lam, gain_ref, l_o, a_o)


def high_kernel(
    own, lam, qh_ref, gain_ref, low_ref, m_i, l_i, a_i, kv_hbm, oa_ref, ob_ref, qz, kv_ref, sem
):
    def load(kb):
        slot = kb - 8
        return pltpu.make_async_copy(kv_hbm.at[high_place(kb)], kv_ref.at[slot], sem.at[slot])

    for kb in range(8, 16):

        @pl.when(kb <= own[1])
        def _(kb=kb):
            load(kb).start()

    split_maps(qh_ref[...], qz)
    refs = (qz, kv_ref, m_i, l_i, a_i)
    attend_blocks(8, own[1] - 8, lambda kb: kb - 8, lambda kb: load(kb).wait(), refs)
    load(own[1]).wait()
    attend_diagonal(own[1] - 8, refs)
    high = finish(lam, gain_ref, l_i, a_i)
    low_first = own[2] == 0
    oa_ref[...] = jnp.where(low_first, low_ref[...], high)
    ob_ref[...] = jnp.where(low_first, high, low_ref[...])


def attention_call(kernel, steps, args, outs, unread, blocks):
    def full(shape):
        return pl.BlockSpec(shape, lambda i, *_: (0,) * len(shape))

    return pl.pallas_call(
        kernel,
        out_shape=outs,
        grid_spec=pltpu.PrefetchScalarGridSpec(
            num_scalar_prefetch=2,
            grid=(steps,),
            in_specs=[full(a.shape) for a in args[2:]] + [in_hbm() for _ in unread],
            out_specs=tuple(full(o.shape) for o in outs),
            scratch_shapes=[
                pltpu.VMEM((2, ROWS, 128), jnp.bfloat16),
                pltpu.VMEM((8, ROWS, 256), jnp.bfloat16),
                pltpu.SemaphoreType.DMA((8,)),
            ],
        ),
        compiler_params=pltpu.CompilerParams(vmem_limit_bytes=60 * 2**20),
        cost_estimate=pl.CostEstimate(
            flops=blocks * 2 * 10**9, bytes_accessed=4 * 2**20, transcendentals=0
        ),
    )(*args, *unread)


def column_kernel(wc_ref, wa_ref, _, o_ref, buf, sem):
    width = o_ref.shape[3]
    loads = [
        pltpu.make_async_copy(w_ref, buf.at[i], sem.at[i, 8])
        for i, w_ref in enumerate((wc_ref, wa_ref))
    ]
    for load in loads:
        load.start()
    stores = []
    for i in range(2):
        loads[i].wait()
        for t in range(8):
            stores.append(
                pltpu.make_async_copy(
                    buf.at[i, :, pl.ds(t * width, width)], o_ref.at[t, i], sem.at[i, t]
                )
            )
            stores[-1].start()
    for store in stores:
        store.wait()


def column_blocks(w_conv, w_attn, before):
    return pl.pallas_call(
        column_kernel,
        out_shape=jax.ShapeDtypeStruct((8, 2, 256, D // 8), jnp.bfloat16),
        in_specs=[in_hbm(), in_hbm(), in_hbm()],
        out_specs=in_hbm(),
        scratch_shapes=[pltpu.VMEM((2, 256, D), jnp.bfloat16), pltpu.SemaphoreType.DMA((2, 9))],
        compiler_params=pltpu.CompilerParams(vmem_limit_bytes=60 * 2**20),
        cost_estimate=pl.CostEstimate(
            flops=3 * 10**9, bytes_accessed=9 * 2**20, transcendentals=0
        ),
        name="column_blocks",
    )(w_conv, w_attn, before)


def whole_conv_kernel(core, own_ref, other_ref, w_ref, o_ref):
    left = [ref[y] for ref in (own_ref, other_ref) for y in range(4)]
    right = [w_ref[2 * y + c, 0] for c in (core[0], 1 - core[0]) for y in range(4)]
    o_ref[...] = jnp.dot(
        jnp.concatenate(left, axis=1),
        jnp.concatenate(right, axis=0),
        preferred_element_type=jnp.float32,
    )


def whole_last_kernel(first, x_ref, w_ref, before_ref, mix_ref, sums_ref, xb, wb, acc, sem):
    copies = []
    for t in range(8):
        copies.append(pltpu.make_async_copy(x_ref.at[t], xb.at[t], sem.at[0, t]))
        copies.append(pltpu.make_async_copy(w_ref.at[t, 1], wb.at[t], sem.at[1, t]))
    head = pltpu.make_async_copy(before_ref, acc, sem.at[2, 0])
    head.start()
    for copy in copies:
        copy.start()
    head.wait()
    for t in range(8):
        copies[2 * t].wait()
        copies[2 * t + 1].wait()
        right = jnp.concatenate(
            [
                wb[t, pl.ds(pl.multiple_of(first[0] * VD, VD), VD), :],
                wb[t, pl.ds(pl.multiple_of((1 - first[0]) * VD, VD), VD), :],
            ],
            axis=0,
        )
        acc[...] += jnp.dot(xb[t], right, preferred_element_type=jnp.float32)
    mix = acc[...].astype(jnp.bfloat16)
    mix_ref[...] = mix
    wide = mix.astype(jnp.float32)
    square = wide * wide
    high = square.astype(jnp.bfloat16)
    low = (square - high.astype(jnp.float32)).astype(jnp.bfloat16)
    ones = jnp.ones((8, mix.shape[1]), jnp.bfloat16)

    def row_sums(values):
        return lax.dot_general(
            ones, values, (((1,), (1,)), ((), ())), preferred_element_type=jnp.float32
        )

    squares = row_sums(high) + row_sums(low)
    sums = jnp.concatenate([row_sums(mix)[0:1], squares[0:1]], axis=0)
    for copy in range(8):
        sums_ref[copy] = sums


def whole_conv(core, own, other, weights):
    width = weights.shape[3]
    half = pl.BlockSpec(own.shape, lambda i, *_: (0, 0, 0))
    return pl.pallas_call(
        whole_conv_kernel,
        out_shape=jax.ShapeDtypeStruct((ROWS, width), jnp.float32),
        grid_spec=pltpu.PrefetchScalarGridSpec(
            num_scalar_prefetch=1,
            grid=(1,),
            in_specs=[
                half,
                half,
                pl.BlockSpec((8, 1, 256, width), lambda i, *_: (0, 0, 0, 0)),
            ],
            out_specs=pl.BlockSpec((ROWS, width), lambda i, *_: (0, 0)),
        ),
        compiler_params=pltpu.CompilerParams(vmem_limit_bytes=60 * 2**20),
        cost_estimate=pl.CostEstimate(
            flops=2 * ROWS * 2048 * width, bytes_accessed=7 * 2**20, transcendentals=0
        ),
        name="whole_conv",
    )(core, own, other, weights)


def whole_last(first, gathered, weights, before):
    width = weights.shape[3]
    return pl.pallas_call(
        whole_last_kernel,
        out_shape=(
            jax.ShapeDtypeStruct((ROWS, width), jnp.bfloat16),
            jax.ShapeDtypeStruct((8, 2, ROWS), jnp.float32),
        ),
        grid_spec=pltpu.PrefetchScalarGridSpec(
            num_scalar_prefetch=1,
            grid=(1,),
            in_specs=[in_hbm(), in_hbm(), in_hbm()],
            out_specs=(
                pl.BlockSpec((ROWS, width), lambda i, *_: (0, 0)),
                pl.BlockSpec((8, 2, ROWS), lambda i, *_: (0, 0, 0)),
            ),
            scratch_shapes=[
                pltpu.VMEM((8, ROWS, 256), jnp.bfloat16),
                pltpu.VMEM((8, 256, width), jnp.bfloat16),
                pltpu.VMEM((ROWS, width), jnp.float32),
                pltpu.SemaphoreType.DMA((3, 8)),
            ],
        ),
        compiler_params=pltpu.CompilerParams(vmem_limit_bytes=60 * 2**20),
        cost_estimate=pl.CostEstimate(
            flops=2 * ROWS * 2048 * width, bytes_accessed=7 * 2**20, transcendentals=0
        ),
        name="whole_last",
    )(first, gathered, weights, before)


def norm_kernel(own, mix_ref, sums_ref, gain_ref, o_ref):
    ones = jnp.ones((8, 128), jnp.float32)

    def column(which):
        total = lax.dot_general(
            sums_ref[:, which, :],
            ones,
            (((0,), (0,)), ((), ())),
            preferred_element_type=jnp.float32,
            precision=lax.Precision.HIGHEST,
        )
        return total * (1.0 / D)

    mean = column(0)
    variance = column(1) - mean * mean
    scale = lax.rsqrt(variance + 1e-5)
    gain = gain_ref[...].astype(jnp.float32)
    for at in range(0, mix_ref.shape[1], 128):
        mix = mix_ref[:, at : at + 128].astype(jnp.float32)
        o_ref[:, at : at + 128] = ((mix - mean) * scale * gain[:, at : at + 128]).astype(
            jnp.bfloat16
        )


def layer_norm(own, mix, sums, gain):
    width = mix.shape[1]
    return pl.pallas_call(
        norm_kernel,
        out_shape=jax.ShapeDtypeStruct(mix.shape, jnp.bfloat16),
        grid_spec=pltpu.PrefetchScalarGridSpec(
            num_scalar_prefetch=1,
            grid=(1,),
            in_specs=[
                pl.BlockSpec(mix.shape, lambda i, *_: (0, 0)),
                pl.BlockSpec(sums.shape, lambda i, *_: (0, 0, 0)),
                pl.BlockSpec((1, width), lambda i, own: (0, own[0])),
            ],
            out_specs=pl.BlockSpec(mix.shape, lambda i, *_: (0, 0)),
        ),
        name="norm",
    )(own, mix, sums, gain)


def per_device(
    hidden_states,
    w_conv_b,
    w_conv_c,
    w_conv_h,
    conv_taps,
    w_query,
    w_key,
    w_value,
    lambdas,
    head_gain,
    w_out_conv,
    w_out_attn,
    out_gain,
):
    z = lax.axis_index("z")
    x = lax.axis_index("x")
    core = lax.axis_index("c")
    sp = z * 4 + x

    z_core = ("z", "c")
    other_lambdas = lax.ppermute(lambdas, "c", [(0, 1), (1, 0)])

    first = jnp.where(z < 2, 0, 1).astype(jnp.int32).reshape(1)
    where = jnp.stack([sp, jnp.where(z < 2, 0, 1)]).astype(jnp.int32)
    route_a, route_b = forward_route(0), forward_route(1)
    head_a, head_b, q_a, q_b, last_rows = project(where, hidden_states, w_key, w_value, w_query)
    rim = lax.ppermute(last_rows, ("z", "x"), [(i, i + 1) for i in range(15)])
    head_a = lax.ppermute(head_a, z_core, route_a)
    head_b = lax.ppermute(head_b, z_core, route_b)
    q_a = lax.ppermute(q_a, z_core, route_a)
    q_b = lax.ppermute(q_b, z_core, route_b)
    even = (z % 2) == 0
    own_low = jnp.where(even, head_a, head_b)
    own_high = jnp.where(even, head_b, head_a)
    q_low = jnp.where(even, q_a, q_b)
    q_high = jnp.where(even, q_b, q_a)
    kv_low = lax.all_gather(own_low, ("x", "c"), axis=0)
    kv_high = lax.all_gather(own_high, ("x", "c"), axis=0)

    blocks = column_blocks(w_out_conv, w_out_attn, own_low)
    w_out = lax.all_to_all(blocks, ("y", "c"), split_axis=0, concat_axis=0, tiled=True)
    conv_out = gated_conv(
        hidden_states, rim, w_conv_b, w_conv_c, w_conv_h, conv_taps, own_low
    )
    conv_own = lax.all_gather(conv_out, "y", axis=0)

    plane_lambdas = jnp.where(
        core == 0,
        jnp.concatenate([lambdas, other_lambdas]),
        jnp.concatenate([other_lambdas, lambdas]),
    )
    lam = lax.dynamic_slice_in_dim(plane_lambdas, z, 1)
    low_z, high_z = jnp.where(core == 0, 0, 1), jnp.where(core == 0, 3, 2)
    own = jnp.stack([low_z * 4 + x, high_z * 4 + x, z % 2]).astype(jnp.int32)
    gain = head_gain.reshape(1, VD)
    rows = jax.ShapeDtypeStruct((ROWS, VD), jnp.bfloat16)
    state = (jax.ShapeDtypeStruct((2, ROWS, VD), jnp.float32),) * 3
    o_low, *carried = attention_call(
        low_kernel, 2, (own, lam, q_low, q_high, gain), (rows, *state), (kv_low, conv_out), 12
    )
    o_a, o_b = attention_call(
        high_kernel, 1, (own, lam, q_high, gain, o_low, *carried), (rows, rows), (kv_high,), 6
    )
    back_a = lax.ppermute(o_a, z_core, reverse(route_a))
    back_b = lax.ppermute(o_b, z_core, reverse(route_b))
    attn_all = lax.all_gather(jnp.concatenate([back_a, back_b], axis=1), ("y", "c"), axis=0)
    conv_other = lax.ppermute(conv_own, "c", [(0, 1), (1, 0)])
    conv_part = whole_conv(
        core.astype(jnp.int32).reshape(1), conv_own, conv_other, w_out
    )
    mix, sums = whole_last(first, attn_all, w_out, conv_part)
    everything = lax.all_to_all(sums, ("y", "c"), split_axis=0, concat_axis=0, tiled=True)
    tp = (lax.axis_index("y") * 2 + core).astype(jnp.int32).reshape(1)
    return layer_norm(tp, mix, everything, out_gain.reshape(1, D))


def solution(mesh):
    chips = Mesh(mesh.devices.reshape(4, 4, 4, 2), ("z", "x", "y", "c"))
    sp, tp = ("z", "x"), ("y", "c")
    return jax.shard_map(
        per_device,
        mesh=chips,
        in_specs=(
            P(sp, None),
            P(None, tp),
            P(None, tp),
            P(None, tp),
            P(None, tp),
            P(None, tp),
            P(None, tp),
            P(None, tp),
            P(tp),
            P(),
            P(tp, None),
            P(tp, None),
            P(),
        ),
        out_specs=P(sp, tp),
        check_vma=False,
    )
```

```python
import jax
import jax.numpy as jnp
import numpy as np
from jax import lax
from jax.experimental import pallas as pl
from jax.experimental.pallas import tpu as pltpu
from jax.sharding import Mesh
from jax.sharding import PartitionSpec as P

D = 4096
QK = 64
VD = 128
ROWS = 768
HALO = 16
LOG2E = 1.4426950408889634

CORE_OF_Z = (0, 1, 1, 0)


def forward_route(round_index):
    route = []
    for z in range(4):
        for c in range(2):
            local = round_index if z < 2 else 1 - round_index
            route.append((z * 2 + c, (2 * c + local) * 2 + CORE_OF_Z[z]))
    return route


def reverse(route):
    return [(b, a) for a, b in route]


GROUP = 96


def rotary_tables():
    inverse = 10000.0 ** (-np.arange(0, QK, 2, dtype=np.float64) / QK)
    inverse = np.tile(inverse, 128 // inverse.size)
    rows = np.arange(GROUP, dtype=np.float64)[:, None] * inverse
    starts = np.arange(0, 16 * ROWS, GROUP, dtype=np.float64)[:, None] * inverse
    tables = (np.cos(rows), np.sin(rows), np.cos(starts), np.sin(starts))
    return tuple(t.astype(np.float32) for t in tables)


CHUNK = 1024
STEPS = D // CHUNK
AHEAD = 3


def streamed_products(pairs, sem, accs):
    copies = []
    for hbm, buf, by_columns in pairs:
        slot = len(copies)

        def copy(k, hbm=hbm, buf=buf, by_columns=by_columns, slot=slot):
            at = pl.ds(k * CHUNK, CHUNK)
            source = hbm.at[:, at] if by_columns else hbm.at[at, :]
            return pltpu.make_async_copy(source, buf.at[k], sem.at[slot, k])

        copies.append(copy)
    for k in range(AHEAD):
        for copy in copies:
            copy(k).start()
    for acc, _, _ in accs:
        acc[...] = jnp.zeros(acc.shape, jnp.float32)

    def step(k, carry):
        @pl.when(k + AHEAD < STEPS)
        def _():
            for copy in copies:
                copy(k + AHEAD).start()

        for copy in copies:
            copy(k).wait()
        for acc, lhs, weights in accs:
            h = lhs[k]
            for i, w in enumerate(weights):
                acc[i] += jnp.dot(h, w[k], preferred_element_type=jnp.float32)
        return carry

    lax.fori_loop(0, STEPS, step, 0)


def rotation(cr, sr, cs, ss):
    groups = range(ROWS // GROUP)
    cosine = jnp.concatenate(
        [cs[g : g + 1] * cr[...] - ss[g : g + 1] * sr[...] for g in groups], axis=0
    )
    sine = jnp.concatenate(
        [ss[g : g + 1] * cr[...] + cs[g : g + 1] * sr[...] for g in groups], axis=0
    )
    lane = lax.broadcasted_iota(jnp.int32, (ROWS, 128), 1)
    upper = (lane % QK) < QK // 2

    def rotated(x):
        x = x.astype(jnp.bfloat16).astype(jnp.float32)
        swapped = jnp.where(upper, -pltpu.roll(x, 128 - QK // 2, 1), pltpu.roll(x, QK // 2, 1))
        return x * cosine + swapped * sine

    return rotated


def qkv_kernel(
    where, h_ref, wk_ref, wv_ref, wq_ref, cr, sr, cs, ss, kva_ref, kvb_ref, qa_ref, qb_ref, rim_ref, acc, hb, kb, vb, qb, sem
):
    streamed_products(
        ((h_ref, hb, True), (wk_ref, kb, False), (wv_ref, vb, False), (wq_ref, qb, False)),
        sem,
        ((acc, hb, (kb, vb, qb)),),
    )
    for k in range(STEPS):
        rim_ref[:, k * CHUNK : (k + 1) * CHUNK] = hb[k, ROWS - HALO :, :]
    rotated = rotation(cr, sr, cs, ss)
    heads = []
    for i in range(2):
        cols = slice(i * 128, i * 128 + 128)
        query = rotated(acc[2, :, cols]) * (LOG2E / 8)
        parts = (rotated(acc[0, :, cols]), acc[1, :, cols], query)
        heads.append([part.astype(jnp.bfloat16) for part in parts])
    for flip, kv_ref, q_ref in ((0, kva_ref, qa_ref), (1, kvb_ref, qb_ref)):
        key, value, query = (
            jnp.where(where[1] == flip, heads[0][i], heads[1][i]) for i in range(3)
        )
        kv_ref[:, 0:128] = key
        kv_ref[:, 128:256] = value
        q_ref[...] = query


def in_hbm():
    return pl.BlockSpec(memory_space=pltpu.HBM)


def stream_buffers(weights, rim):
    rows = [pltpu.VMEM((STEPS, ROWS, CHUNK), jnp.bfloat16)]
    if rim:
        rows.append(pltpu.VMEM((STEPS, HALO, CHUNK), jnp.bfloat16))
    return (
        rows
        + [pltpu.VMEM((STEPS, CHUNK, 256), jnp.bfloat16)] * weights
        + [pltpu.SemaphoreType.DMA((weights + len(rows), STEPS))]
    )


def project(where, hidden, w_key, w_value, w_query):
    row_cos, row_sin, start_cos, start_sin = rotary_tables()
    table = pl.BlockSpec((GROUP, 128), lambda k, *_: (0, 0))
    starts = pl.BlockSpec((ROWS // GROUP, 128), lambda k, where: (where[0], 0))
    shapes = ((ROWS, 256), (ROWS, 256), (ROWS, 128), (ROWS, 128), (HALO, D))
    return pl.pallas_call(
        qkv_kernel,
        out_shape=tuple(jax.ShapeDtypeStruct(shape, jnp.bfloat16) for shape in shapes),
        grid_spec=pltpu.PrefetchScalarGridSpec(
            num_scalar_prefetch=1,
            grid=(1,),
            in_specs=[in_hbm()] * 4 + [table, table, starts, starts],
            out_specs=tuple(pl.BlockSpec(shape, lambda k, *_: (0, 0)) for shape in shapes),
            scratch_shapes=[pltpu.VMEM((3, ROWS, 256), jnp.float32), *stream_buffers(3, False)],
        ),
        compiler_params=pltpu.CompilerParams(vmem_limit_bytes=60 * 2**20),
        cost_estimate=pl.CostEstimate(
            flops=2 * ROWS * D * 768, bytes_accessed=13 * 2**20, transcendentals=0
        ),
        name="qkv",
    )(where, hidden, w_key, w_value, w_query, row_cos, row_sin, start_cos, start_sin)


def conv_kernel(
    h_ref, rim_ref, wb_ref, wc_ref, wh_ref, taps_ref, _, o_ref, acc, rim_acc, padded, hb, rb, b, c, h, sem
):
    streamed_products(
        (
            (h_ref, hb, True),
            (rim_ref, rb, True),
            (wb_ref, b, False),
            (wc_ref, c, False),
            (wh_ref, h, False),
        ),
        sem,
        ((acc, hb, (b, c, h)), (rim_acc, rb, (b, c, h))),
    )

    def once(x):
        return x.astype(jnp.bfloat16).astype(jnp.float32)

    padded[0:HALO] = once(rim_acc[1]) * once(rim_acc[2])
    padded[HALO:] = once(acc[1]) * once(acc[2])
    taps = taps_ref[...].astype(jnp.float32)
    conv = jnp.zeros((ROWS, 256), jnp.float32)
    for tap in range(3):
        conv = conv + taps[tap : tap + 1] * padded[HALO - 2 + tap : HALO - 2 + tap + ROWS]
    o_ref[...] = (once(acc[0]) * conv).astype(jnp.bfloat16)


def gated_conv(hidden, rim, w_b, w_c, w_h, taps, before):
    return pl.pallas_call(
        conv_kernel,
        out_shape=jax.ShapeDtypeStruct((ROWS, 256), jnp.bfloat16),
        grid=(1,),
        in_specs=[
            in_hbm(),
            in_hbm(),
            in_hbm(),
            in_hbm(),
            in_hbm(),
            pl.BlockSpec((3, 256), lambda k: (0, 0)),
            in_hbm(),
        ],
        out_specs=pl.BlockSpec((ROWS, 256), lambda k: (0, 0)),
        scratch_shapes=[
            pltpu.VMEM((3, ROWS, 256), jnp.float32),
            pltpu.VMEM((3, HALO, 256), jnp.float32),
            pltpu.VMEM((HALO + ROWS, 256), jnp.float32),
            *stream_buffers(3, True),
        ],
        compiler_params=pltpu.CompilerParams(vmem_limit_bytes=60 * 2**20),
        cost_estimate=pl.CostEstimate(
            flops=2 * ROWS * D * 768, bytes_accessed=13 * 2**20, transcendentals=0
        ),
        name="gated_conv",
    )(hidden, rim, w_b, w_c, w_h, taps, before)


KEYS_AT_ONCE = 256


def split_maps(q, qz):
    lane = lax.broadcasted_iota(jnp.int32, (ROWS, 128), 1)
    qz[0] = jnp.where(lane < QK, q, jnp.zeros_like(q))
    qz[1] = jnp.where(lane >= QK, q, jnp.zeros_like(q))


def start_state(m_s, l_s, acc):
    m_s[...] = jnp.full(m_s.shape, -1e30, jnp.float32)
    l_s[...] = jnp.zeros(l_s.shape, jnp.float32)
    acc[...] = jnp.zeros(acc.shape, jnp.float32)


def attend(qz, kv_ref, m_s, l_s, acc, first_row, n, place, first_key, width, masked):
    rows = slice(first_row, first_row + n)
    keys = kv_ref[place, first_key : first_key + width, 0:128]
    vals = kv_ref[place, first_key : first_key + width, 128:256]
    s = lax.dot_general(
        qz[:, rows, :].reshape(2 * n, 128),
        keys,
        (((1,), (1,)), ((), ())),
        preferred_element_type=jnp.float32,
    ).reshape(2, n, width)
    if masked:
        r = lax.broadcasted_iota(jnp.int32, (2, n, width), 1) + first_row
        k = lax.broadcasted_iota(jnp.int32, (2, n, width), 2) + first_key
        s = jnp.where(k <= r, s, -1e30)
    m_old = m_s[:, rows, :]
    m_new = jnp.maximum(m_old, jnp.max(s, axis=2, keepdims=True))
    alpha = jnp.exp2(m_old - m_new)
    p = jnp.exp2(s - jnp.tile(m_new, (1, 1, width // 128)))
    part = p[:, :, 0:128]
    for w in range(1, width // 128):
        part = part + p[:, :, w * 128 : (w + 1) * 128]
    l_s[:, rows, :] = l_s[:, rows, :] * alpha + part
    m_s[:, rows, :] = m_new
    pv = jnp.dot(
        p.astype(jnp.bfloat16).reshape(2 * n, width), vals, preferred_element_type=jnp.float32
    )
    acc[:, rows, :] = acc[:, rows, :] * alpha + pv.reshape(2, n, 128)


def attend_blocks(first, count, slot_of, ready, refs):
    def block(kb):
        for j in range(ROWS // KEYS_AT_ONCE):
            attend(*refs, 0, ROWS, slot_of(kb), j * KEYS_AT_ONCE, KEYS_AT_ONCE, False)

    def body(pair, carry):
        kb = first + 2 * pair
        ready(kb)
        ready(kb + 1)
        block(kb)
        block(kb + 1)
        return carry

    lax.fori_loop(0, count // 2, body, 0)

    @pl.when(count % 2 == 1)
    def _():
        ready(first + count - 1)
        block(first + count - 1)


def attend_diagonal(place, refs):
    for t in range(ROWS // 256):
        attend(*refs, t * 256, 256, place, 0, 256 * (t + 1), True)


def finish(lam, gain_ref, l_s, acc):
    denom = jnp.sum(l_s[...], axis=2, keepdims=True)
    diff = acc[0] / denom[0] - lam[0] * acc[1] / denom[1]
    mean_square = jnp.mean(diff * diff, axis=1, keepdims=True)
    normed = diff * lax.rsqrt(mean_square + 1e-5) * gain_ref[...].astype(jnp.float32)
    return normed.astype(jnp.bfloat16)


def low_place(kb):
    return (kb % 4) * 2 + kb // 4


def high_place(kb):
    return (kb % 4) * 2 + 3 - kb // 4


def low_kernel(
    own, lam, ql_ref, qh_ref, gain_ref, high_ref, kv_hbm, _, o_ref, m_o, l_o, a_o, qz, kv_ref, sem
):
    step = pl.program_id(0)

    def load(kb):
        return pltpu.make_async_copy(kv_hbm.at[low_place(kb)], kv_ref.at[kb], sem.at[kb])

    @pl.when(step == 0)
    def _():
        for kb in range(8):
            load(kb).start()

    def ready(kb):
        @pl.when(jnp.logical_or(step == 0, kb > own[0]))
        def _():
            load(kb).wait()

    split_maps(jnp.where(step == 0, ql_ref[...], qh_ref[...]), qz)
    start_state(m_o, l_o, a_o)
    refs = (qz, kv_ref, m_o, l_o, a_o)
    attend_blocks(0, jnp.where(step == 0, own[0], 8), lambda kb: kb, ready, refs)

    @pl.when(step == 0)
    def _():
        load(own[0]).wait()
        attend_diagonal(own[0], refs)
        o_ref[...] = finish(lam, gain_ref, l_o, a_o)

    @pl.when(step == 1)
    def _():
        attend_diagonal(0, (qz, high_ref, m_o, l_o, a_o))


def high_kernel(
    own, lam, qh_ref, gain_ref, low_ref, m_i, l_i, a_i, kv_hbm, oa_ref, ob_ref, qz, kv_ref, sem
):
    def load(kb):
        slot = kb - 8
        return pltpu.make_async_copy(kv_hbm.at[high_place(kb)], kv_ref.at[slot], sem.at[slot])

    for kb in range(8, 16):

        @pl.when(kb < own[1])
        def _(kb=kb):
            load(kb).start()

    split_maps(qh_ref[...], qz)
    refs = (qz, kv_ref, m_i, l_i, a_i)
    attend_blocks(8, own[1] - 8, lambda kb: kb - 8, lambda kb: load(kb).wait(), refs)
    high = finish(lam, gain_ref, l_i, a_i)
    low_first = own[2] == 0
    oa_ref[...] = jnp.where(low_first, low_ref[...], high)
    ob_ref[...] = jnp.where(low_first, high, low_ref[...])


def attention_call(kernel, steps, args, outs, unread, blocks):
    def full(shape):
        return pl.BlockSpec(shape, lambda i, *_: (0,) * len(shape))

    return pl.pallas_call(
        kernel,
        out_shape=outs,
        grid_spec=pltpu.PrefetchScalarGridSpec(
            num_scalar_prefetch=2,
            grid=(steps,),
            in_specs=[full(a.shape) for a in args[2:]] + [in_hbm() for _ in unread],
            out_specs=tuple(full(o.shape) for o in outs),
            scratch_shapes=[
                pltpu.VMEM((2, ROWS, 128), jnp.bfloat16),
                pltpu.VMEM((8, ROWS, 256), jnp.bfloat16),
                pltpu.SemaphoreType.DMA((8,)),
            ],
        ),
        compiler_params=pltpu.CompilerParams(vmem_limit_bytes=60 * 2**20),
        cost_estimate=pl.CostEstimate(
            flops=blocks * 2 * 10**9, bytes_accessed=4 * 2**20, transcendentals=0
        ),
    )(*args, *unread)


def column_kernel(wc_ref, wa_ref, _, o_ref, buf, sem):
    width = o_ref.shape[3]
    loads = [
        pltpu.make_async_copy(w_ref, buf.at[i], sem.at[i, 8])
        for i, w_ref in enumerate((wc_ref, wa_ref))
    ]
    for load in loads:
        load.start()
    stores = []
    for i in range(2):
        loads[i].wait()
        for t in range(8):
            stores.append(
                pltpu.make_async_copy(
                    buf.at[i, :, pl.ds(t * width, width)], o_ref.at[t, i], sem.at[i, t]
                )
            )
            stores[-1].start()
    for store in stores:
        store.wait()


def column_blocks(w_conv, w_attn, before):
    return pl.pallas_call(
        column_kernel,
        out_shape=jax.ShapeDtypeStruct((8, 2, 256, D // 8), jnp.bfloat16),
        in_specs=[in_hbm(), in_hbm(), in_hbm()],
        out_specs=in_hbm(),
        scratch_shapes=[pltpu.VMEM((2, 256, D), jnp.bfloat16), pltpu.SemaphoreType.DMA((2, 9))],
        compiler_params=pltpu.CompilerParams(vmem_limit_bytes=60 * 2**20),
        cost_estimate=pl.CostEstimate(
            flops=3 * 10**9, bytes_accessed=9 * 2**20, transcendentals=0
        ),
        name="column_blocks",
    )(w_conv, w_attn, before)


def whole_conv_kernel(core, own_ref, other_ref, w_ref, o_ref):
    left = [ref[y] for ref in (own_ref, other_ref) for y in range(4)]
    right = [w_ref[2 * y + c, 0] for c in (core[0], 1 - core[0]) for y in range(4)]
    o_ref[...] = jnp.dot(
        jnp.concatenate(left, axis=1),
        jnp.concatenate(right, axis=0),
        preferred_element_type=jnp.float32,
    )


def whole_last_kernel(first, x_ref, w_ref, before_ref, mix_ref, sums_ref, xb, wb, acc, sem):
    copies = []
    for t in range(8):
        copies.append(pltpu.make_async_copy(x_ref.at[t], xb.at[t], sem.at[0, t]))
        copies.append(pltpu.make_async_copy(w_ref.at[t, 1], wb.at[t], sem.at[1, t]))
    head = pltpu.make_async_copy(before_ref, acc, sem.at[2, 0])
    head.start()
    for copy in copies:
        copy.start()
    head.wait()
    for t in range(8):
        copies[2 * t].wait()
        copies[2 * t + 1].wait()
        right = jnp.concatenate(
            [
                wb[t, pl.ds(pl.multiple_of(first[0] * VD, VD), VD), :],
                wb[t, pl.ds(pl.multiple_of((1 - first[0]) * VD, VD), VD), :],
            ],
            axis=0,
        )
        acc[...] += jnp.dot(xb[t], right, preferred_element_type=jnp.float32)
    mix = acc[...].astype(jnp.bfloat16)
    mix_ref[...] = mix
    wide = mix.astype(jnp.float32)
    square = wide * wide
    high = square.astype(jnp.bfloat16)
    low = (square - high.astype(jnp.float32)).astype(jnp.bfloat16)
    ones = jnp.ones((8, mix.shape[1]), jnp.bfloat16)

    def row_sums(values):
        return lax.dot_general(
            ones, values, (((1,), (1,)), ((), ())), preferred_element_type=jnp.float32
        )

    squares = row_sums(high) + row_sums(low)
    sums = jnp.concatenate([row_sums(mix)[0:1], squares[0:1]], axis=0)
    for copy in range(8):
        sums_ref[copy] = sums


def whole_conv(core, own, other, weights):
    width = weights.shape[3]
    half = pl.BlockSpec(own.shape, lambda i, *_: (0, 0, 0))
    return pl.pallas_call(
        whole_conv_kernel,
        out_shape=jax.ShapeDtypeStruct((ROWS, width), jnp.float32),
        grid_spec=pltpu.PrefetchScalarGridSpec(
            num_scalar_prefetch=1,
            grid=(1,),
            in_specs=[
                half,
                half,
                pl.BlockSpec((8, 1, 256, width), lambda i, *_: (0, 0, 0, 0)),
            ],
            out_specs=pl.BlockSpec((ROWS, width), lambda i, *_: (0, 0)),
        ),
        compiler_params=pltpu.CompilerParams(vmem_limit_bytes=60 * 2**20),
        cost_estimate=pl.CostEstimate(
            flops=2 * ROWS * 2048 * width, bytes_accessed=7 * 2**20, transcendentals=0
        ),
        name="whole_conv",
    )(core, own, other, weights)


def whole_last(first, gathered, weights, before):
    width = weights.shape[3]
    return pl.pallas_call(
        whole_last_kernel,
        out_shape=(
            jax.ShapeDtypeStruct((ROWS, width), jnp.bfloat16),
            jax.ShapeDtypeStruct((8, 2, ROWS), jnp.float32),
        ),
        grid_spec=pltpu.PrefetchScalarGridSpec(
            num_scalar_prefetch=1,
            grid=(1,),
            in_specs=[in_hbm(), in_hbm(), in_hbm()],
            out_specs=(
                pl.BlockSpec((ROWS, width), lambda i, *_: (0, 0)),
                pl.BlockSpec((8, 2, ROWS), lambda i, *_: (0, 0, 0)),
            ),
            scratch_shapes=[
                pltpu.VMEM((8, ROWS, 256), jnp.bfloat16),
                pltpu.VMEM((8, 256, width), jnp.bfloat16),
                pltpu.VMEM((ROWS, width), jnp.float32),
                pltpu.SemaphoreType.DMA((3, 8)),
            ],
        ),
        compiler_params=pltpu.CompilerParams(vmem_limit_bytes=60 * 2**20),
        cost_estimate=pl.CostEstimate(
            flops=2 * ROWS * 2048 * width, bytes_accessed=7 * 2**20, transcendentals=0
        ),
        name="whole_last",
    )(first, gathered, weights, before)


def norm_kernel(own, mix_ref, sums_ref, gain_ref, o_ref):
    ones = jnp.ones((8, 128), jnp.float32)

    def column(which):
        total = lax.dot_general(
            sums_ref[:, which, :],
            ones,
            (((0,), (0,)), ((), ())),
            preferred_element_type=jnp.float32,
            precision=lax.Precision.HIGHEST,
        )
        return total * (1.0 / D)

    mean = column(0)
    variance = column(1) - mean * mean
    scale = lax.rsqrt(variance + 1e-5)
    gain = gain_ref[...].astype(jnp.float32)
    for at in range(0, mix_ref.shape[1], 128):
        mix = mix_ref[:, at : at + 128].astype(jnp.float32)
        o_ref[:, at : at + 128] = ((mix - mean) * scale * gain[:, at : at + 128]).astype(
            jnp.bfloat16
        )


def layer_norm(own, mix, sums, gain):
    width = mix.shape[1]
    return pl.pallas_call(
        norm_kernel,
        out_shape=jax.ShapeDtypeStruct(mix.shape, jnp.bfloat16),
        grid_spec=pltpu.PrefetchScalarGridSpec(
            num_scalar_prefetch=1,
            grid=(1,),
            in_specs=[
                pl.BlockSpec(mix.shape, lambda i, *_: (0, 0)),
                pl.BlockSpec(sums.shape, lambda i, *_: (0, 0, 0)),
                pl.BlockSpec((1, width), lambda i, own: (0, own[0])),
            ],
            out_specs=pl.BlockSpec(mix.shape, lambda i, *_: (0, 0)),
        ),
        name="norm",
    )(own, mix, sums, gain)


def per_device(
    hidden_states,
    w_conv_b,
    w_conv_c,
    w_conv_h,
    conv_taps,
    w_query,
    w_key,
    w_value,
    lambdas,
    head_gain,
    w_out_conv,
    w_out_attn,
    out_gain,
):
    z = lax.axis_index("z")
    x = lax.axis_index("x")
    core = lax.axis_index("c")
    sp = z * 4 + x

    z_core = ("z", "c")
    other_lambdas = lax.ppermute(lambdas, "c", [(0, 1), (1, 0)])

    first = jnp.where(z < 2, 0, 1).astype(jnp.int32).reshape(1)
    where = jnp.stack([sp, jnp.where(z < 2, 0, 1)]).astype(jnp.int32)
    route_a, route_b = forward_route(0), forward_route(1)
    head_a, head_b, q_a, q_b, last_rows = project(where, hidden_states, w_key, w_value, w_query)
    rim = lax.ppermute(last_rows, ("z", "x"), [(i, i + 1) for i in range(15)])
    head_a = lax.ppermute(head_a, z_core, route_a)
    head_b = lax.ppermute(head_b, z_core, route_b)
    q_a = lax.ppermute(q_a, z_core, route_a)
    q_b = lax.ppermute(q_b, z_core, route_b)
    even = (z % 2) == 0
    own_low = jnp.where(even, head_a, head_b)
    own_high = jnp.where(even, head_b, head_a)
    q_low = jnp.where(even, q_a, q_b)
    q_high = jnp.where(even, q_b, q_a)
    kv_low = lax.all_gather(own_low, ("x", "c"), axis=0)
    kv_high = lax.all_gather(own_high, ("x", "c"), axis=0)

    blocks = column_blocks(w_out_conv, w_out_attn, own_low)
    w_out = lax.all_to_all(blocks, ("y", "c"), split_axis=0, concat_axis=0, tiled=True)
    conv_out = gated_conv(
        hidden_states, rim, w_conv_b, w_conv_c, w_conv_h, conv_taps, own_low
    )
    conv_own = lax.all_gather(conv_out, "y", axis=0)

    plane_lambdas = jnp.where(
        core == 0,
        jnp.concatenate([lambdas, other_lambdas]),
        jnp.concatenate([other_lambdas, lambdas]),
    )
    lam = lax.dynamic_slice_in_dim(plane_lambdas, z, 1)
    low_z, high_z = jnp.where(core == 0, 0, 1), jnp.where(core == 0, 3, 2)
    own = jnp.stack([low_z * 4 + x, high_z * 4 + x, z % 2]).astype(jnp.int32)
    gain = head_gain.reshape(1, VD)
    rows = jax.ShapeDtypeStruct((ROWS, VD), jnp.bfloat16)
    state = (jax.ShapeDtypeStruct((2, ROWS, VD), jnp.float32),) * 3
    o_low, *carried = attention_call(
        low_kernel,
        2,
        (own, lam, q_low, q_high, gain, own_high[None]),
        (rows, *state),
        (kv_low, conv_out),
        12,
    )
    o_a, o_b = attention_call(
        high_kernel, 1, (own, lam, q_high, gain, o_low, *carried), (rows, rows), (kv_high,), 6
    )
    back_a = lax.ppermute(o_a, z_core, reverse(route_a))
    back_b = lax.ppermute(o_b, z_core, reverse(route_b))
    attn_all = lax.all_gather(jnp.concatenate([back_a, back_b], axis=1), ("y", "c"), axis=0)
    conv_other = lax.ppermute(conv_own, "c", [(0, 1), (1, 0)])
    conv_part = whole_conv(
        core.astype(jnp.int32).reshape(1), conv_own, conv_other, w_out
    )
    mix, sums = whole_last(first, attn_all, w_out, conv_part)
    everything = lax.all_to_all(sums, ("y", "c"), split_axis=0, concat_axis=0, tiled=True)
    tp = (lax.axis_index("y") * 2 + core).astype(jnp.int32).reshape(1)
    return layer_norm(tp, mix, everything, out_gain.reshape(1, D))


def solution(mesh):
    chips = Mesh(mesh.devices.reshape(4, 4, 4, 2), ("z", "x", "y", "c"))
    sp, tp = ("z", "x"), ("y", "c")
    return jax.shard_map(
        per_device,
        mesh=chips,
        in_specs=(
            P(sp, None),
            P(None, tp),
            P(None, tp),
            P(None, tp),
            P(None, tp),
            P(None, tp),
            P(None, tp),
            P(None, tp),
            P(tp),
            P(),
            P(tp, None),
            P(tp, None),
            P(),
        ),
        out_specs=P(sp, tp),
        check_vma=False,
    )
```
